32 devices in a mesh: grp: 2 (over y), sp: 4 (over z), tp: 4 (over x, core).
Axes of the slice: x: 2, y: 2, z: 4, core: 2. Of those that a mesh axis runs over, the one named last changes fastest.
Arguments:
- ssm_input: bfloat16 [1024, 1024], P(('grp', 'sp'), 'tp'), parts along dimension 0, may hold values from -6 to 6
- residual_in: bfloat16 [1024, 2048], P(('grp', 'sp')), parts along dimension 0, may hold values from -4 to 4
- log_step: float32 [64], P('tp'), may hold values from -6.91 to -2.3
- decay_real: float32 [64, 64], P('tp'), may hold values from -34 to 0, as said below
- freq: float32 [64, 64], P('tp'), may hold values from 0.5 to 8
- in_real: float32 [64, 64, 16], P('tp'), may hold values from -1 to 1
- in_imag: float32 [64, 64, 16], P('tp'), may hold values from -1 to 1
- out_real: float32 [64, 16, 64], P('tp'), may hold values from -0.5 to 0.5
- out_imag: float32 [64, 16, 64], P('tp'), may hold values from -0.5 to 0.5
- skip: float32 [1024], P('tp'), may hold values from -3 to 3
- w_glu: bfloat16 [1024, 1024], replicated, may hold values from -0.1875 to 0.1875
- b_glu: float32 [1024], replicated, may hold values from -3 to 3
- w_branch: bfloat16 [1024, 2048], replicated, may hold values from -0.1875 to 0.1875
- norm_gain: float32 [2048], replicated, may hold values from 0.1 to 1.9
- w_gate: bfloat16 [2048, 5632], P('sp', 'tp'), may hold values from -0.125 to 0.125
- w_up: bfloat16 [2048, 5632], P('sp', 'tp'), may hold values from -0.125 to 0.125
- w_down: bfloat16 [5632, 2048], P('tp', 'sp'), may hold values from -0.078125 to 0.078125
Outputs:
- mixed: bfloat16 [1024, 2048], P(('grp', 'sp', 'tp')), parts along dimension 0
The draws below stay inside these ranges and needn't reach their ends.
There are 2 independent parts, one for each index of `grp`. The reference program is written for one: setup_inputs(seed, part) draws one part's arguments, and reference() takes and returns one part's arrays. A program takes and returns all parts, laid end to end along the dimension named above; an argument that names none is the same for every part. Nothing has to cross between parts.
Inputs may be any that keep to these rules, and one draw needn't show every extreme that they name: `decay_real`: negative in every entry.
All inputs are finite; a program needn't handle non-finite values.
Results may differ from the reference program's by a relative error of at most 0.015.
Values may be sent and summed in bfloat16 or wider, within the bound.
A program may use at most 128 MiB of HBM per device.

```python
import math
import jax
import jax.numpy as jnp
from jax import lax

D = 2048
FF = 5632
SSM_GROUPS = 64
SSM_GROUP = 16
SSM_STATE = 64
TOK_DEV = 128
SSM_WIDTH = 1024
TOKENS = 512
N_SP = 4


def decay_plan(key):
    subkeys = jax.random.split(jax.random.fold_in(key, 11), 5)
    fast_share = 0.5
    fast_group = jax.random.uniform(subkeys[0], (SSM_GROUPS,), jnp.float32) < fast_share
    slow_rate = jax.random.uniform(subkeys[1], (SSM_GROUPS,), jnp.float32, 0.3, 2.0) / TOKENS
    fast_rate = jax.random.uniform(subkeys[2], (SSM_GROUPS,), jnp.float32, 1.0 / 100.0, 1.0 / 30.0)
    decay_rate = jnp.where(fast_group, fast_rate, slow_rate)
    log_steps = jax.random.uniform(subkeys[3], (SSM_GROUPS,), jnp.float32, math.log(0.001), math.log(0.1))
    spread = jax.random.uniform(subkeys[4], (SSM_GROUPS, SSM_STATE), jnp.float32, 0.5, 1.0)
    return (log_steps, decay_rate, spread)


def draw_log_step(key, part):
    return decay_plan(key)[0]


def draw_decay_real(key, part):
    log_steps, decay_rate, spread = decay_plan(key)
    return -decay_rate[:, None] * spread / jnp.exp(log_steps)[:, None]


def shard_levels(rng, shape, pieces, smallest, largest):
    gain = 1.0
    for position, blocks in pieces:
        heights = jax.random.uniform(jax.random.fold_in(jax.random.fold_in(rng, 6), position), (blocks,), jnp.float32, smallest / len(pieces), largest / len(pieces))
        gain = gain * jnp.repeat(jnp.exp(heights), shape[position] // blocks).reshape((-1,) + (1,) * (len(shape) - 1 - position))
    return gain


def centred(own_key, shape, scale, most, cuts=(), kind=jnp.bfloat16):
    result = scale * jax.random.normal(own_key, shape, jnp.float32)
    if cuts:
        result = result * shard_levels(own_key, shape, cuts, -0.22, 0.18)
    return jnp.clip(result, -most, most).astype(kind)


def setup_inputs(seed: int = 0, part: int = 0) -> dict:
    key_of = jax.random.split(jax.random.key(seed), 18)
    own_keys = jax.random.split(jax.random.fold_in(key_of[17], part), 18)
    return {
        "ssm_input": centred(own_keys[0], (TOKENS, SSM_WIDTH), 1.0, 6.0, ((0, 4), (1, 4))),
        "residual_in": centred(own_keys[1], (TOKENS, D), 0.5, 4.0, ((0, 4),)),
        "log_step": draw_log_step(jax.random.fold_in(key_of[17], 71), part),
        "decay_real": draw_decay_real(jax.random.fold_in(key_of[17], 71), part),
        "freq": jnp.clip(0.5 + 7.5 * jax.random.uniform(key_of[4], (SSM_GROUPS, SSM_STATE), jnp.float32) ** shard_levels(key_of[4], (SSM_GROUPS, SSM_STATE), ((0, 4),), -0.2, 0.2), 0.5, 8.0),
        "in_real": centred(key_of[5], (SSM_GROUPS, SSM_STATE, SSM_GROUP), (2 * SSM_GROUP) ** -0.5, 1.0, ((0, 4),), jnp.float32),
        "in_imag": centred(key_of[6], (SSM_GROUPS, SSM_STATE, SSM_GROUP), (2 * SSM_GROUP) ** -0.5, 1.0, ((0, 4),), jnp.float32),
        "out_real": centred(key_of[7], (SSM_GROUPS, SSM_GROUP, SSM_STATE), (2 * SSM_STATE) ** -0.5, 0.5, ((0, 4),), jnp.float32),
        "out_imag": centred(key_of[8], (SSM_GROUPS, SSM_GROUP, SSM_STATE), (2 * SSM_STATE) ** -0.5, 0.5, ((0, 4),), jnp.float32),
        "skip": centred(key_of[9], (SSM_WIDTH,), 0.5, 3.0, ((0, 4),), jnp.float32),
        "w_glu": centred(key_of[10], (SSM_WIDTH, SSM_WIDTH), SSM_WIDTH ** -0.5, 0.1875),
        "b_glu": centred(key_of[11], (SSM_WIDTH,), 0.5, 3.0, (), jnp.float32),
        "w_branch": centred(key_of[12], (SSM_WIDTH, D), SSM_WIDTH ** -0.5, 0.1875),
        "norm_gain": jnp.clip(1.0 + 0.18 * jax.random.normal(key_of[13], (D,), jnp.float32), 0.1, 1.9),
        "w_gate": centred(key_of[14], (D, FF), D ** -0.5, 0.125, ((0, 4), (1, 4))),
        "w_up": centred(key_of[15], (D, FF), D ** -0.5, 0.125, ((0, 4), (1, 4))),
        "w_down": centred(key_of[16], (FF, D), FF ** -0.5, 0.078125, ((0, 4), (1, 4))),
    }


EPS = 1e-06

def discretize(log_step, decay_real, freq, in_real, in_imag):
    step_size = jnp.exp(log_step)[:, None]
    magnitude = jnp.exp(decay_real * step_size)
    abar_re = magnitude * jnp.cos(freq * step_size)
    abar_im = magnitude * jnp.sin(freq * step_size)
    denominator = decay_real * decay_real + freq * freq
    less_re = abar_re - 1.0
    less_im = abar_im
    hold_re = ((less_re * decay_real + less_im * freq) / denominator)[..., None]
    hold_im = ((less_im * decay_real - less_re * freq) / denominator)[..., None]
    bbar_re = hold_re * in_real - hold_im * in_imag
    bbar_im = hold_re * in_imag + hold_im * in_real
    return (step_size, abar_re, abar_im, bbar_re, bbar_im)

def powers(decay_real, freq, step_size, length):
    steps_up = (jnp.arange(length, dtype=jnp.int32) + 1).astype(jnp.float32)[:, None, None]
    magnitude = jnp.exp((decay_real * step_size)[None] * steps_up)
    phase = (freq * step_size)[None] * steps_up
    return (magnitude * jnp.cos(phase), magnitude * jnp.sin(phase))

def compose(earlier, later):
    a1r, a1i, b1r, b1i = earlier
    a2r, a2i, b2r, b2i = later
    return (a2r * a1r - a2i * a1i, a2r * a1i + a2i * a1r, a2r * b1r - a2i * b1i + b2r, a2r * b1i + a2i * b1r + b2i)

def local_states(inputs, abar_re, abar_im, bbar_re, bbar_im):
    hp = lax.Precision.HIGHEST
    drive_re = jnp.einsum('lgm,gpm->lgp', inputs, bbar_re, precision=hp)
    drive_im = jnp.einsum('lgm,gpm->lgp', inputs, bbar_im, precision=hp)
    full_re = jnp.broadcast_to(abar_re[None], drive_re.shape)
    full_im = jnp.broadcast_to(abar_im[None], drive_re.shape)
    scanned = lax.associative_scan(compose, (full_re, full_im, drive_re, drive_im), axis=0)
    return (scanned[2], scanned[3])

def readout(state_re, state_im, out_real, out_imag, skip_mat, inputs):
    hp = lax.Precision.HIGHEST
    values = jnp.einsum('lgp,gmp->lgm', state_re, out_real, precision=hp) - jnp.einsum('lgp,gmp->lgm', state_im, out_imag, precision=hp) + skip_mat[None] * inputs
    values = jax.nn.gelu(values)
    return values.reshape(values.shape[0], -1).astype(jnp.bfloat16)

def reference(ssm_input, residual_in, log_step, decay_real, freq, in_real, in_imag, out_real, out_imag, skip, w_glu, b_glu, w_branch, norm_gain, w_gate, w_up, w_down):
    step_size, abar_re, abar_im, bbar_re, bbar_im = discretize(log_step, decay_real, freq, in_real, in_imag)
    pow_re, pow_im = powers(decay_real, freq, step_size, TOK_DEV)
    skip_mat = skip.reshape(SSM_GROUPS, SSM_GROUP)
    blocks = ssm_input.astype(jnp.float32).reshape(N_SP, TOK_DEV, SSM_GROUPS, SSM_GROUP)

    def one_block(carried, inputs):
        local_re, local_im = local_states(inputs, abar_re, abar_im, bbar_re, bbar_im)
        state_re = local_re + pow_re * carried[0][None] - pow_im * carried[1][None]
        state_im = local_im + pow_re * carried[1][None] + pow_im * carried[0][None]
        mixer_out = readout(state_re, state_im, out_real, out_imag, skip_mat, inputs)
        return ((state_re[-1], state_im[-1]), mixer_out)
    start_state = (jnp.zeros((SSM_GROUPS, SSM_STATE), jnp.float32), jnp.zeros((SSM_GROUPS, SSM_STATE), jnp.float32))
    unused, outputs = lax.scan(one_block, start_state, blocks)
    mixer_out = outputs.reshape(TOKENS, SSM_WIDTH)
    glu_pre = jnp.dot(mixer_out, w_glu, preferred_element_type=jnp.float32) + b_glu
    gated = (mixer_out.astype(jnp.float32) * jax.nn.sigmoid(glu_pre)).astype(jnp.bfloat16)
    stream = residual_in.astype(jnp.float32) + jnp.dot(gated, w_branch, preferred_element_type=jnp.float32)
    scale_rows = lax.rsqrt(lax.optimization_barrier(jnp.mean(stream * stream, axis=-1, keepdims=True)) + EPS)
    normed = (stream * scale_rows * norm_gain).astype(jnp.bfloat16)
    gate_sum = jnp.dot(normed, w_gate, preferred_element_type=jnp.float32)
    up_sum = jnp.dot(normed, w_up, preferred_element_type=jnp.float32)
    hidden = (jax.nn.silu(gate_sum) * up_sum).astype(jnp.bfloat16)
    return (stream + jnp.dot(hidden, w_down, preferred_element_type=jnp.float32)).astype(jnp.bfloat16)
```

```python
import functools
import math

import jax
import jax.numpy as jnp
from jax import lax
from jax.experimental import pallas as pl
from jax.experimental.pallas import tpu as pltpu
from jax.sharding import PartitionSpec as P

EPS = 1e-06


def prefix(shard, axis, combine, identity):
    count, place = (lax.axis_size(axis), lax.axis_index(axis))
    everything = jax.tree.map(lambda part: lax.all_gather(part, axis), shard)
    start = jax.tree.map(
        lambda part, zero: jnp.broadcast_to(jnp.asarray(zero, part.dtype), part.shape),
        shard,
        identity,
    )

    def lap(k, before):
        reached = k < place
        new = combine(before, jax.tree.map(lambda part: part[k], everything))
        return jax.tree.map(lambda a, b: jnp.where(reached, a, b), new, before)

    return lax.fori_loop(0, count, lap, start)


def discretize(log_step, decay_real, freq, in_real, in_imag):
    step_size = jnp.exp(log_step)[:, None]
    magnitude = jnp.exp(decay_real * step_size)
    abar_re = magnitude * jnp.cos(freq * step_size)
    abar_im = magnitude * jnp.sin(freq * step_size)
    denominator = decay_real * decay_real + freq * freq
    less_re = abar_re - 1.0
    hold_re = ((less_re * decay_real + abar_im * freq) / denominator)[..., None]
    hold_im = ((abar_im * decay_real - less_re * freq) / denominator)[..., None]
    bbar_re = hold_re * in_real - hold_im * in_imag
    bbar_im = hold_re * in_imag + hold_im * in_real
    return (step_size, abar_re, abar_im, bbar_re, bbar_im)


def powers(decay_real, freq, step_size, length):
    steps_up = (jnp.arange(length, dtype=jnp.int32) + 1).astype(jnp.float32)[:, None, None]
    magnitude = jnp.exp((decay_real * step_size)[None] * steps_up)
    phase = (freq * step_size)[None] * steps_up
    return (magnitude * jnp.cos(phase), magnitude * jnp.sin(phase))


def compose(earlier, later):
    a1r, a1i, b1r, b1i = earlier
    a2r, a2i, b2r, b2i = later
    return (
        a2r * a1r - a2i * a1i,
        a2r * a1i + a2i * a1r,
        a2r * b1r - a2i * b1i + b2r,
        a2r * b1i + a2i * b1r + b2i,
    )


def local_states(inputs, decay_real, freq, step_size, bbar_re, bbar_im):
    highest = lax.Precision.HIGHEST
    tok_rows, group_count, unused = inputs.shape
    lanes = group_count * decay_real.shape[1]
    drive_re = jnp.einsum("lgm,gpm->lgp", inputs, bbar_re, precision=highest).reshape(
        tok_rows, lanes
    )
    drive_im = jnp.einsum("lgm,gpm->lgp", inputs, bbar_im, precision=highest).reshape(
        tok_rows, lanes
    )
    span = math.gcd(tok_rows, 16)
    spans = tok_rows // span
    rate = (decay_real * step_size).reshape(lanes)
    turn = (freq * step_size).reshape(lanes)
    later = jnp.arange(span, dtype=jnp.int32)[:, None]
    earlier = jnp.arange(span, dtype=jnp.int32)[None, :]
    lag = (later - earlier).astype(jnp.float32)
    causal = (later >= earlier)[..., None]
    lag_pos = jnp.maximum(lag, 0.0)[..., None]
    table_mag = jnp.exp(rate[None, None] * lag_pos)
    table_re = jnp.where(causal, table_mag * jnp.cos(turn[None, None] * lag_pos), 0.0)
    table_im = jnp.where(causal, table_mag * jnp.sin(turn[None, None] * lag_pos), 0.0)
    block_re = drive_re.reshape(spans, 1, span, lanes)
    block_im = drive_im.reshape(spans, 1, span, lanes)
    inner_re = jnp.sum(table_re[None] * block_re - table_im[None] * block_im, axis=2)
    inner_im = jnp.sum(table_re[None] * block_im + table_im[None] * block_re, axis=2)
    steps_up = (jnp.arange(span, dtype=jnp.int32) + 1).astype(jnp.float32)[:, None]
    pow_mag = jnp.exp(rate[None] * steps_up)
    pow_re = pow_mag * jnp.cos(turn[None] * steps_up)
    pow_im = pow_mag * jnp.sin(turn[None] * steps_up)
    span_re = pow_re[-1]
    span_im = pow_im[-1]

    def carry_step(entering, ends):
        next_re = span_re * entering[0] - span_im * entering[1] + ends[0]
        next_im = span_re * entering[1] + span_im * entering[0] + ends[1]
        return ((next_re, next_im), entering)

    zeros = jnp.zeros((lanes,), jnp.float32)
    unused_carry, entering = lax.scan(
        carry_step, (zeros, zeros), (inner_re[:, -1], inner_im[:, -1])
    )
    state_re = inner_re + pow_re[None] * entering[0][:, None] - pow_im[None] * entering[1][:, None]
    state_im = inner_im + pow_re[None] * entering[1][:, None] + pow_im[None] * entering[0][:, None]
    shape = (tok_rows, group_count, decay_real.shape[1])
    return (state_re.reshape(shape), state_im.reshape(shape))


def readout(state_re, state_im, out_real, out_imag, skip_mat, inputs):
    highest = lax.Precision.HIGHEST
    values = (
        jnp.einsum("lgp,gmp->lgm", state_re, out_real, precision=highest)
        - jnp.einsum("lgp,gmp->lgm", state_im, out_imag, precision=highest)
        + skip_mat[None] * inputs
    )
    values = jax.nn.gelu(values)
    return values.reshape(values.shape[0], -1).astype(jnp.bfloat16)


def row_norm(stream, norm_gain):
    scale_rows = lax.rsqrt(jnp.mean(stream * stream, axis=-1, keepdims=True) + EPS)
    return (stream * scale_rows * norm_gain).astype(jnp.bfloat16)


def gathered_weights(
    ssm_input,
    residual_in,
    log_step,
    decay_real,
    freq,
    in_real,
    in_imag,
    out_real,
    out_imag,
    skip,
    w_glu,
    b_glu,
    w_branch,
    norm_gain,
    w_gate,
    w_up,
    w_down,
):
    tok_rows, width_local = ssm_input.shape
    group_count = log_step.shape[0]
    group_size = in_real.shape[2]
    tp_count = lax.axis_size("tp")
    tp_index = lax.axis_index("tp")
    own_rows = tok_rows // tp_count
    step_size, abar_re, abar_im, bbar_re, bbar_im = discretize(
        log_step, decay_real, freq, in_real, in_imag
    )
    pow_re, pow_im = powers(decay_real, freq, step_size, tok_rows)
    inputs = ssm_input.astype(jnp.float32).reshape(tok_rows, group_count, group_size)
    local_re, local_im = local_states(inputs, decay_real, freq, step_size, bbar_re, bbar_im)
    identity = (
        jnp.ones_like(abar_re),
        jnp.zeros_like(abar_re),
        jnp.zeros_like(abar_re),
        jnp.zeros_like(abar_re),
    )
    carried = prefix((pow_re[-1], pow_im[-1], local_re[-1], local_im[-1]), "sp", compose, identity)
    state_re = local_re + pow_re * carried[2][None] - pow_im * carried[3][None]
    state_im = local_im + pow_re * carried[3][None] + pow_im * carried[2][None]
    mixer_out = readout(
        state_re, state_im, out_real, out_imag, skip.reshape(group_count, group_size), inputs
    )
    mixer_rows = lax.all_to_all(mixer_out, "tp", split_axis=0, concat_axis=1, tiled=True)
    glu_pre = jnp.dot(mixer_rows, w_glu, preferred_element_type=jnp.float32) + b_glu
    gated = (mixer_rows.astype(jnp.float32) * jax.nn.sigmoid(glu_pre)).astype(jnp.bfloat16)
    residual_own = lax.dynamic_slice_in_dim(residual_in, tp_index * own_rows, own_rows, 0)
    stream = residual_own.astype(jnp.float32) + jnp.dot(
        gated, w_branch, preferred_element_type=jnp.float32
    )
    normed = row_norm(stream, norm_gain)
    normed_all = lax.all_gather(normed, "tp", axis=0, tiled=True)
    gate_sum = jnp.dot(
        normed_all,
        lax.all_gather(w_gate, "sp", axis=0, tiled=True),
        preferred_element_type=jnp.float32,
    )
    up_sum = jnp.dot(
        normed_all,
        lax.all_gather(w_up, "sp", axis=0, tiled=True),
        preferred_element_type=jnp.float32,
    )
    hidden = (jax.nn.silu(gate_sum) * up_sum).astype(jnp.bfloat16)
    down_whole = lax.all_gather(w_down, "sp", axis=1, tiled=True)
    summed = lax.psum_scatter(
        jnp.dot(hidden, down_whole, preferred_element_type=jnp.float32).astype(jnp.bfloat16),
        "tp",
        scatter_dimension=0,
        tiled=True,
    ).astype(jnp.float32)
    return (stream + summed).astype(jnp.bfloat16)


MESH = pl.DeviceIdType.MESH
F32 = jnp.float32
BF16 = jnp.bfloat16
NT = (((1,), (1,)), ((), ()))


def greet(sizes, place):
    barrier = pltpu.get_barrier_semaphore()
    for axis in sizes:
        for d in range(1, sizes[axis]):
            pl.semaphore_signal(
                barrier, inc=1, device_id={axis: lax.rem(place[axis] + d, sizes[axis])},
                device_id_type=MESH,
            )
    pl.semaphore_wait(barrier, sum(sizes.values()) - len(sizes))


def send(src, dst, ss, rs, **to):
    copy = pltpu.make_async_remote_copy(
        src_ref=src, dst_ref=dst, send_sem=ss, recv_sem=rs, device_id=to, device_id_type=MESH
    )
    copy.start()
    return copy


def aligned(index, size):
    return pl.ds(pl.multiple_of(index * size, size), size)


def mixer(
    n_sp, n_tp, after_ends, during,
    u_ref, res_ref, ls_ref, dec_ref, frq_ref, inr_ref, ini_ref, outr_ref, outi_ref,
    skip_ref, wglu_ref, bglu_ref, wbr_ref, gain_ref,
    normed_ref, stream_ref,
    wglu, wbr, res, coef, xr, xi, pr_all, pi_all, fin, fin_in, mo, rows_in, glu,
    load_sem, fs, fr, rs, rr,
):
    me_s, me_t = lax.axis_index("sp"), lax.axis_index("tp")
    tok, width = u_ref.shape
    groups, states = dec_ref.shape
    group = width // groups
    lanes = groups * states
    own = tok // n_tp
    loads = [
        pltpu.make_async_copy(
            res_ref.at[pl.ds(pl.multiple_of(me_t * own, own), own)], res, load_sem.at[0]
        ),
        pltpu.make_async_copy(wglu_ref, wglu, load_sem.at[1]),
        pltpu.make_async_copy(wbr_ref, wbr, load_sem.at[2]),
    ]
    for load in loads:
        load.start()

    same = lax.broadcasted_iota(jnp.int32, (groups, groups), 0) == lax.broadcasted_iota(
        jnp.int32, (groups, groups), 1
    )
    step = jnp.exp(jnp.sum(jnp.where(same, ls_ref[...], 0.0), axis=1, keepdims=True))
    dec, frq = dec_ref[...], frq_ref[...]
    mag = jnp.exp(dec * step)
    ar = mag * jnp.cos(frq * step)
    ai = mag * jnp.sin(frq * step)
    den = dec * dec + frq * frq
    less = ar - 1.0
    hr = (less * dec + ai * frq) / den
    hi = (ai * dec - less * frq) / den
    for g in range(groups):
        at = slice(g * states, (g + 1) * states)
        coef[0:1, at] = ar[g : g + 1, :]
        coef[1:2, at] = ai[g : g + 1, :]
        coef[2:3, at] = hr[g : g + 1, :]
        coef[3:4, at] = hi[g : g + 1, :]

    u = u_ref[...]
    part = 128
    spread = (
        lax.broadcasted_iota(jnp.int32, (states, part), 1) % states
        == lax.broadcasted_iota(jnp.int32, (states, part), 0)
    ).astype(BF16)
    rows_group = lax.broadcasted_iota(jnp.int32, (width, part), 0) // group
    lane_group = lax.broadcasted_iota(jnp.int32, (width, part), 1) // states

    def spread_out(ref):
        return jnp.dot(ref[...].astype(BF16), spread, preferred_element_type=F32)

    def only(wide, c):
        return jnp.where(rows_group == lane_group + c * (part // states), wide, 0.0).astype(BF16)

    in_r, in_i = spread_out(inr_ref), spread_out(ini_ref)
    row = lax.broadcasted_iota(jnp.int32, (tok, part), 0)
    row8 = lax.broadcasted_iota(jnp.int32, (8, part), 0)
    for c in range(lanes // part):
        at = slice(c * part, (c + 1) * part)
        vr = jnp.dot(u, only(in_r, c), preferred_element_type=F32)
        vi = jnp.dot(u, only(in_i, c), preferred_element_type=F32)
        cr, ci = coef[2:3, at], coef[3:4, at]
        sr, si = cr * vr - ci * vi, cr * vi + ci * vr
        pr, pi = coef[0:1, at], coef[1:2, at]
        tr, ti = jnp.ones((8, part), F32), jnp.zeros((8, part), F32)
        s = 1
        while s <= tok:
            if s <= 8:
                bit = ((row8 + 1) & s) != 0
                br, bi = jnp.where(bit, pr, 1.0), jnp.where(bit, pi, 0.0)
                tr, ti = tr * br - ti * bi, tr * bi + ti * br
            if s >= 8 and s < tok:
                tr, ti = (
                    jnp.concatenate([tr, tr * pr - ti * pi], 0),
                    jnp.concatenate([ti, tr * pi + ti * pr], 0),
                )
            if s < tok:
                if s < 8:
                    yr = jnp.where(row >= s, pltpu.roll(sr, s, 0), 0.0)
                    yi = jnp.where(row >= s, pltpu.roll(si, s, 0), 0.0)
                else:
                    gap = jnp.zeros((s, part), F32)
                    yr = jnp.concatenate([gap, sr[: tok - s]], 0)
                    yi = jnp.concatenate([gap, si[: tok - s]], 0)
                sr, si = sr + (pr * yr - pi * yi), si + (pr * yi + pi * yr)
            pr, pi = pr * pr - pi * pi, 2.0 * pr * pi
            s *= 2
        xr[:, at], xi[:, at] = sr, si
        pr_all[:, at], pi_all[:, at] = tr, ti
        fin[0:1, at] = sr[tok - 1 : tok]
        fin[1:2, at] = si[tok - 1 : tok]

    ends = []
    for d in range(1, n_sp):
        copy = pltpu.make_async_remote_copy(
            src_ref=fin, dst_ref=fin_in.at[d - 1], send_sem=fs.at[d - 1], recv_sem=fr.at[d - 1],
            device_id={"sp": lax.rem(me_s + d, n_sp)}, device_id_type=MESH,
        )
        copy.start()
        ends.append(copy)
    after_ends()

    out_r, out_i = spread_out(outr_ref), spread_out(outi_ref)
    outr = jnp.concatenate([only(out_r, c) for c in range(lanes // part)], axis=1)
    outi = jnp.concatenate([only(out_i, c) for c in range(lanes // part)], axis=1)
    for copy in ends:
        copy.wait()
    er, ei = pr_all[tok - 1 : tok, :], pi_all[tok - 1 : tok, :]
    pr, pi = jnp.ones((1, lanes), F32), jnp.zeros((1, lanes), F32)
    cr, ci = jnp.zeros((1, lanes), F32), jnp.zeros((1, lanes), F32)
    for d in range(1, n_sp):
        fr_, fi_ = fin_in[d - 1, 0:1, :], fin_in[d - 1, 1:2, :]
        reached = me_s >= d
        cr = cr + jnp.where(reached, pr * fr_ - pi * fi_, 0.0)
        ci = ci + jnp.where(reached, pr * fi_ + pi * fr_, 0.0)
        pr, pi = pr * er - pi * ei, pr * ei + pi * er
    tr, ti = pr_all[...], pi_all[...]
    sr = (xr[...] + (tr * cr - ti * ci)).astype(BF16)
    si = (xi[...] + (tr * ci + ti * cr)).astype(BF16)
    y = lax.dot_general(sr, outr, NT, preferred_element_type=F32) - lax.dot_general(
        si, outi, NT, preferred_element_type=F32
    )
    y = jax.nn.gelu(y + skip_ref[...] * u.astype(F32))
    mo[...] = y.astype(BF16).reshape(n_tp, own, width)
    turns = []
    for d in range(1, n_tp):
        to = lax.rem(me_t + d, n_tp)
        copy = pltpu.make_async_remote_copy(
            src_ref=mo.at[to], dst_ref=rows_in.at[d - 1], send_sem=rs.at[d - 1],
            recv_sem=rr.at[d - 1], device_id={"tp": to}, device_id_type=MESH,
        )
        copy.start()
        turns.append(copy)
    during()
    for load in loads:
        load.wait()

    def source(d):
        return pl.ds(pl.multiple_of(lax.rem(me_t + n_tp - d, n_tp) * width, width), width)

    blocks = [mo[me_t]]
    pre = bglu_ref[...] + jnp.dot(blocks[0], wglu[source(0), :], preferred_element_type=F32)
    for d in range(1, n_tp):
        turns[d - 1].wait()
        blocks.append(rows_in[d - 1])
        pre = pre + jnp.dot(blocks[d], wglu[source(d), :], preferred_element_type=F32)
    glu[...] = pre
    stream = res[...].astype(F32)
    for d in range(n_tp):
        gate = jax.nn.sigmoid(glu[:, source(d)])
        gated = (blocks[d].astype(F32) * gate).astype(BF16)
        stream = stream + jnp.dot(gated, wbr[source(d), :], preferred_element_type=F32)
    stream_ref[...] = stream
    scale = lax.rsqrt(jnp.mean(stream * stream, axis=-1, keepdims=True) + EPS)
    normed_ref[...] = (stream * scale * gain_ref[...]).astype(BF16)


TILE = 128


def layer_kernel(sizes, *refs):
    n_sp, n_tp = sizes["sp"], sizes["tp"]
    place = {axis: lax.axis_index(axis) for axis in sizes}
    me_g, me_s, me_t = place["grp"], place["sp"], place["tp"]
    wg_ref, wu_ref, wd_ref, out_ref = refs[14:18]
    x, stream, wgu, wd, acc, h = refs[18:24]
    keep, y1_out, y1_in, y2_out, y2_in, y3_out, y3_in, y4_out, y4_in = refs[24:33]
    (load_sem, ws, wr, fs, fr, az_s, az_r, ax_s, ax_r, am_s, am_r,
     s1, r1, s2, r2, s3, r3, s4, r4) = refs[33:52]
    mixer_scratch = refs[52:]
    own, d_model = stream.shape
    depth, hid = wg_ref.shape
    cols = wd_ref.shape[1]
    wide = wgu.shape[1] // 2
    rows = n_sp * n_tp * own
    parity = me_t % 2
    short = (n_sp - 1) * (1 - parity)
    half_row, half_col = depth // 2, cols // 2

    side = me_s // 2
    inner = me_s % 2 != side
    partner = me_s + 1 - 2 * (me_s % 2)
    opposite = lax.rem(me_s + 2, n_sp)
    near = [partner, 2 - side, 3 * (1 - side)]
    order = [me_s] + near
    mate = me_t + 1 - 2 * (me_t % 2)
    across = lax.rem(me_t + 2, n_tp)

    def sized(to, act):
        @pl.when(to == short)
        def _():
            act(wide - TILE)

        @pl.when(to != short)
        def _():
            act(wide)

    def first(to):
        return (3 * to - parity * ((to + 3) // 4)) * TILE

    def shipped(k, i, width):
        start = pl.ds(pl.multiple_of(first(near[i]), TILE), width)
        if k < 2:
            src = (wg_ref, wu_ref)[k].at[aligned(me_g, half_row), start]
            dst = wgu.at[aligned(2 * me_s + me_g, half_row), pl.ds(k * wide, width)]
        else:
            src = wd_ref.at[start, aligned(me_g, half_col)]
            dst = wd.at[pl.ds(0, width), aligned(2 * me_s + me_g, half_col)]
        return pltpu.make_async_remote_copy(
            src_ref=src, dst_ref=dst, send_sem=ws.at[k, i], recv_sem=wr.at[k, me_s],
            device_id={"sp": near[i]}, device_id_type=MESH,
        )

    def ship(k, i):
        sized(near[i], lambda width: shipped(k, i, width).start())

    def handed(k, i, width, g):
        at = 2 * near[i] + g
        if k < 2:
            piece = wgu.at[aligned(at, half_row), pl.ds(k * wide, width)]
        else:
            piece = wd.at[pl.ds(0, width), aligned(at, half_col)]
        return piece

    def passed(k, i, width):
        piece = handed(k, i, width, me_g)
        return pltpu.make_async_remote_copy(
            src_ref=piece, dst_ref=piece, send_sem=fs.at[k, i], recv_sem=fr.at[k, i],
            device_id={"grp": 1 - me_g}, device_id_type=MESH,
        )

    def relay(k, i):
        def act(width):
            piece = handed(k, i, width, me_g)
            pltpu.make_async_remote_copy(
                src_ref=piece, dst_ref=piece, send_sem=ws.at[k, i], recv_sem=wr.at[k, near[i]],
                device_id={"sp": near[i]}, device_id_type=MESH,
            ).wait_recv()
            passed(k, i, width).start()

        sized(me_s, act)

    def arrived(k, i):
        sized(me_s, lambda width: passed(k, i, width).wait_recv())

    def own_loads(width):
        start = pl.ds(pl.multiple_of(first(me_s), TILE), width)
        return [
            pltpu.make_async_copy(
                ref.at[:, start], wgu.at[aligned(me_s, depth), pl.ds(k * wide, width)],
                load_sem.at[k],
            )
            for k, ref in enumerate((wg_ref, wu_ref))
        ] + [
            pltpu.make_async_copy(
                wd_ref.at[start, :], wd.at[pl.ds(0, width), aligned(me_s, cols)], load_sem.at[2]
            )
        ]

    def start_loads(width):
        for load in own_loads(width):
            load.start()

    greet(sizes, place)
    ship(0, 0)
    sized(me_s, start_loads)

    @pl.when(me_s == short)
    def _():
        for k in range(2):
            wgu[:, (k + 1) * wide - TILE : (k + 1) * wide] = jnp.zeros((n_sp * depth, TILE), BF16)
        wd[wide - TILE :, :] = jnp.zeros((TILE, d_model), BF16)

    def after_ends():
        ship(1, 0)
        ship(0, 1)

    def during():
        relay(0, 0)

    mixer(
        n_sp, n_tp, after_ends, during, *refs[:14], x.at[me_s, 0], stream, *mixer_scratch
    )

    def along(b, n, to):
        return pltpu.make_async_remote_copy(
            src_ref=x.at[b, 0], dst_ref=x.at[b, 0], send_sem=az_s.at[n], recv_sem=az_r.at[b],
            device_id={"sp": to}, device_id_type=MESH,
        )

    sent = []

    def share(b):
        sent.append(send(x.at[b, 0], x.at[b, 2], ax_s.at[b], ax_r.at[b], tp=across))
        sent.append(send(x.at[b, 0], x.at[b, 1], am_s.at[b, 0], am_r.at[b, 0], tp=mate))

    def spread(b):
        pltpu.make_async_remote_copy(
            src_ref=x.at[b, 2], dst_ref=x.at[b, 2], send_sem=ax_s.at[b], recv_sem=ax_r.at[b],
            device_id={"tp": across}, device_id_type=MESH,
        ).wait_recv()
        sent.append(send(x.at[b, 2], x.at[b, 3], am_s.at[b, 1], am_r.at[b, 1], tp=mate))

    def collected(b):
        for n, slot in ((0, 1), (1, 3)):
            pltpu.make_async_remote_copy(
                src_ref=x.at[b, slot], dst_ref=x.at[b, slot], send_sem=am_s.at[b, n],
                recv_sem=am_r.at[b, n], device_id={"tp": mate}, device_id_type=MESH,
            ).wait_recv()

    along(me_s, 0, near[0]).start()
    along(me_s, 1, near[1]).start()
    for k, i in ((1, 1), (0, 2), (1, 2), (2, 0), (2, 1), (2, 2)):
        ship(k, i)
    share(me_s)
    relay(1, 0)
    relay(0, 1)
    for i in range(3):
        b = near[i]
        along(b, 0, near[0]).wait_recv()
        if i:
            @pl.when(inner)
            def _():
                along(b, 1 + i, near[0]).start()
        share(b)
    spread(order[0])
    spread(order[1])
    relay(1, 1)
    spread(order[2])
    spread(order[3])
    relay(0, 2)
    for b in order:
        collected(b)

    def product(b):
        lhs = x[:, :, :, aligned(b, depth)].reshape(rows, depth)
        return jnp.dot(lhs, wgu[aligned(b, depth), :], preferred_element_type=F32)

    def loaded(which):
        def act(width):
            loads = own_loads(width)
            for n in which:
                loads[n].wait()

        sized(me_s, act)

    loaded((0, 1))
    acc[...] = product(me_s)
    for i in range(2):
        for k in range(2):
            arrived(k, i)
        acc[...] += product(near[i])
        if i == 0:
            relay(1, 2)
    for k in range(2):
        arrived(k, 2)
    total = acc[...] + product(near[2])
    h[...] = (jax.nn.silu(total[:, :wide]) * total[:, wide:]).astype(BF16)

    def down(i):
        if i:
            relay(2, i - 1)
            arrived(2, i - 1)
        else:
            loaded((2,))
        y = jnp.dot(h[...], wd[:, aligned(order[i], cols)], preferred_element_type=F32)
        y = y.reshape(n_sp, n_tp, own, cols)
        y1_out[i, 0] = y[:, 1].astype(BF16)
        y1_out[i, 1] = y[:, 3].astype(BF16)
        sent.append(send(y1_out.at[i], y1_in.at[i], s1.at[i], r1.at[i], tp=mate))
        keep[i, 0] = y[:, 0]
        keep[i, 1] = y[:, 2]

    pairs, turns = {}, {}

    def stage_two(i):
        sent[firsts[i]].wait_recv()
        y2_out[i] = (keep[i, 1] + y1_in[i, 1].astype(F32)).astype(BF16)
        turns[i] = send(y2_out.at[i], y2_in.at[i], s2.at[i], r2.at[i], tp=across)
        keep[i, 0] += y1_in[i, 0].astype(F32)

    def stage_three(i):
        c = order[i]
        turns[i].wait_recv()
        keep[i, 0] += y2_in[i].astype(F32)
        for n, row in enumerate((partner, lax.rem(partner + 2, n_sp))):
            y3_out[c, n] = keep[i, 0, row].astype(BF16)
        pairs[i] = send(y3_out.at[c], y3_in.at[c], s3.at[c], r3.at[c], sp=partner)

    ends = {}

    def stage_four(i):
        c = order[i]
        pairs[i].wait_recv()
        y4_out[c] = (keep[i, 0, opposite] + y3_in[c, 1].astype(F32)).astype(BF16)
        ends[i] = send(y4_out.at[c], y4_in.at[c], s4.at[c], r4.at[c], sp=opposite)
        at = aligned(c, cols)
        stream[:, at] += keep[i, 0, me_s] + y3_in[c, 0].astype(F32)

    def finish(i):
        c = order[i]
        ends[i].wait_recv()
        at = aligned(c, cols)
        out_ref[:, at] = (stream[:, at] + y4_in[c].astype(F32)).astype(BF16)

    firsts = {}
    for step in range(n_sp):
        firsts[step] = len(sent)
        down(step)
        if step >= 1:
            stage_two(step - 1)
        if step >= 2:
            stage_three(step - 2)
    stage_two(3)
    stage_three(2)
    stage_four(0)
    stage_four(1)
    stage_three(3)
    stage_four(2)
    stage_four(3)
    for i in range(n_sp):
        finish(i)

    for copy in sent + [d[i] for d in (turns, pairs, ends) for i in range(n_sp)]:
        copy.wait_send()
    along(me_s, 0, near[0]).wait_send()
    along(me_s, 1, near[1]).wait_send()

    @pl.when(inner)
    def _():
        for n in (2, 3):
            along(me_s, n, near[0]).wait_send()

    for k in range(3):
        for i in range(3):
            sized(near[i], lambda width: shipped(k, i, width).wait_send())
            sized(me_s, lambda width: passed(k, i, width).wait_send())


def moved_weights(
    ssm_input, residual_in, log_step, decay_real, freq, in_real, in_imag, out_real, out_imag,
    skip, w_glu, b_glu, w_branch, norm_gain, w_gate, w_up, w_down,
):
    sizes = {axis: lax.axis_size(axis) for axis in ("grp", "sp", "tp")}
    n_sp, n_tp = sizes["sp"], sizes["tp"]
    tok, width = ssm_input.shape
    groups, states = decay_real.shape
    group = in_real.shape[2]
    lanes = groups * states
    own = tok // n_tp
    chan, d_model = w_branch.shape
    depth, hid = w_gate.shape
    cols = w_down.shape[1]
    wide = -(-hid // (TILE * n_sp)) * TILE
    rows = n_sp * tok
    vm = pl.BlockSpec(memory_space=pltpu.VMEM)
    hbm = pl.BlockSpec(memory_space=pl.ANY)
    dma = pltpu.SemaphoreType.DMA
    vmem = pltpu.VMEM
    return pl.pallas_call(
        functools.partial(layer_kernel, sizes),
        out_shape=jax.ShapeDtypeStruct((own, d_model), BF16),
        in_specs=[vm, hbm] + [vm] * 8 + [hbm, vm, hbm, vm] + [hbm] * 3,
        out_specs=vm,
        scratch_shapes=[
            vmem((n_sp, n_tp, own, d_model), BF16),
            vmem((own, d_model), F32),
            vmem((d_model, 2 * wide), BF16),
            vmem((wide, d_model), BF16),
            vmem((rows, 2 * wide), F32),
            vmem((rows, wide), BF16),
            vmem((n_sp, 2, n_sp, own, cols), F32),
            vmem((n_sp, 2, n_sp, own, cols), BF16),
            vmem((n_sp, 2, n_sp, own, cols), BF16),
            vmem((n_sp, n_sp, own, cols), BF16),
            vmem((n_sp, n_sp, own, cols), BF16),
            vmem((n_sp, 2, own, cols), BF16),
            vmem((n_sp, 2, own, cols), BF16),
            vmem((n_sp, own, cols), BF16),
            vmem((n_sp, own, cols), BF16),
            dma((3,)),
            dma((3, 3)), dma((3, n_sp)), dma((3, 3)), dma((3, 3)),
            dma((4,)), dma((n_sp,)),
            dma((n_sp,)), dma((n_sp,)),
            dma((n_sp, 2)), dma((n_sp, 2)),
            dma((n_sp,)), dma((n_sp,)), dma((n_sp,)), dma((n_sp,)),
            dma((n_sp,)), dma((n_sp,)), dma((n_sp,)), dma((n_sp,)),
            vmem((chan, chan), BF16),
            vmem((chan, d_model), BF16),
            vmem((own, d_model), BF16),
            vmem((8, lanes), F32),
            vmem((tok, lanes), F32),
            vmem((tok, lanes), F32),
            vmem((tok, lanes), F32),
            vmem((tok, lanes), F32),
            vmem((2, lanes), F32),
            vmem((n_sp - 1, 2, lanes), F32),
            vmem((n_tp, own, width), BF16),
            vmem((n_tp - 1, own, width), BF16),
            vmem((own, chan), F32),
            dma((3,)),
            dma((n_sp - 1,)), dma((n_sp - 1,)),
            dma((n_tp - 1,)), dma((n_tp - 1,)),
        ],
        compiler_params=pltpu.CompilerParams(collective_id=0, has_side_effects=True),
        name="layer",
    )(
        ssm_input, residual_in, log_step[None], decay_real, freq,
        in_real.swapaxes(1, 2).reshape(width, states),
        in_imag.swapaxes(1, 2).reshape(width, states),
        out_real.reshape(width, states), out_imag.reshape(width, states),
        skip[None], w_glu, b_glu[None], w_branch, norm_gain[None], w_gate, w_up, w_down,
    )


def per_device(*arguments):
    sizes = tuple(lax.axis_size(axis) for axis in ("grp", "sp", "tp"))
    tiles = arguments[14].shape[1] // TILE
    fits = sizes == (2, 4, 4) and tiles % 4 == 3
    return (moved_weights if fits else gathered_weights)(*arguments)


def solution(mesh):
    placed = (
        P(("grp", "sp"), "tp"),
        P(("grp", "sp"), None),
        P("tp"),
        P("tp", None),
        P("tp", None),
        P("tp", None, None),
        P("tp", None, None),
        P("tp", None, None),
        P("tp", None, None),
        P("tp"),
        P(),
        P(),
        P(),
        P(),
        P("sp", "tp"),
        P("sp", "tp"),
        P("tp", "sp"),
    )
    return jax.shard_map(
        per_device,
        mesh=mesh,
        in_specs=placed,
        out_specs=P(("grp", "sp", "tp"), None),
        check_vma=False,
    )
```

```python
import functools
import math

import jax
import jax.numpy as jnp
from jax import lax
from jax.experimental import pallas as pl
from jax.experimental.pallas import tpu as pltpu
from jax.sharding import PartitionSpec as P

EPS = 1e-06


def prefix(shard, axis, combine, identity):
    count, place = (lax.axis_size(axis), lax.axis_index(axis))
    everything = jax.tree.map(lambda part: lax.all_gather(part, axis), shard)
    start = jax.tree.map(
        lambda part, zero: jnp.broadcast_to(jnp.asarray(zero, part.dtype), part.shape),
        shard,
        identity,
    )

    def lap(k, before):
        reached = k < place
        new = combine(before, jax.tree.map(lambda part: part[k], everything))
        return jax.tree.map(lambda a, b: jnp.where(reached, a, b), new, before)

    return lax.fori_loop(0, count, lap, start)


def discretize(log_step, decay_real, freq, in_real, in_imag):
    step_size = jnp.exp(log_step)[:, None]
    magnitude = jnp.exp(decay_real * step_size)
    abar_re = magnitude * jnp.cos(freq * step_size)
    abar_im = magnitude * jnp.sin(freq * step_size)
    denominator = decay_real * decay_real + freq * freq
    less_re = abar_re - 1.0
    hold_re = ((less_re * decay_real + abar_im * freq) / denominator)[..., None]
    hold_im = ((abar_im * decay_real - less_re * freq) / denominator)[..., None]
    bbar_re = hold_re * in_real - hold_im * in_imag
    bbar_im = hold_re * in_imag + hold_im * in_real
    return (step_size, abar_re, abar_im, bbar_re, bbar_im)


def powers(decay_real, freq, step_size, length):
    steps_up = (jnp.arange(length, dtype=jnp.int32) + 1).astype(jnp.float32)[:, None, None]
    magnitude = jnp.exp((decay_real * step_size)[None] * steps_up)
    phase = (freq * step_size)[None] * steps_up
    return (magnitude * jnp.cos(phase), magnitude * jnp.sin(phase))


def compose(earlier, later):
    a1r, a1i, b1r, b1i = earlier
    a2r, a2i, b2r, b2i = later
    return (
        a2r * a1r - a2i * a1i,
        a2r * a1i + a2i * a1r,
        a2r * b1r - a2i * b1i + b2r,
        a2r * b1i + a2i * b1r + b2i,
    )


def local_states(inputs, decay_real, freq, step_size, bbar_re, bbar_im):
    highest = lax.Precision.HIGHEST
    tok_rows, group_count, unused = inputs.shape
    lanes = group_count * decay_real.shape[1]
    drive_re = jnp.einsum("lgm,gpm->lgp", inputs, bbar_re, precision=highest).reshape(
        tok_rows, lanes
    )
    drive_im = jnp.einsum("lgm,gpm->lgp", inputs, bbar_im, precision=highest).reshape(
        tok_rows, lanes
    )
    span = math.gcd(tok_rows, 16)
    spans = tok_rows // span
    rate = (decay_real * step_size).reshape(lanes)
    turn = (freq * step_size).reshape(lanes)
    later = jnp.arange(span, dtype=jnp.int32)[:, None]
    earlier = jnp.arange(span, dtype=jnp.int32)[None, :]
    lag = (later - earlier).astype(jnp.float32)
    causal = (later >= earlier)[..., None]
    lag_pos = jnp.maximum(lag, 0.0)[..., None]
    table_mag = jnp.exp(rate[None, None] * lag_pos)
    table_re = jnp.where(causal, table_mag * jnp.cos(turn[None, None] * lag_pos), 0.0)
    table_im = jnp.where(causal, table_mag * jnp.sin(turn[None, None] * lag_pos), 0.0)
    block_re = drive_re.reshape(spans, 1, span, lanes)
    block_im = drive_im.reshape(spans, 1, span, lanes)
    inner_re = jnp.sum(table_re[None] * block_re - table_im[None] * block_im, axis=2)
    inner_im = jnp.sum(table_re[None] * block_im + table_im[None] * block_re, axis=2)
    steps_up = (jnp.arange(span, dtype=jnp.int32) + 1).astype(jnp.float32)[:, None]
    pow_mag = jnp.exp(rate[None] * steps_up)
    pow_re = pow_mag * jnp.cos(turn[None] * steps_up)
    pow_im = pow_mag * jnp.sin(turn[None] * steps_up)
    span_re = pow_re[-1]
    span_im = pow_im[-1]

    def carry_step(entering, ends):
        next_re = span_re * entering[0] - span_im * entering[1] + ends[0]
        next_im = span_re * entering[1] + span_im * entering[0] + ends[1]
        return ((next_re, next_im), entering)

    zeros = jnp.zeros((lanes,), jnp.float32)
    unused_carry, entering = lax.scan(
        carry_step, (zeros, zeros), (inner_re[:, -1], inner_im[:, -1])
    )
    state_re = inner_re + pow_re[None] * entering[0][:, None] - pow_im[None] * entering[1][:, None]
    state_im = inner_im + pow_re[None] * entering[1][:, None] + pow_im[None] * entering[0][:, None]
    shape = (tok_rows, group_count, decay_real.shape[1])
    return (state_re.reshape(shape), state_im.reshape(shape))


def readout(state_re, state_im, out_real, out_imag, skip_mat, inputs):
    highest = lax.Precision.HIGHEST
    values = (
        jnp.einsum("lgp,gmp->lgm", state_re, out_real, precision=highest)
        - jnp.einsum("lgp,gmp->lgm", state_im, out_imag, precision=highest)
        + skip_mat[None] * inputs
    )
    values = jax.nn.gelu(values)
    return values.reshape(values.shape[0], -1).astype(jnp.bfloat16)


def row_norm(stream, norm_gain):
    scale_rows = lax.rsqrt(jnp.mean(stream * stream, axis=-1, keepdims=True) + EPS)
    return (stream * scale_rows * norm_gain).astype(jnp.bfloat16)


def gathered_weights(
    ssm_input,
    residual_in,
    log_step,
    decay_real,
    freq,
    in_real,
    in_imag,
    out_real,
    out_imag,
    skip,
    w_glu,
    b_glu,
    w_branch,
    norm_gain,
    w_gate,
    w_up,
    w_down,
):
    tok_rows, width_local = ssm_input.shape
    group_count = log_step.shape[0]
    group_size = in_real.shape[2]
    tp_count = lax.axis_size("tp")
    tp_index = lax.axis_index("tp")
    own_rows = tok_rows // tp_count
    step_size, abar_re, abar_im, bbar_re, bbar_im = discretize(
        log_step, decay_real, freq, in_real, in_imag
    )
    pow_re, pow_im = powers(decay_real, freq, step_size, tok_rows)
    inputs = ssm_input.astype(jnp.float32).reshape(tok_rows, group_count, group_size)
    local_re, local_im = local_states(inputs, decay_real, freq, step_size, bbar_re, bbar_im)
    identity = (
        jnp.ones_like(abar_re),
        jnp.zeros_like(abar_re),
        jnp.zeros_like(abar_re),
        jnp.zeros_like(abar_re),
    )
    carried = prefix((pow_re[-1], pow_im[-1], local_re[-1], local_im[-1]), "sp", compose, identity)
    state_re = local_re + pow_re * carried[2][None] - pow_im * carried[3][None]
    state_im = local_im + pow_re * carried[3][None] + pow_im * carried[2][None]
    mixer_out = readout(
        state_re, state_im, out_real, out_imag, skip.reshape(group_count, group_size), inputs
    )
    mixer_rows = lax.all_to_all(mixer_out, "tp", split_axis=0, concat_axis=1, tiled=True)
    glu_pre = jnp.dot(mixer_rows, w_glu, preferred_element_type=jnp.float32) + b_glu
    gated = (mixer_rows.astype(jnp.float32) * jax.nn.sigmoid(glu_pre)).astype(jnp.bfloat16)
    residual_own = lax.dynamic_slice_in_dim(residual_in, tp_index * own_rows, own_rows, 0)
    stream = residual_own.astype(jnp.float32) + jnp.dot(
        gated, w_branch, preferred_element_type=jnp.float32
    )
    normed = row_norm(stream, norm_gain)
    normed_all = lax.all_gather(normed, "tp", axis=0, tiled=True)
    gate_sum = jnp.dot(
        normed_all,
        lax.all_gather(w_gate, "sp", axis=0, tiled=True),
        preferred_element_type=jnp.float32,
    )
    up_sum = jnp.dot(
        normed_all,
        lax.all_gather(w_up, "sp", axis=0, tiled=True),
        preferred_element_type=jnp.float32,
    )
    hidden = (jax.nn.silu(gate_sum) * up_sum).astype(jnp.bfloat16)
    down_whole = lax.all_gather(w_down, "sp", axis=1, tiled=True)
    summed = lax.psum_scatter(
        jnp.dot(hidden, down_whole, preferred_element_type=jnp.float32).astype(jnp.bfloat16),
        "tp",
        scatter_dimension=0,
        tiled=True,
    ).astype(jnp.float32)
    return (stream + summed).astype(jnp.bfloat16)


MESH = pl.DeviceIdType.MESH
F32 = jnp.float32
BF16 = jnp.bfloat16
NT = (((1,), (1,)), ((), ()))


def greet(sizes, place):
    barrier = pltpu.get_barrier_semaphore()
    for axis in sizes:
        for d in range(1, sizes[axis]):
            pl.semaphore_signal(
                barrier, inc=1, device_id={axis: lax.rem(place[axis] + d, sizes[axis])},
                device_id_type=MESH,
            )
    pl.semaphore_wait(barrier, sum(sizes.values()) - len(sizes))


def send(src, dst, ss, rs, **to):
    copy = pltpu.make_async_remote_copy(
        src_ref=src, dst_ref=dst, send_sem=ss, recv_sem=rs, device_id=to, device_id_type=MESH
    )
    copy.start()
    return copy


def aligned(index, size):
    return pl.ds(pl.multiple_of(index * size, size), size)


def mixer(
    n_sp, n_tp, after_ends,
    u_ref, res_ref, ls_ref, dec_ref, frq_ref, inr_ref, ini_ref, outr_ref, outi_ref,
    skip_ref, wglu_ref, bglu_ref, wbr_ref, gain_ref,
    normed_ref, stream_ref,
    wglu, wbr, res, coef, xr, xi, pr_all, pi_all, fin, fin_in, mo, rows_in, glu,
    load_sem, fs, fr, rs, rr,
):
    me_s, me_t = lax.axis_index("sp"), lax.axis_index("tp")
    tok, width = u_ref.shape
    groups, states = dec_ref.shape
    group = width // groups
    lanes = groups * states
    own = tok // n_tp
    loads = [
        pltpu.make_async_copy(
            res_ref.at[pl.ds(pl.multiple_of(me_t * own, own), own)], res, load_sem.at[0]
        ),
        pltpu.make_async_copy(wglu_ref, wglu, load_sem.at[1]),
        pltpu.make_async_copy(wbr_ref, wbr, load_sem.at[2]),
    ]
    for load in loads:
        load.start()

    same = lax.broadcasted_iota(jnp.int32, (groups, groups), 0) == lax.broadcasted_iota(
        jnp.int32, (groups, groups), 1
    )
    step = jnp.exp(jnp.sum(jnp.where(same, ls_ref[...], 0.0), axis=1, keepdims=True))
    dec, frq = dec_ref[...], frq_ref[...]
    mag = jnp.exp(dec * step)
    ar = mag * jnp.cos(frq * step)
    ai = mag * jnp.sin(frq * step)
    den = dec * dec + frq * frq
    less = ar - 1.0
    hr = (less * dec + ai * frq) / den
    hi = (ai * dec - less * frq) / den
    for g in range(groups):
        at = slice(g * states, (g + 1) * states)
        coef[0:1, at] = ar[g : g + 1, :]
        coef[1:2, at] = ai[g : g + 1, :]
        coef[2:3, at] = hr[g : g + 1, :]
        coef[3:4, at] = hi[g : g + 1, :]

    u = u_ref[...]
    part = 128
    spread = (
        lax.broadcasted_iota(jnp.int32, (states, part), 1) % states
        == lax.broadcasted_iota(jnp.int32, (states, part), 0)
    ).astype(BF16)
    rows_group = lax.broadcasted_iota(jnp.int32, (width, part), 0) // group
    lane_group = lax.broadcasted_iota(jnp.int32, (width, part), 1) // states

    def spread_out(ref):
        return jnp.dot(ref[...].astype(BF16), spread, preferred_element_type=F32)

    def only(wide, c):
        return jnp.where(rows_group == lane_group + c * (part // states), wide, 0.0).astype(BF16)

    in_r, in_i = spread_out(inr_ref), spread_out(ini_ref)
    row = lax.broadcasted_iota(jnp.int32, (tok, part), 0)
    row8 = lax.broadcasted_iota(jnp.int32, (8, part), 0)
    for c in range(lanes // part):
        at = slice(c * part, (c + 1) * part)
        vr = jnp.dot(u, only(in_r, c), preferred_element_type=F32)
        vi = jnp.dot(u, only(in_i, c), preferred_element_type=F32)
        cr, ci = coef[2:3, at], coef[3:4, at]
        sr, si = cr * vr - ci * vi, cr * vi + ci * vr
        pr, pi = coef[0:1, at], coef[1:2, at]
        tr, ti = jnp.ones((8, part), F32), jnp.zeros((8, part), F32)
        s = 1
        while s <= tok:
            if s <= 8:
                bit = ((row8 + 1) & s) != 0
                br, bi = jnp.where(bit, pr, 1.0), jnp.where(bit, pi, 0.0)
                tr, ti = tr * br - ti * bi, tr * bi + ti * br
            if s >= 8 and s < tok:
                tr, ti = (
                    jnp.concatenate([tr, tr * pr - ti * pi], 0),
                    jnp.concatenate([ti, tr * pi + ti * pr], 0),
                )
            if s < tok:
                if s < 8:
                    yr = jnp.where(row >= s, pltpu.roll(sr, s, 0), 0.0)
                    yi = jnp.where(row >= s, pltpu.roll(si, s, 0), 0.0)
                else:
                    gap = jnp.zeros((s, part), F32)
                    yr = jnp.concatenate([gap, sr[: tok - s]], 0)
                    yi = jnp.concatenate([gap, si[: tok - s]], 0)
                sr, si = sr + (pr * yr - pi * yi), si + (pr * yi + pi * yr)
            pr, pi = pr * pr - pi * pi, 2.0 * pr * pi
            s *= 2
        xr[:, at], xi[:, at] = sr, si
        pr_all[:, at], pi_all[:, at] = tr, ti
        fin[0:1, at] = sr[tok - 1 : tok]
        fin[1:2, at] = si[tok - 1 : tok]

    def end_to(d):
        return pltpu.make_async_remote_copy(
            src_ref=fin, dst_ref=fin_in.at[d - 1], send_sem=fs.at[d - 1], recv_sem=fr.at[d - 1],
            device_id={"sp": lax.rem(me_s + d, n_sp)}, device_id_type=MESH,
        )

    for d in range(1, n_sp):
        @pl.when(me_s + d < n_sp)
        def _():
            end_to(d).start()
    after_ends()

    out_r, out_i = spread_out(outr_ref), spread_out(outi_ref)
    outr = jnp.concatenate([only(out_r, c) for c in range(lanes // part)], axis=1)
    outi = jnp.concatenate([only(out_i, c) for c in range(lanes // part)], axis=1)
    for d in range(1, n_sp):
        @pl.when(me_s >= d)
        def _():
            end_to(d).wait_recv()
    er, ei = pr_all[tok - 1 : tok, :], pi_all[tok - 1 : tok, :]
    pr, pi = jnp.ones((1, lanes), F32), jnp.zeros((1, lanes), F32)
    cr, ci = jnp.zeros((1, lanes), F32), jnp.zeros((1, lanes), F32)
    for d in range(1, n_sp):
        fr_, fi_ = fin_in[d - 1, 0:1, :], fin_in[d - 1, 1:2, :]
        reached = me_s >= d
        cr = cr + jnp.where(reached, pr * fr_ - pi * fi_, 0.0)
        ci = ci + jnp.where(reached, pr * fi_ + pi * fr_, 0.0)
        pr, pi = pr * er - pi * ei, pr * ei + pi * er
    tr, ti = pr_all[...], pi_all[...]
    sr = (xr[...] + (tr * cr - ti * ci)).astype(BF16)
    si = (xi[...] + (tr * ci + ti * cr)).astype(BF16)
    y = lax.dot_general(sr, outr, NT, preferred_element_type=F32) - lax.dot_general(
        si, outi, NT, preferred_element_type=F32
    )
    for d in range(1, n_sp):
        @pl.when(me_s + d < n_sp)
        def _():
            end_to(d).wait_send()
    y = jax.nn.gelu(y + skip_ref[...] * u.astype(F32))
    mo[...] = y.astype(BF16).reshape(n_tp, own, width)
    turns = []
    for d in range(1, n_tp):
        to = lax.rem(me_t + d, n_tp)
        copy = pltpu.make_async_remote_copy(
            src_ref=mo.at[to], dst_ref=rows_in.at[d - 1], send_sem=rs.at[d - 1],
            recv_sem=rr.at[d - 1], device_id={"tp": to}, device_id_type=MESH,
        )
        copy.start()
        turns.append(copy)
    for load in loads:
        load.wait()

    def source(d):
        return pl.ds(pl.multiple_of(lax.rem(me_t + n_tp - d, n_tp) * width, width), width)

    blocks = [mo[me_t]]
    pre = bglu_ref[...] + jnp.dot(blocks[0], wglu[source(0), :], preferred_element_type=F32)
    for d in range(1, n_tp):
        turns[d - 1].wait()
        blocks.append(rows_in[d - 1])
        pre = pre + jnp.dot(blocks[d], wglu[source(d), :], preferred_element_type=F32)
    glu[...] = pre
    stream = res[...].astype(F32)
    for d in range(n_tp):
        gate = jax.nn.sigmoid(glu[:, source(d)])
        gated = (blocks[d].astype(F32) * gate).astype(BF16)
        stream = stream + jnp.dot(gated, wbr[source(d), :], preferred_element_type=F32)
    stream_ref[...] = stream
    scale = lax.rsqrt(jnp.mean(stream * stream, axis=-1, keepdims=True) + EPS)
    normed_ref[...] = (stream * scale * gain_ref[...]).astype(BF16)


TILE = 128


def layer_kernel(sizes, *refs):
    n_sp, n_tp = sizes["sp"], sizes["tp"]
    place = {axis: lax.axis_index(axis) for axis in sizes}
    me_g, me_s, me_t = place["grp"], place["sp"], place["tp"]
    wg_ref, wu_ref, wd_ref, out_ref = refs[14:18]
    x, stream, wgu, wd, acc, h = refs[18:24]
    keep, y1_out, y1_in, y2_out, y2_in, y3_out, y3_in, y4_out, y4_in = refs[24:33]
    (load_sem, ws, wr, fs, fr, az_s, az_r, ax_s, ax_r, am_s, am_r,
     s1, r1, s2, r2, s3, r3, s4, r4, met) = refs[33:53]
    mixer_scratch = refs[53:]
    own, d_model = stream.shape
    depth, hid = wg_ref.shape
    cols = wd_ref.shape[1]
    wide = wgu.shape[1] // 2
    rows = n_sp * n_tp * own
    parity = me_t % 2
    short = (n_sp - 1) * (1 - parity)
    half_row, part_col = depth // 2, cols // 4
    half_col = 2 * part_col

    side = me_s // 2
    inner = me_s % 2 != side
    partner = me_s + 1 - 2 * (me_s % 2)
    opposite = lax.rem(me_s + 2, n_sp)
    near = [partner, 2 - side, 3 * (1 - side)]
    order = [me_s] + near
    mate = me_t + 1 - 2 * (me_t % 2)
    across = lax.rem(me_t + 2, n_tp)

    def sized(to, act):
        @pl.when(to == short)
        def _():
            act(wide - TILE)

        @pl.when(to != short)
        def _():
            act(wide)

    def first(to):
        return (3 * to - parity * ((to + 3) // 4)) * TILE

    def shipped(k, i, width):
        start = pl.ds(pl.multiple_of(first(near[i]), TILE), width)
        if k < 2:
            src = (wg_ref, wu_ref)[k].at[aligned(me_g, half_row), start]
            dst = wgu.at[aligned(2 * me_s + me_g, half_row), pl.ds(k * wide, width)]
        else:
            at = 2 * (k - 2) + me_g
            src = wd_ref.at[start, aligned(at, part_col)]
            dst = wd.at[pl.ds(0, width), aligned(4 * me_s + at, part_col)]
        return pltpu.make_async_remote_copy(
            src_ref=src, dst_ref=dst, send_sem=ws.at[k, i], recv_sem=wr.at[k, me_s],
            device_id={"sp": near[i]}, device_id_type=MESH,
        )

    def ship(k, i):
        sized(near[i], lambda width: shipped(k, i, width).start())

    def handed(k, i, width):
        if k < 2:
            return wgu.at[aligned(2 * near[i] + me_g, half_row), pl.ds(k * wide, width)]
        at = 4 * near[i] + 2 * (k - 2) + me_g
        return wd.at[pl.ds(0, width), aligned(at, part_col)]

    def passed(k, i, width):
        piece = handed(k, i, width)
        return pltpu.make_async_remote_copy(
            src_ref=piece, dst_ref=piece, send_sem=fs.at[k, i], recv_sem=fr.at[k, i],
            device_id={"grp": 1 - me_g}, device_id_type=MESH,
        )

    def relay(k, i):
        def act(width):
            piece = handed(k, i, width)
            pltpu.make_async_remote_copy(
                src_ref=piece, dst_ref=piece, send_sem=ws.at[k, i], recv_sem=wr.at[k, near[i]],
                device_id={"sp": near[i]}, device_id_type=MESH,
            ).wait_recv()
            passed(k, i, width).start()

        sized(me_s, act)

    def arrived(k, i):
        sized(me_s, lambda width: passed(k, i, width).wait_recv())

    def own_loads(width):
        start = pl.ds(pl.multiple_of(first(me_s), TILE), width)
        return [
            pltpu.make_async_copy(
                ref.at[:, start], wgu.at[aligned(me_s, depth), pl.ds(k * wide, width)],
                load_sem.at[k],
            )
            for k, ref in enumerate((wg_ref, wu_ref))
        ] + [
            pltpu.make_async_copy(
                wd_ref.at[start, :], wd.at[pl.ds(0, width), aligned(me_s, cols)], load_sem.at[2]
            )
        ]

    def start_loads(width):
        for load in own_loads(width):
            load.start()

    edge = jnp.logical_not(inner)

    def issue(at_inner, at_edge):
        for where, jobs in ((inner, at_inner), (edge, at_edge)):
            @pl.when(where)
            def _():
                for act, k, i in jobs:
                    act(k, i)

    ends_in = mixer_scratch[9]
    ends_in[...] = jnp.zeros_like(ends_in)
    greet(sizes, place)
    issue([(ship, 0, 0), (ship, 0, 1)], [(ship, 0, 0)])
    sized(me_s, start_loads)

    @pl.when(me_s == short)
    def _():
        for k in range(2):
            wgu[:, (k + 1) * wide - TILE : (k + 1) * wide] = jnp.zeros((n_sp * depth, TILE), BF16)
        wd[wide - TILE :, :] = jnp.zeros((TILE, d_model), BF16)

    def after_ends():
        ship(1, 0)
        ship(0, 2)

    mixer(
        n_sp, n_tp, after_ends, *refs[:14], x.at[me_s, 0], stream, *mixer_scratch
    )

    def along(b, n, to):
        return pltpu.make_async_remote_copy(
            src_ref=x.at[b, 0], dst_ref=x.at[b, 0], send_sem=az_s.at[n], recv_sem=az_r.at[b],
            device_id={"sp": to}, device_id_type=MESH,
        )

    sent = []

    def share(b):
        sent.append(send(x.at[b, 0], x.at[b, 2], ax_s.at[b], ax_r.at[b], tp=across))
        sent.append(send(x.at[b, 0], x.at[b, 1], am_s.at[b, 0], am_r.at[b, 0], tp=mate))

    def spread(b):
        pltpu.make_async_remote_copy(
            src_ref=x.at[b, 2], dst_ref=x.at[b, 2], send_sem=ax_s.at[b], recv_sem=ax_r.at[b],
            device_id={"tp": across}, device_id_type=MESH,
        ).wait_recv()
        sent.append(send(x.at[b, 2], x.at[b, 3], am_s.at[b, 1], am_r.at[b, 1], tp=mate))

    def collected(b):
        for n, slot in ((0, 1), (1, 3)):
            pltpu.make_async_remote_copy(
                src_ref=x.at[b, slot], dst_ref=x.at[b, slot], send_sem=am_s.at[b, n],
                recv_sem=am_r.at[b, n], device_id={"tp": mate}, device_id_type=MESH,
            ).wait_recv()

    def meet(n):
        pl.semaphore_signal(met.at[n], inc=1, device_id={"tp": mate}, device_id_type=MESH)
        pl.semaphore_wait(met.at[n], 1)

    def gone(k, i):
        sized(near[i], lambda width: shipped(k, i, width).wait_send())

    firsthand = [along(me_s, i, near[i]) for i in range(2)]
    for copy in firsthand:
        copy.start()
    share(me_s)

    def gathered(i):
        b = near[i]
        along(b, 0, near[0]).wait_recv()
        if i:
            @pl.when(inner)
            def _():
                along(b, 1 + i, near[0]).start()
        share(b)

    issue([(relay, 0, 1)], [])
    relay(0, 0)
    for copy in firsthand:
        copy.wait_send()
    meet(0)
    ship(1, 2)
    issue([], [(ship, 0, 1)])
    ship(1, 1)
    issue([], [(ship, 2, 0), (ship, 3, 0)])
    relay(1, 0)
    spread(order[0])
    issue([], [(relay, 0, 1)])
    gathered(0)
    issue([], [(relay, 0, 2)])
    gathered(1)
    spread(order[1])
    gathered(2)
    issue([], [(relay, 1, 2)])
    spread(order[2])
    spread(order[3])
    issue([(relay, 0, 2)], [])
    for b in order:
        collected(b)

    def product(b):
        lhs = x[:, :, :, aligned(b, depth)].reshape(rows, depth)
        return jnp.dot(lhs, wgu[aligned(b, depth), :], preferred_element_type=F32)

    def loaded(which):
        def act(width):
            loads = own_loads(width)
            for n in which:
                loads[n].wait()

        sized(me_s, act)

    def landed(i):
        for k in range(2):
            arrived(k, i)

    loaded((0, 1))
    acc[...] = product(me_s)
    landed(0)
    acc[...] += product(near[0])
    issue([(relay, 1, 2), (relay, 1, 1)], [(relay, 1, 1)])

    def release():
        issue([], [(gone, 0, 1)])
        gone(1, 1)
        gone(1, 2)
        meet(1)
        issue([(ship, 2, 0), (ship, 3, 0)], [])
        for i in (2, 1):
            for k in (2, 3):
                ship(k, i)

    pl.when(inner)(release)
    landed(2)
    acc[...] += product(near[2])
    issue([(relay, 2, 0), (relay, 3, 0)], [])
    landed(1)
    total = acc[...] + product(near[1])
    h[...] = (jax.nn.silu(total[:, :wide]) * total[:, wide:]).astype(BF16)

    blocks = [(i, q) for i in (0, 1, 3, 2) for q in range(2)]

    def place_of(n):
        i, q = blocks[n]
        return 2 * order[i] + q

    firsts, turns, pairs, ends = {}, {}, {}, {}

    def down(n):
        i, q = blocks[n]
        if i:
            arrived(2 + q, i - 1)
        y = jnp.dot(h[...], wd[:, aligned(place_of(n), half_col)], preferred_element_type=F32)
        y = y.reshape(n_sp, n_tp, own, half_col)
        y1_out[n, 0] = y[:, 1].astype(BF16)
        y1_out[n, 1] = y[:, 3].astype(BF16)
        firsts[n] = send(y1_out.at[n], y1_in.at[n], s1.at[n], r1.at[n], tp=mate)
        keep[n, 0] = y[:, 0]
        keep[n, 1] = y[:, 2]

    def stage_two(n):
        firsts[n].wait_recv()
        y2_out[n] = (keep[n, 1] + y1_in[n, 1].astype(F32)).astype(BF16)
        turns[n] = send(y2_out.at[n], y2_in.at[n], s2.at[n], r2.at[n], tp=across)
        keep[n, 0] += y1_in[n, 0].astype(F32)

    def stage_three(n):
        c = place_of(n)
        turns[n].wait_recv()
        keep[n, 0] += y2_in[n].astype(F32)
        for m, row in enumerate((partner, lax.rem(partner + 2, n_sp))):
            y3_out[c, m] = keep[n, 0, row].astype(BF16)
        pairs[n] = send(y3_out.at[c], y3_in.at[c], s3.at[c], r3.at[c], sp=partner)

    def stage_four(n):
        c = place_of(n)
        pairs[n].wait_recv()
        y4_out[c] = (keep[n, 0, opposite] + y3_in[c, 1].astype(F32)).astype(BF16)
        ends[n] = send(y4_out.at[c], y4_in.at[c], s4.at[c], r4.at[c], sp=opposite)
        at = aligned(c, half_col)
        stream[:, at] += keep[n, 0, me_s] + y3_in[c, 0].astype(F32)

    def finish(n):
        c = place_of(n)
        ends[n].wait_recv()
        at = aligned(c, half_col)
        out_ref[:, at] = (stream[:, at] + y4_in[c].astype(F32)).astype(BF16)

    count = len(blocks)
    loaded((2,))
    for n in range(count):
        if n == 1:
            issue([(relay, 2, 2)], [(relay, 2, 0), (relay, 3, 0)])
        if n == 2:
            issue([(relay, 3, 2)], [(relay, 2, 2), (relay, 3, 2)])
        if n == 4:
            relay(2, 1)
        if n == 5:
            relay(3, 1)
        down(n)
        if n == 0:
            pl.when(edge)(release)
        if n >= 1:
            stage_two(n - 1)
        if n >= 2:
            stage_three(n - 2)
    stage_two(count - 1)
    stage_three(count - 2)
    stage_four(0)
    stage_four(1)
    stage_three(count - 1)
    for n in range(2, count):
        stage_four(n)
    for n in range(count):
        finish(n)

    for copy in sent + [d[n] for d in (firsts, turns, pairs, ends) for n in range(count)]:
        copy.wait_send()

    @pl.when(inner)
    def _():
        for n in (2, 3):
            along(me_s, n, near[0]).wait_send()

    for k in range(4):
        for i in range(3):
            if k != 1 or i == 0:
                if (k, i) != (0, 1):
                    gone(k, i)
            sized(me_s, lambda width: passed(k, i, width).wait_send())
    issue([(gone, 0, 1)], [])


def moved_weights(
    ssm_input, residual_in, log_step, decay_real, freq, in_real, in_imag, out_real, out_imag,
    skip, w_glu, b_glu, w_branch, norm_gain, w_gate, w_up, w_down,
):
    sizes = {axis: lax.axis_size(axis) for axis in ("grp", "sp", "tp")}
    n_sp, n_tp = sizes["sp"], sizes["tp"]
    tok, width = ssm_input.shape
    groups, states = decay_real.shape
    group = in_real.shape[2]
    lanes = groups * states
    own = tok // n_tp
    chan, d_model = w_branch.shape
    depth, hid = w_gate.shape
    cols = w_down.shape[1]
    wide = -(-hid // (TILE * n_sp)) * TILE
    rows = n_sp * tok
    blocks = 2 * n_sp
    vm = pl.BlockSpec(memory_space=pltpu.VMEM)
    hbm = pl.BlockSpec(memory_space=pl.ANY)
    dma = pltpu.SemaphoreType.DMA
    vmem = pltpu.VMEM
    return pl.pallas_call(
        functools.partial(layer_kernel, sizes),
        out_shape=jax.ShapeDtypeStruct((own, d_model), BF16),
        in_specs=[vm, hbm] + [vm] * 8 + [hbm, vm, hbm, vm] + [hbm] * 3,
        out_specs=vm,
        scratch_shapes=[
            vmem((n_sp, n_tp, own, d_model), BF16),
            vmem((own, d_model), F32),
            vmem((d_model, 2 * wide), BF16),
            vmem((wide, d_model), BF16),
            vmem((rows, 2 * wide), F32),
            vmem((rows, wide), BF16),
            vmem((blocks, 2, n_sp, own, cols // 2), F32),
            vmem((blocks, 2, n_sp, own, cols // 2), BF16),
            vmem((blocks, 2, n_sp, own, cols // 2), BF16),
            vmem((blocks, n_sp, own, cols // 2), BF16),
            vmem((blocks, n_sp, own, cols // 2), BF16),
            vmem((blocks, 2, own, cols // 2), BF16),
            vmem((blocks, 2, own, cols // 2), BF16),
            vmem((blocks, own, cols // 2), BF16),
            vmem((blocks, own, cols // 2), BF16),
            dma((3,)),
            dma((4, 3)), dma((4, n_sp)), dma((4, 3)), dma((4, 3)),
            dma((4,)), dma((n_sp,)),
            dma((n_sp,)), dma((n_sp,)),
            dma((n_sp, 2)), dma((n_sp, 2)),
            dma((blocks,)), dma((blocks,)), dma((blocks,)), dma((blocks,)),
            dma((blocks,)), dma((blocks,)), dma((blocks,)), dma((blocks,)),
            pltpu.SemaphoreType.REGULAR((2,)),
            vmem((chan, chan), BF16),
            vmem((chan, d_model), BF16),
            vmem((own, d_model), BF16),
            vmem((8, lanes), F32),
            vmem((tok, lanes), F32),
            vmem((tok, lanes), F32),
            vmem((tok, lanes), F32),
            vmem((tok, lanes), F32),
            vmem((2, lanes), F32),
            vmem((n_sp - 1, 2, lanes), F32),
            vmem((n_tp, own, width), BF16),
            vmem((n_tp - 1, own, width), BF16),
            vmem((own, chan), F32),
            dma((3,)),
            dma((n_sp - 1,)), dma((n_sp - 1,)),
            dma((n_tp - 1,)), dma((n_tp - 1,)),
        ],
        compiler_params=pltpu.CompilerParams(collective_id=0, has_side_effects=True),
        name="layer",
    )(
        ssm_input, residual_in, log_step[None], decay_real, freq,
        in_real.swapaxes(1, 2).reshape(width, states),
        in_imag.swapaxes(1, 2).reshape(width, states),
        out_real.reshape(width, states), out_imag.reshape(width, states),
        skip[None], w_glu, b_glu[None], w_branch, norm_gain[None], w_gate, w_up, w_down,
    )


def per_device(*arguments):
    sizes = tuple(lax.axis_size(axis) for axis in ("grp", "sp", "tp"))
    tiles = arguments[14].shape[1] // TILE
    fits = sizes == (2, 4, 4) and tiles % 4 == 3
    return (moved_weights if fits else gathered_weights)(*arguments)


def solution(mesh):
    placed = (
        P(("grp", "sp"), "tp"),
        P(("grp", "sp"), None),
        P("tp"),
        P("tp", None),
        P("tp", None),
        P("tp", None, None),
        P("tp", None, None),
        P("tp", None, None),
        P("tp", None, None),
        P("tp"),
        P(),
        P(),
        P(),
        P(),
        P("sp", "tp"),
        P("sp", "tp"),
        P("tp", "sp"),
    )
    return jax.shard_map(
        per_device,
        mesh=mesh,
        in_specs=placed,
        out_specs=P(("grp", "sp", "tp"), None),
        check_vma=False,
    )
```

```python
import functools
import math

import jax
import jax.numpy as jnp
from jax import lax
from jax.experimental import pallas as pl
from jax.experimental.pallas import tpu as pltpu
from jax.sharding import PartitionSpec as P

EPS = 1e-06


def prefix(shard, axis, combine, identity):
    count, place = (lax.axis_size(axis), lax.axis_index(axis))
    everything = jax.tree.map(lambda part: lax.all_gather(part, axis), shard)
    start = jax.tree.map(
        lambda part, zero: jnp.broadcast_to(jnp.asarray(zero, part.dtype), part.shape),
        shard,
        identity,
    )

    def lap(k, before):
        reached = k < place
        new = combine(before, jax.tree.map(lambda part: part[k], everything))
        return jax.tree.map(lambda a, b: jnp.where(reached, a, b), new, before)

    return lax.fori_loop(0, count, lap, start)


def discretize(log_step, decay_real, freq, in_real, in_imag):
    step_size = jnp.exp(log_step)[:, None]
    magnitude = jnp.exp(decay_real * step_size)
    abar_re = magnitude * jnp.cos(freq * step_size)
    abar_im = magnitude * jnp.sin(freq * step_size)
    denominator = decay_real * decay_real + freq * freq
    less_re = abar_re - 1.0
    hold_re = ((less_re * decay_real + abar_im * freq) / denominator)[..., None]
    hold_im = ((abar_im * decay_real - less_re * freq) / denominator)[..., None]
    bbar_re = hold_re * in_real - hold_im * in_imag
    bbar_im = hold_re * in_imag + hold_im * in_real
    return (step_size, abar_re, abar_im, bbar_re, bbar_im)


def powers(decay_real, freq, step_size, length):
    steps_up = (jnp.arange(length, dtype=jnp.int32) + 1).astype(jnp.float32)[:, None, None]
    magnitude = jnp.exp((decay_real * step_size)[None] * steps_up)
    phase = (freq * step_size)[None] * steps_up
    return (magnitude * jnp.cos(phase), magnitude * jnp.sin(phase))


def compose(earlier, later):
    a1r, a1i, b1r, b1i = earlier
    a2r, a2i, b2r, b2i = later
    return (
        a2r * a1r - a2i * a1i,
        a2r * a1i + a2i * a1r,
        a2r * b1r - a2i * b1i + b2r,
        a2r * b1i + a2i * b1r + b2i,
    )


def local_states(inputs, decay_real, freq, step_size, bbar_re, bbar_im):
    highest = lax.Precision.HIGHEST
    tok_rows, group_count, unused = inputs.shape
    lanes = group_count * decay_real.shape[1]
    drive_re = jnp.einsum("lgm,gpm->lgp", inputs, bbar_re, precision=highest).reshape(
        tok_rows, lanes
    )
    drive_im = jnp.einsum("lgm,gpm->lgp", inputs, bbar_im, precision=highest).reshape(
        tok_rows, lanes
    )
    span = math.gcd(tok_rows, 16)
    spans = tok_rows // span
    rate = (decay_real * step_size).reshape(lanes)
    turn = (freq * step_size).reshape(lanes)
    later = jnp.arange(span, dtype=jnp.int32)[:, None]
    earlier = jnp.arange(span, dtype=jnp.int32)[None, :]
    lag = (later - earlier).astype(jnp.float32)
    causal = (later >= earlier)[..., None]
    lag_pos = jnp.maximum(lag, 0.0)[..., None]
    table_mag = jnp.exp(rate[None, None] * lag_pos)
    table_re = jnp.where(causal, table_mag * jnp.cos(turn[None, None] * lag_pos), 0.0)
    table_im = jnp.where(causal, table_mag * jnp.sin(turn[None, None] * lag_pos), 0.0)
    block_re = drive_re.reshape(spans, 1, span, lanes)
    block_im = drive_im.reshape(spans, 1, span, lanes)
    inner_re = jnp.sum(table_re[None] * block_re - table_im[None] * block_im, axis=2)
    inner_im = jnp.sum(table_re[None] * block_im + table_im[None] * block_re, axis=2)
    steps_up = (jnp.arange(span, dtype=jnp.int32) + 1).astype(jnp.float32)[:, None]
    pow_mag = jnp.exp(rate[None] * steps_up)
    pow_re = pow_mag * jnp.cos(turn[None] * steps_up)
    pow_im = pow_mag * jnp.sin(turn[None] * steps_up)
    span_re = pow_re[-1]
    span_im = pow_im[-1]

    def carry_step(entering, ends):
        next_re = span_re * entering[0] - span_im * entering[1] + ends[0]
        next_im = span_re * entering[1] + span_im * entering[0] + ends[1]
        return ((next_re, next_im), entering)

    zeros = jnp.zeros((lanes,), jnp.float32)
    unused_carry, entering = lax.scan(
        carry_step, (zeros, zeros), (inner_re[:, -1], inner_im[:, -1])
    )
    state_re = inner_re + pow_re[None] * entering[0][:, None] - pow_im[None] * entering[1][:, None]
    state_im = inner_im + pow_re[None] * entering[1][:, None] + pow_im[None] * entering[0][:, None]
    shape = (tok_rows, group_count, decay_real.shape[1])
    return (state_re.reshape(shape), state_im.reshape(shape))


def readout(state_re, state_im, out_real, out_imag, skip_mat, inputs):
    highest = lax.Precision.HIGHEST
    values = (
        jnp.einsum("lgp,gmp->lgm", state_re, out_real, precision=highest)
        - jnp.einsum("lgp,gmp->lgm", state_im, out_imag, precision=highest)
        + skip_mat[None] * inputs
    )
    values = jax.nn.gelu(values)
    return values.reshape(values.shape[0], -1).astype(jnp.bfloat16)


def row_norm(stream, norm_gain):
    scale_rows = lax.rsqrt(jnp.mean(stream * stream, axis=-1, keepdims=True) + EPS)
    return (stream * scale_rows * norm_gain).astype(jnp.bfloat16)


def gathered_weights(
    ssm_input,
    residual_in,
    log_step,
    decay_real,
    freq,
    in_real,
    in_imag,
    out_real,
    out_imag,
    skip,
    w_glu,
    b_glu,
    w_branch,
    norm_gain,
    w_gate,
    w_up,
    w_down,
):
    tok_rows, width_local = ssm_input.shape
    group_count = log_step.shape[0]
    group_size = in_real.shape[2]
    tp_count = lax.axis_size("tp")
    tp_index = lax.axis_index("tp")
    own_rows = tok_rows // tp_count
    step_size, abar_re, abar_im, bbar_re, bbar_im = discretize(
        log_step, decay_real, freq, in_real, in_imag
    )
    pow_re, pow_im = powers(decay_real, freq, step_size, tok_rows)
    inputs = ssm_input.astype(jnp.float32).reshape(tok_rows, group_count, group_size)
    local_re, local_im = local_states(inputs, decay_real, freq, step_size, bbar_re, bbar_im)
    identity = (
        jnp.ones_like(abar_re),
        jnp.zeros_like(abar_re),
        jnp.zeros_like(abar_re),
        jnp.zeros_like(abar_re),
    )
    carried = prefix((pow_re[-1], pow_im[-1], local_re[-1], local_im[-1]), "sp", compose, identity)
    state_re = local_re + pow_re * carried[2][None] - pow_im * carried[3][None]
    state_im = local_im + pow_re * carried[3][None] + pow_im * carried[2][None]
    mixer_out = readout(
        state_re, state_im, out_real, out_imag, skip.reshape(group_count, group_size), inputs
    )
    mixer_rows = lax.all_to_all(mixer_out, "tp", split_axis=0, concat_axis=1, tiled=True)
    glu_pre = jnp.dot(mixer_rows, w_glu, preferred_element_type=jnp.float32) + b_glu
    gated = (mixer_rows.astype(jnp.float32) * jax.nn.sigmoid(glu_pre)).astype(jnp.bfloat16)
    residual_own = lax.dynamic_slice_in_dim(residual_in, tp_index * own_rows, own_rows, 0)
    stream = residual_own.astype(jnp.float32) + jnp.dot(
        gated, w_branch, preferred_element_type=jnp.float32
    )
    normed = row_norm(stream, norm_gain)
    normed_all = lax.all_gather(normed, "tp", axis=0, tiled=True)
    gate_sum = jnp.dot(
        normed_all,
        lax.all_gather(w_gate, "sp", axis=0, tiled=True),
        preferred_element_type=jnp.float32,
    )
    up_sum = jnp.dot(
        normed_all,
        lax.all_gather(w_up, "sp", axis=0, tiled=True),
        preferred_element_type=jnp.float32,
    )
    hidden = (jax.nn.silu(gate_sum) * up_sum).astype(jnp.bfloat16)
    down_whole = lax.all_gather(w_down, "sp", axis=1, tiled=True)
    summed = lax.psum_scatter(
        jnp.dot(hidden, down_whole, preferred_element_type=jnp.float32).astype(jnp.bfloat16),
        "tp",
        scatter_dimension=0,
        tiled=True,
    ).astype(jnp.float32)
    return (stream + summed).astype(jnp.bfloat16)


MESH = pl.DeviceIdType.MESH
F32 = jnp.float32
BF16 = jnp.bfloat16
NT = (((1,), (1,)), ((), ()))


def greet(sizes, place):
    barrier = pltpu.get_barrier_semaphore()
    for axis in sizes:
        for d in range(1, sizes[axis]):
            pl.semaphore_signal(
                barrier, inc=1, device_id={axis: lax.rem(place[axis] + d, sizes[axis])},
                device_id_type=MESH,
            )
    pl.semaphore_wait(barrier, sum(sizes.values()) - len(sizes))


def send(src, dst, ss, rs, **to):
    copy = pltpu.make_async_remote_copy(
        src_ref=src, dst_ref=dst, send_sem=ss, recv_sem=rs, device_id=to, device_id_type=MESH
    )
    copy.start()
    return copy


def aligned(index, size):
    return pl.ds(pl.multiple_of(index * size, size), size)


def mixer(
    n_sp, n_tp, after_ends,
    u_ref, res_ref, ls_ref, dec_ref, frq_ref, inr_ref, ini_ref, outr_ref, outi_ref,
    skip_ref, wglu_ref, bglu_ref, wbr_ref, gain_ref,
    normed_ref, stream_ref,
    wglu, wbr, res, coef, xr, xi, pr_all, pi_all, fin, fin_in, mo, rows_in, glu,
    load_sem, fs, fr, rs, rr,
):
    me_s, me_t = lax.axis_index("sp"), lax.axis_index("tp")
    tok, width = u_ref.shape
    groups, states = dec_ref.shape
    group = width // groups
    lanes = groups * states
    own = tok // n_tp
    loads = [
        pltpu.make_async_copy(
            res_ref.at[pl.ds(pl.multiple_of(me_t * own, own), own)], res, load_sem.at[0]
        ),
        pltpu.make_async_copy(wglu_ref, wglu, load_sem.at[1]),
        pltpu.make_async_copy(wbr_ref, wbr, load_sem.at[2]),
    ]
    for load in loads:
        load.start()

    same = lax.broadcasted_iota(jnp.int32, (groups, groups), 0) == lax.broadcasted_iota(
        jnp.int32, (groups, groups), 1
    )
    step = jnp.exp(jnp.sum(jnp.where(same, ls_ref[...], 0.0), axis=1, keepdims=True))
    dec, frq = dec_ref[...], frq_ref[...]
    mag = jnp.exp(dec * step)
    ar = mag * jnp.cos(frq * step)
    ai = mag * jnp.sin(frq * step)
    den = dec * dec + frq * frq
    less = ar - 1.0
    hr = (less * dec + ai * frq) / den
    hi = (ai * dec - less * frq) / den
    for g in range(groups):
        at = slice(g * states, (g + 1) * states)
        coef[0:1, at] = ar[g : g + 1, :]
        coef[1:2, at] = ai[g : g + 1, :]
        coef[2:3, at] = hr[g : g + 1, :]
        coef[3:4, at] = hi[g : g + 1, :]

    u = u_ref[...]
    part = 128
    spread = (
        lax.broadcasted_iota(jnp.int32, (states, part), 1) % states
        == lax.broadcasted_iota(jnp.int32, (states, part), 0)
    ).astype(BF16)
    rows_group = lax.broadcasted_iota(jnp.int32, (width, part), 0) // group
    lane_group = lax.broadcasted_iota(jnp.int32, (width, part), 1) // states

    def spread_out(ref):
        return jnp.dot(ref[...].astype(BF16), spread, preferred_element_type=F32)

    def only(wide, c):
        return jnp.where(rows_group == lane_group + c * (part // states), wide, 0.0).astype(BF16)

    in_r, in_i = spread_out(inr_ref), spread_out(ini_ref)
    row = lax.broadcasted_iota(jnp.int32, (tok, part), 0)
    row8 = lax.broadcasted_iota(jnp.int32, (8, part), 0)
    for c in range(lanes // part):
        at = slice(c * part, (c + 1) * part)
        vr = jnp.dot(u, only(in_r, c), preferred_element_type=F32)
        vi = jnp.dot(u, only(in_i, c), preferred_element_type=F32)
        cr, ci = coef[2:3, at], coef[3:4, at]
        sr, si = cr * vr - ci * vi, cr * vi + ci * vr
        pr, pi = coef[0:1, at], coef[1:2, at]
        tr, ti = jnp.ones((8, part), F32), jnp.zeros((8, part), F32)
        s = 1
        while s <= tok:
            if s <= 8:
                bit = ((row8 + 1) & s) != 0
                br, bi = jnp.where(bit, pr, 1.0), jnp.where(bit, pi, 0.0)
                tr, ti = tr * br - ti * bi, tr * bi + ti * br
            if s >= 8 and s < tok:
                tr, ti = (
                    jnp.concatenate([tr, tr * pr - ti * pi], 0),
                    jnp.concatenate([ti, tr * pi + ti * pr], 0),
                )
            if s < tok:
                if s < 8:
                    yr = jnp.where(row >= s, pltpu.roll(sr, s, 0), 0.0)
                    yi = jnp.where(row >= s, pltpu.roll(si, s, 0), 0.0)
                else:
                    gap = jnp.zeros((s, part), F32)
                    yr = jnp.concatenate([gap, sr[: tok - s]], 0)
                    yi = jnp.concatenate([gap, si[: tok - s]], 0)
                sr, si = sr + (pr * yr - pi * yi), si + (pr * yi + pi * yr)
            pr, pi = pr * pr - pi * pi, 2.0 * pr * pi
            s *= 2
        xr[:, at], xi[:, at] = sr, si
        pr_all[:, at], pi_all[:, at] = tr, ti
        fin[0:1, at] = sr[tok - 1 : tok]
        fin[1:2, at] = si[tok - 1 : tok]

    def end_to(d):
        return pltpu.make_async_remote_copy(
            src_ref=fin, dst_ref=fin_in.at[d - 1], send_sem=fs.at[d - 1], recv_sem=fr.at[d - 1],
            device_id={"sp": lax.rem(me_s + d, n_sp)}, device_id_type=MESH,
        )

    for d in range(1, n_sp):
        @pl.when(me_s + d < n_sp)
        def _():
            end_to(d).start()
    after_ends()

    out_r, out_i = spread_out(outr_ref), spread_out(outi_ref)
    outr = jnp.concatenate([only(out_r, c) for c in range(lanes // part)], axis=1)
    outi = jnp.concatenate([only(out_i, c) for c in range(lanes // part)], axis=1)
    for d in range(1, n_sp):
        @pl.when(me_s >= d)
        def _():
            end_to(d).wait_recv()
    er, ei = pr_all[tok - 1 : tok, :], pi_all[tok - 1 : tok, :]
    pr, pi = jnp.ones((1, lanes), F32), jnp.zeros((1, lanes), F32)
    cr, ci = jnp.zeros((1, lanes), F32), jnp.zeros((1, lanes), F32)
    for d in range(1, n_sp):
        fr_, fi_ = fin_in[d - 1, 0:1, :], fin_in[d - 1, 1:2, :]
        reached = me_s >= d
        cr = cr + jnp.where(reached, pr * fr_ - pi * fi_, 0.0)
        ci = ci + jnp.where(reached, pr * fi_ + pi * fr_, 0.0)
        pr, pi = pr * er - pi * ei, pr * ei + pi * er
    tr, ti = pr_all[...], pi_all[...]
    sr = (xr[...] + (tr * cr - ti * ci)).astype(BF16)
    si = (xi[...] + (tr * ci + ti * cr)).astype(BF16)
    y = lax.dot_general(sr, outr, NT, preferred_element_type=F32) - lax.dot_general(
        si, outi, NT, preferred_element_type=F32
    )
    for d in range(1, n_sp):
        @pl.when(me_s + d < n_sp)
        def _():
            end_to(d).wait_send()
    y = jax.nn.gelu(y + skip_ref[...] * u.astype(F32))
    mo[...] = y.astype(BF16).reshape(n_tp, own, width)
    turns = []
    for d in range(1, n_tp):
        to = lax.rem(me_t + d, n_tp)
        copy = pltpu.make_async_remote_copy(
            src_ref=mo.at[to], dst_ref=rows_in.at[d - 1], send_sem=rs.at[d - 1],
            recv_sem=rr.at[d - 1], device_id={"tp": to}, device_id_type=MESH,
        )
        copy.start()
        turns.append(copy)
    for load in loads:
        load.wait()

    def source(d):
        return pl.ds(pl.multiple_of(lax.rem(me_t + n_tp - d, n_tp) * width, width), width)

    blocks = [mo[me_t]]
    pre = bglu_ref[...] + jnp.dot(blocks[0], wglu[source(0), :], preferred_element_type=F32)
    for d in range(1, n_tp):
        turns[d - 1].wait()
        blocks.append(rows_in[d - 1])
        pre = pre + jnp.dot(blocks[d], wglu[source(d), :], preferred_element_type=F32)
    glu[...] = pre
    stream = res[...].astype(F32)
    for d in range(n_tp):
        gate = jax.nn.sigmoid(glu[:, source(d)])
        gated = (blocks[d].astype(F32) * gate).astype(BF16)
        stream = stream + jnp.dot(gated, wbr[source(d), :], preferred_element_type=F32)
    stream_ref[...] = stream
    scale = lax.rsqrt(jnp.mean(stream * stream, axis=-1, keepdims=True) + EPS)
    normed_ref[...] = (stream * scale * gain_ref[...]).astype(BF16)


TILE = 128


def layer_kernel(sizes, *refs):
    n_sp, n_tp = sizes["sp"], sizes["tp"]
    place = {axis: lax.axis_index(axis) for axis in sizes}
    me_g, me_s, me_t = place["grp"], place["sp"], place["tp"]
    wg_ref, wu_ref, wd_ref, out_ref = refs[14:18]
    x, stream, wgu, wd, acc, h = refs[18:24]
    keep, y1_out, y1_in, y2_out, y2_in, y3_out, y3_in, y4_out, y4_in, y5_out, y5_in = refs[24:35]
    (load_sem, ws, wr, fs, fr, az_s, az_r, ax_s, ax_r, am_s, am_r,
     s1, r1, s2, r2, s3, r3, s4, r4, s5, r5, met) = refs[35:57]
    mixer_scratch = refs[57:]
    own, d_model = stream.shape
    depth, hid = wg_ref.shape
    cols = wd_ref.shape[1]
    wide = wgu.shape[1] // 2
    rows = n_sp * n_tp * own
    parity = me_t % 2
    short = (n_sp - 1) * (1 - parity)
    part_row, part_col = depth // 4, cols // 4
    half_col = 2 * part_col

    side = me_s // 2
    inner = me_s % 2 != side
    partner = me_s + 1 - 2 * (me_s % 2)
    opposite = lax.rem(me_s + 2, n_sp)
    near = [partner, 2 - side, 3 * (1 - side)]
    order = [me_s] + near
    mate = me_t + 1 - 2 * (me_t % 2)
    across = lax.rem(me_t + 2, n_tp)

    def sized(to, act):
        @pl.when(to == short)
        def _():
            act(wide - TILE)

        @pl.when(to != short)
        def _():
            act(wide)

    def first(to):
        return (3 * to - parity * ((to + 3) // 4)) * TILE

    def shipped(k, i, width):
        start = pl.ds(pl.multiple_of(first(near[i]), TILE), width)
        if k < 4:
            at = 2 * me_g + k % 2
            src = (wg_ref, wu_ref)[k // 2].at[aligned(at, part_row), start]
            dst = wgu.at[aligned(4 * me_s + at, part_row), pl.ds(k // 2 * wide, width)]
        else:
            at = 2 * (k - 4) + me_g
            src = wd_ref.at[start, aligned(at, part_col)]
            dst = wd.at[pl.ds(0, width), aligned(4 * me_s + at, part_col)]
        return pltpu.make_async_remote_copy(
            src_ref=src, dst_ref=dst, send_sem=ws.at[k, i], recv_sem=wr.at[k, me_s],
            device_id={"sp": near[i]}, device_id_type=MESH,
        )

    def ship(k, i):
        sized(near[i], lambda width: shipped(k, i, width).start())

    def handed(k, i, width):
        at = 4 * near[i] + 2 * me_g + k % 2
        if k < 4:
            return wgu.at[aligned(at, part_row), pl.ds(k // 2 * wide, width)]
        at = 4 * near[i] + 2 * (k - 4) + me_g
        return wd.at[pl.ds(0, width), aligned(at, part_col)]

    def passed(k, i, width):
        piece = handed(k, i, width)
        return pltpu.make_async_remote_copy(
            src_ref=piece, dst_ref=piece, send_sem=fs.at[k, i], recv_sem=fr.at[k, i],
            device_id={"grp": 1 - me_g}, device_id_type=MESH,
        )

    def relay(k, i):
        def act(width):
            piece = handed(k, i, width)
            pltpu.make_async_remote_copy(
                src_ref=piece, dst_ref=piece, send_sem=ws.at[k, i], recv_sem=wr.at[k, near[i]],
                device_id={"sp": near[i]}, device_id_type=MESH,
            ).wait_recv()
            passed(k, i, width).start()

        sized(me_s, act)

    def arrived(k, i):
        sized(me_s, lambda width: passed(k, i, width).wait_recv())

    def own_loads(width):
        start = pl.ds(pl.multiple_of(first(me_s), TILE), width)
        return [
            pltpu.make_async_copy(
                ref.at[:, start], wgu.at[aligned(me_s, depth), pl.ds(k * wide, width)],
                load_sem.at[k],
            )
            for k, ref in enumerate((wg_ref, wu_ref))
        ] + [
            pltpu.make_async_copy(
                wd_ref.at[start, :], wd.at[pl.ds(0, width), aligned(me_s, cols)], load_sem.at[2]
            )
        ]

    def start_loads(width):
        for load in own_loads(width):
            load.start()

    edge = jnp.logical_not(inner)

    def issue(at_inner, at_edge):
        for where, jobs in ((inner, at_inner), (edge, at_edge)):
            @pl.when(where)
            def _():
                for act, *where_to in jobs:
                    act(*where_to)

    ends_in = mixer_scratch[9]
    ends_in[...] = jnp.zeros_like(ends_in)
    greet(sizes, place)
    issue([(ship, 0, 1), (ship, 0, 0)], [(ship, 0, 0)])
    sized(me_s, start_loads)

    @pl.when(me_s == short)
    def _():
        for k in range(2):
            wgu[:, (k + 1) * wide - TILE : (k + 1) * wide] = jnp.zeros((n_sp * depth, TILE), BF16)
        wd[wide - TILE :, :] = jnp.zeros((TILE, d_model), BF16)

    def after_ends():
        issue([(ship, 1, 1)] + [(ship, k, 2) for k in range(4)], [])
        for k in (1, 2, 3):
            ship(k, 0)

    mixer(
        n_sp, n_tp, after_ends, *refs[:14], x.at[me_s, 0], stream, *mixer_scratch
    )

    def along(b, n, to):
        return pltpu.make_async_remote_copy(
            src_ref=x.at[b, 0], dst_ref=x.at[b, 0], send_sem=az_s.at[n], recv_sem=az_r.at[b],
            device_id={"sp": to}, device_id_type=MESH,
        )

    sent = []

    def share(b):
        sent.append(send(x.at[b, 0], x.at[b, 2], ax_s.at[b], ax_r.at[b], tp=across))
        sent.append(send(x.at[b, 0], x.at[b, 1], am_s.at[b, 0], am_r.at[b, 0], tp=mate))

    def spread(b):
        pltpu.make_async_remote_copy(
            src_ref=x.at[b, 2], dst_ref=x.at[b, 2], send_sem=ax_s.at[b], recv_sem=ax_r.at[b],
            device_id={"tp": across}, device_id_type=MESH,
        ).wait_recv()
        sent.append(send(x.at[b, 2], x.at[b, 3], am_s.at[b, 1], am_r.at[b, 1], tp=mate))

    def collected(b):
        for n, slot in ((0, 1), (1, 3)):
            pltpu.make_async_remote_copy(
                src_ref=x.at[b, slot], dst_ref=x.at[b, slot], send_sem=am_s.at[b, n],
                recv_sem=am_r.at[b, n], device_id={"tp": mate}, device_id_type=MESH,
            ).wait_recv()

    def meet(n):
        pl.semaphore_signal(met.at[n], inc=1, device_id={"tp": mate}, device_id_type=MESH)
        pl.semaphore_wait(met.at[n], 1)

    def gone(k, i):
        sized(near[i], lambda width: shipped(k, i, width).wait_send())

    firsthand = [along(me_s, i, near[i]) for i in range(2)]
    for copy in firsthand:
        copy.start()
    share(me_s)

    def gathered(i):
        b = near[i]
        along(b, 0, near[0]).wait_recv()
        if i:
            @pl.when(inner)
            def _():
                along(b, 1 + i, near[0]).start()
        share(b)

    gates, ups, downs = (0, 1), (2, 3), (4, 5)

    def each(act, *groups):
        return [(act, k, i) for ks, i in groups for k in ks]

    issue(each(relay, (gates, 1)), [])
    issue(each(relay, (gates, 0), (ups, 0)), each(relay, (gates, 0), (ups, 0), (gates, 1)))
    for copy in firsthand:
        copy.wait_send()
    meet(0)
    issue(
        each(ship, (ups, 1)),
        each(ship, (gates, 1), (ups, 1), (gates, 2), (ups, 2), (downs, 0)),
    )
    spread(order[0])
    gathered(0)
    issue([], each(relay, (ups, 1)))
    gathered(1)
    spread(order[1])
    gathered(2)
    issue(each(relay, (gates, 2)) + each(ship, (downs, 0)), [])
    spread(order[2])
    spread(order[3])
    issue(each(relay, (ups, 2)), each(relay, (gates, 2)))
    for b in order:
        collected(b)

    def product(b):
        lhs = x[:, :, :, aligned(b, depth)].reshape(rows, depth)
        return jnp.dot(lhs, wgu[aligned(b, depth), :], preferred_element_type=F32)

    def loaded(which):
        def act(width):
            loads = own_loads(width)
            for n in which:
                loads[n].wait()

        sized(me_s, act)

    def landed(i):
        for k in range(4):
            arrived(k, i)

    loaded((0, 1))
    acc[...] = product(me_s)
    landed(0)
    acc[...] += product(near[0])
    issue(each(relay, (ups, 1)), each(relay, (ups, 2)))

    def release():
        for k in ups:
            gone(k, 1)
        issue([], each(gone, (gates, 1), (gates, 2), (ups, 2)))
        meet(1)
        issue(
            [
                (lambda: pl.semaphore_signal(
                    met.at[2], inc=1, device_id={"sp": near[0]}, device_id_type=MESH
                ),)
            ],
            [(lambda: pl.semaphore_wait(met.at[2], 1),)],
        )
        for i in (2, 1):
            for k in downs:
                ship(k, i)

    pl.when(inner)(release)

    def add(i):
        landed(i)
        acc[...] += product(near[i])

    pl.when(inner)(lambda: add(2))
    pl.when(edge)(lambda: add(1))
    for k in downs:
        relay(k, 0)
    pl.when(edge)(release)
    last = jnp.where(inner, near[1], near[2])
    pl.when(inner)(lambda: landed(1))
    pl.when(edge)(lambda: landed(2))
    total = acc[...] + product(last)
    h[...] = (jax.nn.silu(total[:, :wide]) * total[:, wide:]).astype(BF16)

    blocks = [(i, q) for i in (0, 1, 3, 2) for q in range(2)]

    def place_of(n):
        i, q = blocks[n]
        return 2 * order[i] + q

    firsts, turns, pairs, ends, straight = {}, {}, {}, {}, []
    held = len(blocks) // 2

    def down(n):
        i, q = blocks[n]
        if i:
            arrived(downs[q], i - 1)
        y = jnp.dot(h[...], wd[:, aligned(place_of(n), half_col)], preferred_element_type=F32)
        y = y.reshape(n_sp, n_tp, own, half_col)
        y1_out[n, 0] = y[:, 1].astype(BF16)
        y1_out[n, 1] = y[:, 3].astype(BF16)
        firsts[n] = send(y1_out.at[n], y1_in.at[n], s1.at[n], r1.at[n], tp=mate)
        keep[n, 0] = y[:, 0]
        keep[n, 1] = y[:, 2]

    def stage_two(n):
        firsts[n].wait_recv()
        y2_out[n] = (keep[n, 1] + y1_in[n, 1].astype(F32)).astype(BF16)
        turns[n] = send(y2_out.at[n], y2_in.at[n], s2.at[n], r2.at[n], tp=across)
        keep[n, 0] += y1_in[n, 0].astype(F32)

    def stage_three(n):
        c = place_of(n)
        turns[n].wait_recv()
        keep[n, 0] += y2_in[n].astype(F32)
        y3_out[c, 0] = keep[n, 0, partner].astype(BF16)
        if n < held:
            y3_out[c, 1] = keep[n, 0, lax.rem(partner + 2, n_sp)].astype(BF16)
            pairs[n] = send(y3_out.at[c], y3_in.at[c], s3.at[c], r3.at[c], sp=partner)
            return
        pairs[n] = send(y3_out.at[c, 0], y3_in.at[c, 0], s3.at[c], r3.at[c], sp=partner)
        for j in range(2):
            y5_out[n - held, j] = keep[n, 0, 2 - 2 * side + j].astype(BF16)
            straight.append(
                send(y5_out.at[n - held, j], y5_in.at[c % held, me_s % 2],
                     s5.at[n - held, j], r5.at[c % held, me_s % 2], sp=2 - 2 * side + j)
            )

    def stage_four(n):
        c = place_of(n)
        pairs[n].wait_recv()
        y4_out[c] = (keep[n, 0, opposite] + y3_in[c, 1].astype(F32)).astype(BF16)
        ends[n] = send(y4_out.at[c], y4_in.at[c], s4.at[c], r4.at[c], sp=opposite)
        at = aligned(c, half_col)
        stream[:, at] += keep[n, 0, me_s] + y3_in[c, 0].astype(F32)

    def finish(n):
        c = place_of(n)
        at = aligned(c, half_col)
        total = stream[:, at]
        if n < held:
            for j in range(2):
                piece = y5_in.at[c % held, j]
                pltpu.make_async_remote_copy(
                    src_ref=piece, dst_ref=piece, send_sem=s5.at[0, j],
                    recv_sem=r5.at[c % held, j], device_id={"sp": opposite}, device_id_type=MESH,
                ).wait_recv()
                total += y5_in[c % held, j].astype(F32)
        else:
            pairs[n].wait_recv()
            piece = y4_in.at[c]
            pltpu.make_async_remote_copy(
                src_ref=piece, dst_ref=piece, send_sem=s4.at[c], recv_sem=r4.at[c],
                device_id={"sp": opposite}, device_id_type=MESH,
            ).wait_recv()
            total += keep[n, 0, me_s] + y3_in[c, 0].astype(F32) + y4_in[c].astype(F32)
        out_ref[:, at] = total.astype(BF16)

    count = len(blocks)
    loaded((2,))
    for n in range(count):
        if n in (1, 2):
            relay(downs[n - 1], 2)
        if n in (4, 5):
            relay(downs[n - 4], 1)
        down(n)
        if n >= 1:
            stage_two(n - 1)
        if n >= 3:
            stage_three(n - 3)
    stage_two(count - 1)
    stage_three(5)
    stage_four(0)
    stage_four(1)
    stage_three(6)
    stage_four(2)
    stage_four(3)
    stage_three(7)
    for n in (4, 5, 0, 1, 2, 3, 6, 7):
        finish(n)

    pending = sent + straight + [d[n] for d in (firsts, turns, pairs, ends) for n in d]
    for copy in pending:
        copy.wait_send()

    @pl.when(inner)
    def _():
        for n in (2, 3):
            along(me_s, n, near[0]).wait_send()

    issue(each(gone, (gates, 1), (gates, 2), (ups, 2)), [])
    for k in range(6):
        for i in range(3):
            if i == 0 or k > 3:
                gone(k, i)
            sized(me_s, lambda width: passed(k, i, width).wait_send())


def moved_weights(
    ssm_input, residual_in, log_step, decay_real, freq, in_real, in_imag, out_real, out_imag,
    skip, w_glu, b_glu, w_branch, norm_gain, w_gate, w_up, w_down,
):
    sizes = {axis: lax.axis_size(axis) for axis in ("grp", "sp", "tp")}
    n_sp, n_tp = sizes["sp"], sizes["tp"]
    tok, width = ssm_input.shape
    groups, states = decay_real.shape
    group = in_real.shape[2]
    lanes = groups * states
    own = tok // n_tp
    chan, d_model = w_branch.shape
    depth, hid = w_gate.shape
    cols = w_down.shape[1]
    wide = -(-hid // (TILE * n_sp)) * TILE
    rows = n_sp * tok
    blocks = 2 * n_sp
    vm = pl.BlockSpec(memory_space=pltpu.VMEM)
    hbm = pl.BlockSpec(memory_space=pl.ANY)
    dma = pltpu.SemaphoreType.DMA
    vmem = pltpu.VMEM
    return pl.pallas_call(
        functools.partial(layer_kernel, sizes),
        out_shape=pltpu.VMEM((own, d_model), BF16),
        in_specs=[vm, hbm] + [vm] * 8 + [hbm, vm, hbm, vm] + [hbm] * 3,
        out_specs=vm,
        scratch_shapes=[
            vmem((n_sp, n_tp, own, d_model), BF16),
            vmem((own, d_model), F32),
            vmem((d_model, 2 * wide), BF16),
            vmem((wide, d_model), BF16),
            vmem((rows, 2 * wide), F32),
            vmem((rows, wide), BF16),
            vmem((blocks, 2, n_sp, own, cols // 2), F32),
            vmem((blocks, 2, n_sp, own, cols // 2), BF16),
            vmem((blocks, 2, n_sp, own, cols // 2), BF16),
            vmem((blocks, n_sp, own, cols // 2), BF16),
            vmem((blocks, n_sp, own, cols // 2), BF16),
            vmem((blocks, 2, own, cols // 2), BF16),
            vmem((blocks, 2, own, cols // 2), BF16),
            vmem((blocks, own, cols // 2), BF16),
            vmem((blocks, own, cols // 2), BF16),
            vmem((blocks // 2, 2, own, cols // 2), BF16),
            vmem((blocks // 2, 2, own, cols // 2), BF16),
            dma((3,)),
            dma((6, 3)), dma((6, n_sp)), dma((6, 3)), dma((6, 3)),
            dma((4,)), dma((n_sp,)),
            dma((n_sp,)), dma((n_sp,)),
            dma((n_sp, 2)), dma((n_sp, 2)),
            dma((blocks,)), dma((blocks,)), dma((blocks,)), dma((blocks,)),
            dma((blocks,)), dma((blocks,)), dma((blocks,)), dma((blocks,)),
            dma((blocks // 2, 2)), dma((blocks // 2, 2)),
            pltpu.SemaphoreType.REGULAR((3,)),
            vmem((chan, chan), BF16),
            vmem((chan, d_model), BF16),
            vmem((own, d_model), BF16),
            vmem((8, lanes), F32),
            vmem((tok, lanes), F32),
            vmem((tok, lanes), F32),
            vmem((tok, lanes), F32),
            vmem((tok, lanes), F32),
            vmem((2, lanes), F32),
            vmem((n_sp - 1, 2, lanes), F32),
            vmem((n_tp, own, width), BF16),
            vmem((n_tp - 1, own, width), BF16),
            vmem((own, chan), F32),
            dma((3,)),
            dma((n_sp - 1,)), dma((n_sp - 1,)),
            dma((n_tp - 1,)), dma((n_tp - 1,)),
        ],
        compiler_params=pltpu.CompilerParams(collective_id=0, has_side_effects=True),
        name="layer",
    )(
        ssm_input, residual_in, log_step[None], decay_real, freq,
        in_real.swapaxes(1, 2).reshape(width, states),
        in_imag.swapaxes(1, 2).reshape(width, states),
        out_real.reshape(width, states), out_imag.reshape(width, states),
        skip[None], w_glu, b_glu[None], w_branch, norm_gain[None], w_gate, w_up, w_down,
    )


def per_device(*arguments):
    sizes = tuple(lax.axis_size(axis) for axis in ("grp", "sp", "tp"))
    tiles = arguments[14].shape[1] // TILE
    fits = sizes == (2, 4, 4) and tiles % 4 == 3
    return (moved_weights if fits else gathered_weights)(*arguments)


def solution(mesh):
    placed = (
        P(("grp", "sp"), "tp"),
        P(("grp", "sp"), None),
        P("tp"),
        P("tp", None),
        P("tp", None),
        P("tp", None, None),
        P("tp", None, None),
        P("tp", None, None),
        P("tp", None, None),
        P("tp"),
        P(),
        P(),
        P(),
        P(),
        P("sp", "tp"),
        P("sp", "tp"),
        P("tp", "sp"),
    )
    return jax.shard_map(
        per_device,
        mesh=mesh,
        in_specs=placed,
        out_specs=P(("grp", "sp", "tp"), None),
        check_vma=False,
    )
```

```python
import functools
import math

import jax
import jax.numpy as jnp
from jax import lax
from jax.experimental import pallas as pl
from jax.experimental.pallas import tpu as pltpu
from jax.sharding import PartitionSpec as P

EPS = 1e-06


def prefix(shard, axis, combine, identity):
    count, place = (lax.axis_size(axis), lax.axis_index(axis))
    everything = jax.tree.map(lambda part: lax.all_gather(part, axis), shard)
    start = jax.tree.map(
        lambda part, zero: jnp.broadcast_to(jnp.asarray(zero, part.dtype), part.shape),
        shard,
        identity,
    )

    def lap(k, before):
        reached = k < place
        new = combine(before, jax.tree.map(lambda part: part[k], everything))
        return jax.tree.map(lambda a, b: jnp.where(reached, a, b), new, before)

    return lax.fori_loop(0, count, lap, start)


def discretize(log_step, decay_real, freq, in_real, in_imag):
    step_size = jnp.exp(log_step)[:, None]
    magnitude = jnp.exp(decay_real * step_size)
    abar_re = magnitude * jnp.cos(freq * step_size)
    abar_im = magnitude * jnp.sin(freq * step_size)
    denominator = decay_real * decay_real + freq * freq
    less_re = abar_re - 1.0
    hold_re = ((less_re * decay_real + abar_im * freq) / denominator)[..., None]
    hold_im = ((abar_im * decay_real - less_re * freq) / denominator)[..., None]
    bbar_re = hold_re * in_real - hold_im * in_imag
    bbar_im = hold_re * in_imag + hold_im * in_real
    return (step_size, abar_re, abar_im, bbar_re, bbar_im)


def powers(decay_real, freq, step_size, length):
    steps_up = (jnp.arange(length, dtype=jnp.int32) + 1).astype(jnp.float32)[:, None, None]
    magnitude = jnp.exp((decay_real * step_size)[None] * steps_up)
    phase = (freq * step_size)[None] * steps_up
    return (magnitude * jnp.cos(phase), magnitude * jnp.sin(phase))


def compose(earlier, later):
    a1r, a1i, b1r, b1i = earlier
    a2r, a2i, b2r, b2i = later
    return (
        a2r * a1r - a2i * a1i,
        a2r * a1i + a2i * a1r,
        a2r * b1r - a2i * b1i + b2r,
        a2r * b1i + a2i * b1r + b2i,
    )


def local_states(inputs, decay_real, freq, step_size, bbar_re, bbar_im):
    highest = lax.Precision.HIGHEST
    tok_rows, group_count, unused = inputs.shape
    lanes = group_count * decay_real.shape[1]
    drive_re = jnp.einsum("lgm,gpm->lgp", inputs, bbar_re, precision=highest).reshape(
        tok_rows, lanes
    )
    drive_im = jnp.einsum("lgm,gpm->lgp", inputs, bbar_im, precision=highest).reshape(
        tok_rows, lanes
    )
    span = math.gcd(tok_rows, 16)
    spans = tok_rows // span
    rate = (decay_real * step_size).reshape(lanes)
    turn = (freq * step_size).reshape(lanes)
    later = jnp.arange(span, dtype=jnp.int32)[:, None]
    earlier = jnp.arange(span, dtype=jnp.int32)[None, :]
    lag = (later - earlier).astype(jnp.float32)
    causal = (later >= earlier)[..., None]
    lag_pos = jnp.maximum(lag, 0.0)[..., None]
    table_mag = jnp.exp(rate[None, None] * lag_pos)
    table_re = jnp.where(causal, table_mag * jnp.cos(turn[None, None] * lag_pos), 0.0)
    table_im = jnp.where(causal, table_mag * jnp.sin(turn[None, None] * lag_pos), 0.0)
    block_re = drive_re.reshape(spans, 1, span, lanes)
    block_im = drive_im.reshape(spans, 1, span, lanes)
    inner_re = jnp.sum(table_re[None] * block_re - table_im[None] * block_im, axis=2)
    inner_im = jnp.sum(table_re[None] * block_im + table_im[None] * block_re, axis=2)
    steps_up = (jnp.arange(span, dtype=jnp.int32) + 1).astype(jnp.float32)[:, None]
    pow_mag = jnp.exp(rate[None] * steps_up)
    pow_re = pow_mag * jnp.cos(turn[None] * steps_up)
    pow_im = pow_mag * jnp.sin(turn[None] * steps_up)
    span_re = pow_re[-1]
    span_im = pow_im[-1]

    def carry_step(entering, ends):
        next_re = span_re * entering[0] - span_im * entering[1] + ends[0]
        next_im = span_re * entering[1] + span_im * entering[0] + ends[1]
        return ((next_re, next_im), entering)

    zeros = jnp.zeros((lanes,), jnp.float32)
    unused_carry, entering = lax.scan(
        carry_step, (zeros, zeros), (inner_re[:, -1], inner_im[:, -1])
    )
    state_re = inner_re + pow_re[None] * entering[0][:, None] - pow_im[None] * entering[1][:, None]
    state_im = inner_im + pow_re[None] * entering[1][:, None] + pow_im[None] * entering[0][:, None]
    shape = (tok_rows, group_count, decay_real.shape[1])
    return (state_re.reshape(shape), state_im.reshape(shape))


def readout(state_re, state_im, out_real, out_imag, skip_mat, inputs):
    highest = lax.Precision.HIGHEST
    values = (
        jnp.einsum("lgp,gmp->lgm", state_re, out_real, precision=highest)
        - jnp.einsum("lgp,gmp->lgm", state_im, out_imag, precision=highest)
        + skip_mat[None] * inputs
    )
    values = jax.nn.gelu(values)
    return values.reshape(values.shape[0], -1).astype(jnp.bfloat16)


def row_norm(stream, norm_gain):
    scale_rows = lax.rsqrt(jnp.mean(stream * stream, axis=-1, keepdims=True) + EPS)
    return (stream * scale_rows * norm_gain).astype(jnp.bfloat16)


def gathered_weights(
    ssm_input,
    residual_in,
    log_step,
    decay_real,
    freq,
    in_real,
    in_imag,
    out_real,
    out_imag,
    skip,
    w_glu,
    b_glu,
    w_branch,
    norm_gain,
    w_gate,
    w_up,
    w_down,
):
    tok_rows, width_local = ssm_input.shape
    group_count = log_step.shape[0]
    group_size = in_real.shape[2]
    tp_count = lax.axis_size("tp")
    tp_index = lax.axis_index("tp")
    own_rows = tok_rows // tp_count
    step_size, abar_re, abar_im, bbar_re, bbar_im = discretize(
        log_step, decay_real, freq, in_real, in_imag
    )
    pow_re, pow_im = powers(decay_real, freq, step_size, tok_rows)
    inputs = ssm_input.astype(jnp.float32).reshape(tok_rows, group_count, group_size)
    local_re, local_im = local_states(inputs, decay_real, freq, step_size, bbar_re, bbar_im)
    identity = (
        jnp.ones_like(abar_re),
        jnp.zeros_like(abar_re),
        jnp.zeros_like(abar_re),
        jnp.zeros_like(abar_re),
    )
    carried = prefix((pow_re[-1], pow_im[-1], local_re[-1], local_im[-1]), "sp", compose, identity)
    state_re = local_re + pow_re * carried[2][None] - pow_im * carried[3][None]
    state_im = local_im + pow_re * carried[3][None] + pow_im * carried[2][None]
    mixer_out = readout(
        state_re, state_im, out_real, out_imag, skip.reshape(group_count, group_size), inputs
    )
    mixer_rows = lax.all_to_all(mixer_out, "tp", split_axis=0, concat_axis=1, tiled=True)
    glu_pre = jnp.dot(mixer_rows, w_glu, preferred_element_type=jnp.float32) + b_glu
    gated = (mixer_rows.astype(jnp.float32) * jax.nn.sigmoid(glu_pre)).astype(jnp.bfloat16)
    residual_own = lax.dynamic_slice_in_dim(residual_in, tp_index * own_rows, own_rows, 0)
    stream = residual_own.astype(jnp.float32) + jnp.dot(
        gated, w_branch, preferred_element_type=jnp.float32
    )
    normed = row_norm(stream, norm_gain)
    normed_all = lax.all_gather(normed, "tp", axis=0, tiled=True)
    gate_sum = jnp.dot(
        normed_all,
        lax.all_gather(w_gate, "sp", axis=0, tiled=True),
        preferred_element_type=jnp.float32,
    )
    up_sum = jnp.dot(
        normed_all,
        lax.all_gather(w_up, "sp", axis=0, tiled=True),
        preferred_element_type=jnp.float32,
    )
    hidden = (jax.nn.silu(gate_sum) * up_sum).astype(jnp.bfloat16)
    down_whole = lax.all_gather(w_down, "sp", axis=1, tiled=True)
    summed = lax.psum_scatter(
        jnp.dot(hidden, down_whole, preferred_element_type=jnp.float32).astype(jnp.bfloat16),
        "tp",
        scatter_dimension=0,
        tiled=True,
    ).astype(jnp.float32)
    return (stream + summed).astype(jnp.bfloat16)


MESH = pl.DeviceIdType.MESH
F32 = jnp.float32
BF16 = jnp.bfloat16
NT = (((1,), (1,)), ((), ()))


def greet(sizes, place):
    barrier = pltpu.get_barrier_semaphore()
    for axis in sizes:
        for d in range(1, sizes[axis]):
            pl.semaphore_signal(
                barrier, inc=1, device_id={axis: lax.rem(place[axis] + d, sizes[axis])},
                device_id_type=MESH,
            )
    pl.semaphore_wait(barrier, sum(sizes.values()) - len(sizes))


def send(src, dst, ss, rs, **to):
    copy = pltpu.make_async_remote_copy(
        src_ref=src, dst_ref=dst, send_sem=ss, recv_sem=rs, device_id=to, device_id_type=MESH
    )
    copy.start()
    return copy


def aligned(index, size):
    return pl.ds(pl.multiple_of(index * size, size), size)


def mixer(
    n_sp, n_tp, after_ends,
    u_ref, res_ref, ls_ref, dec_ref, frq_ref, inr_ref, ini_ref, outr_ref, outi_ref,
    skip_ref, wglu_ref, bglu_ref, wbr_ref, gain_ref,
    normed_ref, stream_ref,
    wglu, wbr, res, coef, xr, xi, pr_all, pi_all, fin, fin_in, mo, rows_in, glu,
    load_sem, fs, fr, rs, rr,
):
    me_s, me_t = lax.axis_index("sp"), lax.axis_index("tp")
    tok, width = u_ref.shape
    groups, states = dec_ref.shape
    group = width // groups
    lanes = groups * states
    own = tok // n_tp
    loads = [
        pltpu.make_async_copy(
            res_ref.at[pl.ds(pl.multiple_of(me_t * own, own), own)], res, load_sem.at[0]
        ),
        pltpu.make_async_copy(wglu_ref, wglu, load_sem.at[1]),
        pltpu.make_async_copy(wbr_ref, wbr, load_sem.at[2]),
    ]
    for load in loads:
        load.start()

    same = lax.broadcasted_iota(jnp.int32, (groups, groups), 0) == lax.broadcasted_iota(
        jnp.int32, (groups, groups), 1
    )
    step = jnp.exp(jnp.sum(jnp.where(same, ls_ref[...], 0.0), axis=1, keepdims=True))
    dec, frq = dec_ref[...], frq_ref[...]
    mag = jnp.exp(dec * step)
    ar = mag * jnp.cos(frq * step)
    ai = mag * jnp.sin(frq * step)
    den = dec * dec + frq * frq
    less = ar - 1.0
    hr = (less * dec + ai * frq) / den
    hi = (ai * dec - less * frq) / den
    for g in range(groups):
        at = slice(g * states, (g + 1) * states)
        coef[0:1, at] = ar[g : g + 1, :]
        coef[1:2, at] = ai[g : g + 1, :]
        coef[2:3, at] = hr[g : g + 1, :]
        coef[3:4, at] = hi[g : g + 1, :]

    u = u_ref[...]
    part = 128
    spread = (
        lax.broadcasted_iota(jnp.int32, (states, part), 1) % states
        == lax.broadcasted_iota(jnp.int32, (states, part), 0)
    ).astype(BF16)
    rows_group = lax.broadcasted_iota(jnp.int32, (width, part), 0) // group
    lane_group = lax.broadcasted_iota(jnp.int32, (width, part), 1) // states

    def spread_out(ref):
        return jnp.dot(ref[...].astype(BF16), spread, preferred_element_type=F32)

    def only(wide, c):
        return jnp.where(rows_group == lane_group + c * (part // states), wide, 0.0).astype(BF16)

    in_r, in_i = spread_out(inr_ref), spread_out(ini_ref)
    row = lax.broadcasted_iota(jnp.int32, (tok, part), 0)
    row8 = lax.broadcasted_iota(jnp.int32, (8, part), 0)
    for c in range(lanes // part):
        at = slice(c * part, (c + 1) * part)
        vr = jnp.dot(u, only(in_r, c), preferred_element_type=F32)
        vi = jnp.dot(u, only(in_i, c), preferred_element_type=F32)
        cr, ci = coef[2:3, at], coef[3:4, at]
        sr, si = cr * vr - ci * vi, cr * vi + ci * vr
        pr, pi = coef[0:1, at], coef[1:2, at]
        tr, ti = jnp.ones((8, part), F32), jnp.zeros((8, part), F32)
        s = 1
        while s <= tok:
            if s <= 8:
                bit = ((row8 + 1) & s) != 0
                br, bi = jnp.where(bit, pr, 1.0), jnp.where(bit, pi, 0.0)
                tr, ti = tr * br - ti * bi, tr * bi + ti * br
            if s >= 8 and s < tok:
                tr, ti = (
                    jnp.concatenate([tr, tr * pr - ti * pi], 0),
                    jnp.concatenate([ti, tr * pi + ti * pr], 0),
                )
            if s < tok:
                if s < 8:
                    yr = jnp.where(row >= s, pltpu.roll(sr, s, 0), 0.0)
                    yi = jnp.where(row >= s, pltpu.roll(si, s, 0), 0.0)
                else:
                    gap = jnp.zeros((s, part), F32)
                    yr = jnp.concatenate([gap, sr[: tok - s]], 0)
                    yi = jnp.concatenate([gap, si[: tok - s]], 0)
                sr, si = sr + (pr * yr - pi * yi), si + (pr * yi + pi * yr)
            pr, pi = pr * pr - pi * pi, 2.0 * pr * pi
            s *= 2
        xr[:, at], xi[:, at] = sr, si
        pr_all[:, at], pi_all[:, at] = tr, ti
        fin[0:1, at] = sr[tok - 1 : tok]
        fin[1:2, at] = si[tok - 1 : tok]

    def end_to(d):
        return pltpu.make_async_remote_copy(
            src_ref=fin, dst_ref=fin_in.at[d - 1], send_sem=fs.at[d - 1], recv_sem=fr.at[d - 1],
            device_id={"sp": lax.rem(me_s + d, n_sp)}, device_id_type=MESH,
        )

    for d in range(1, n_sp):
        @pl.when(me_s + d < n_sp)
        def _():
            end_to(d).start()
    after_ends()

    out_r, out_i = spread_out(outr_ref), spread_out(outi_ref)
    outr = jnp.concatenate([only(out_r, c) for c in range(lanes // part)], axis=1)
    outi = jnp.concatenate([only(out_i, c) for c in range(lanes // part)], axis=1)
    for d in range(1, n_sp):
        @pl.when(me_s >= d)
        def _():
            end_to(d).wait_recv()
    er, ei = pr_all[tok - 1 : tok, :], pi_all[tok - 1 : tok, :]
    pr, pi = jnp.ones((1, lanes), F32), jnp.zeros((1, lanes), F32)
    cr, ci = jnp.zeros((1, lanes), F32), jnp.zeros((1, lanes), F32)
    for d in range(1, n_sp):
        fr_, fi_ = fin_in[d - 1, 0:1, :], fin_in[d - 1, 1:2, :]
        reached = me_s >= d
        cr = cr + jnp.where(reached, pr * fr_ - pi * fi_, 0.0)
        ci = ci + jnp.where(reached, pr * fi_ + pi * fr_, 0.0)
        pr, pi = pr * er - pi * ei, pr * ei + pi * er
    tr, ti = pr_all[...], pi_all[...]
    sr = (xr[...] + (tr * cr - ti * ci)).astype(BF16)
    si = (xi[...] + (tr * ci + ti * cr)).astype(BF16)
    y = lax.dot_general(sr, outr, NT, preferred_element_type=F32) - lax.dot_general(
        si, outi, NT, preferred_element_type=F32
    )
    for d in range(1, n_sp):
        @pl.when(me_s + d < n_sp)
        def _():
            end_to(d).wait_send()
    y = jax.nn.gelu(y + skip_ref[...] * u.astype(F32))
    mo[...] = y.astype(BF16).reshape(n_tp, own, width)
    turns = []
    for d in range(1, n_tp):
        to = lax.rem(me_t + d, n_tp)
        copy = pltpu.make_async_remote_copy(
            src_ref=mo.at[to], dst_ref=rows_in.at[d - 1], send_sem=rs.at[d - 1],
            recv_sem=rr.at[d - 1], device_id={"tp": to}, device_id_type=MESH,
        )
        copy.start()
        turns.append(copy)
    for load in loads:
        load.wait()

    def source(d):
        return pl.ds(pl.multiple_of(lax.rem(me_t + n_tp - d, n_tp) * width, width), width)

    blocks = [mo[me_t]]
    pre = bglu_ref[...] + jnp.dot(blocks[0], wglu[source(0), :], preferred_element_type=F32)
    for d in range(1, n_tp):
        turns[d - 1].wait()
        blocks.append(rows_in[d - 1])
        pre = pre + jnp.dot(blocks[d], wglu[source(d), :], preferred_element_type=F32)
    glu[...] = pre
    stream = res[...].astype(F32)
    for d in range(n_tp):
        gate = jax.nn.sigmoid(glu[:, source(d)])
        gated = (blocks[d].astype(F32) * gate).astype(BF16)
        stream = stream + jnp.dot(gated, wbr[source(d), :], preferred_element_type=F32)
    stream_ref[...] = stream
    scale = lax.rsqrt(jnp.mean(stream * stream, axis=-1, keepdims=True) + EPS)
    normed_ref[...] = (stream * scale * gain_ref[...]).astype(BF16)


TILE = 128
SMALL = (0, 2, 3, 4, 5, 6, 7, 8, 9, 11, 13)


def layer_kernel(sizes, *refs):
    n_sp, n_tp = sizes["sp"], sizes["tp"]
    place = {axis: lax.axis_index(axis) for axis in sizes}
    me_g, me_s, me_t = place["grp"], place["sp"], place["tp"]
    wg_ref, wu_ref, wd_ref, out_ref = refs[14:18]
    x, stream, wgu, wd, acc, h = refs[18:24]
    keep, y1_out, y1_in, y2_out, y2_in, y3_out, y3_in, y4_out, y4_in, y5_out, y5_in = refs[24:35]
    (load_sem, ws, wr, fs, fr, az_s, az_r, ax_s, ax_r, am_s, am_r,
     s1, r1, s2, r2, s3, r3, s4, r4, s5, r5, met, small_sem) = refs[35:58]
    small = refs[58 : 58 + len(SMALL)]
    mixer_scratch = refs[58 + len(SMALL) :]
    inputs = list(refs[:14])
    fetches = []
    for n, at in enumerate(SMALL):
        fetches.append(pltpu.make_async_copy(inputs[at], small[n], small_sem.at[n]))
        inputs[at] = small[n]
    for fetch in fetches:
        fetch.start()
    own, d_model = stream.shape
    depth, hid = wg_ref.shape
    cols = wd_ref.shape[1]
    wide = wgu.shape[1] // 2
    rows = n_sp * n_tp * own
    parity = me_t % 2
    short = (n_sp - 1) * (1 - parity)
    part_row, part_col = depth // 4, cols // 4
    half_col = 2 * part_col

    side = me_s // 2
    inner = me_s % 2 != side
    partner = me_s + 1 - 2 * (me_s % 2)
    opposite = lax.rem(me_s + 2, n_sp)
    near = [partner, 2 - side, 3 * (1 - side)]
    order = [me_s] + near
    mate = me_t + 1 - 2 * (me_t % 2)
    across = lax.rem(me_t + 2, n_tp)

    def sized(to, act):
        @pl.when(to == short)
        def _():
            act(wide - TILE)

        @pl.when(to != short)
        def _():
            act(wide)

    def first(to):
        return (3 * to - parity * ((to + 3) // 4)) * TILE

    def shipped(k, i, width):
        start = pl.ds(pl.multiple_of(first(near[i]), TILE), width)
        if k < 4:
            at = 2 * me_g + k % 2
            src = (wg_ref, wu_ref)[k // 2].at[aligned(at, part_row), start]
            dst = wgu.at[aligned(4 * me_s + at, part_row), pl.ds(k // 2 * wide, width)]
        else:
            at = 2 * ((k - 4) // 2) + me_g
            skipped, count = k % 2 * (width // 2), width // 2
            start = pl.ds(pl.multiple_of(first(near[i]) + skipped, TILE // 2), count)
            src = wd_ref.at[start, aligned(at, part_col)]
            dst = wd.at[pl.ds(skipped, count), aligned(4 * me_s + at, part_col)]
        return pltpu.make_async_remote_copy(
            src_ref=src, dst_ref=dst, send_sem=ws.at[k, i], recv_sem=wr.at[k, me_s],
            device_id={"sp": near[i]}, device_id_type=MESH,
        )

    def ship(k, i):
        sized(near[i], lambda width: shipped(k, i, width).start())

    def handed(k, i, width):
        at = 4 * near[i] + 2 * me_g + k % 2
        if k < 4:
            return wgu.at[aligned(at, part_row), pl.ds(k // 2 * wide, width)]
        at = 4 * near[i] + 2 * ((k - 4) // 2) + me_g
        return wd.at[pl.ds(k % 2 * (width // 2), width // 2), aligned(at, part_col)]

    def passed(k, i, width):
        piece = handed(k, i, width)
        return pltpu.make_async_remote_copy(
            src_ref=piece, dst_ref=piece, send_sem=fs.at[k, i], recv_sem=fr.at[k, i],
            device_id={"grp": 1 - me_g}, device_id_type=MESH,
        )

    def relay(k, i):
        def act(width):
            piece = handed(k, i, width)
            pltpu.make_async_remote_copy(
                src_ref=piece, dst_ref=piece, send_sem=ws.at[k, i], recv_sem=wr.at[k, near[i]],
                device_id={"sp": near[i]}, device_id_type=MESH,
            ).wait_recv()
            passed(k, i, width).start()

        sized(me_s, act)

    def arrived(k, i):
        sized(me_s, lambda width: passed(k, i, width).wait_recv())

    def own_loads(width):
        start = pl.ds(pl.multiple_of(first(me_s), TILE), width)
        return [
            pltpu.make_async_copy(
                ref.at[:, start], wgu.at[aligned(me_s, depth), pl.ds(k * wide, width)],
                load_sem.at[k],
            )
            for k, ref in enumerate((wg_ref, wu_ref))
        ] + [
            pltpu.make_async_copy(
                wd_ref.at[start, :], wd.at[pl.ds(0, width), aligned(me_s, cols)], load_sem.at[2]
            )
        ]

    def start_loads(width):
        for load in own_loads(width):
            load.start()

    edge = jnp.logical_not(inner)

    def issue(at_inner, at_edge):
        for where, jobs in ((inner, at_inner), (edge, at_edge)):
            @pl.when(where)
            def _():
                for act, *where_to in jobs:
                    act(*where_to)

    ends_in = mixer_scratch[9]
    ends_in[...] = jnp.zeros_like(ends_in)
    greet(sizes, place)
    issue([(ship, 0, 1), (ship, 0, 0)], [(ship, 0, 0)])
    sized(me_s, start_loads)

    @pl.when(me_s == short)
    def _():
        for k in range(2):
            wgu[:, (k + 1) * wide - TILE : (k + 1) * wide] = jnp.zeros((n_sp * depth, TILE), BF16)
        wd[wide - TILE :, :] = jnp.zeros((TILE, d_model), BF16)

    for fetch in fetches:
        fetch.wait()

    def after_ends():
        issue([(ship, 1, 1)] + [(ship, k, 2) for k in range(4)], [])
        for k in (1, 2, 3):
            ship(k, 0)

    mixer(
        n_sp, n_tp, after_ends, *inputs, x.at[me_s, 0], stream, *mixer_scratch
    )

    def along(b, n, to):
        return pltpu.make_async_remote_copy(
            src_ref=x.at[b, 0], dst_ref=x.at[b, 0], send_sem=az_s.at[n], recv_sem=az_r.at[b],
            device_id={"sp": to}, device_id_type=MESH,
        )

    sent = []

    def share(b):
        sent.append(send(x.at[b, 0], x.at[b, 2], ax_s.at[b], ax_r.at[b], tp=across))
        sent.append(send(x.at[b, 0], x.at[b, 1], am_s.at[b, 0], am_r.at[b, 0], tp=mate))

    def spread(b):
        pltpu.make_async_remote_copy(
            src_ref=x.at[b, 2], dst_ref=x.at[b, 2], send_sem=ax_s.at[b], recv_sem=ax_r.at[b],
            device_id={"tp": across}, device_id_type=MESH,
        ).wait_recv()
        sent.append(send(x.at[b, 2], x.at[b, 3], am_s.at[b, 1], am_r.at[b, 1], tp=mate))

    def collected(b):
        for n, slot in ((0, 1), (1, 3)):
            pltpu.make_async_remote_copy(
                src_ref=x.at[b, slot], dst_ref=x.at[b, slot], send_sem=am_s.at[b, n],
                recv_sem=am_r.at[b, n], device_id={"tp": mate}, device_id_type=MESH,
            ).wait_recv()

    def meet(n):
        pl.semaphore_signal(met.at[n], inc=1, device_id={"tp": mate}, device_id_type=MESH)
        pl.semaphore_wait(met.at[n], 1)

    def gone(k, i):
        sized(near[i], lambda width: shipped(k, i, width).wait_send())

    firsthand = [along(me_s, i, near[i]) for i in range(2)]
    for copy in firsthand:
        copy.start()
    share(me_s)

    def gathered(i):
        b = near[i]
        along(b, 0, near[0]).wait_recv()
        if i:
            @pl.when(inner)
            def _():
                along(b, 1 + i, near[0]).start()
        share(b)

    gates, ups, downs = (0, 1), (2, 3), (4, 5, 6, 7)

    def each(act, *groups):
        return [(act, k, i) for ks, i in groups for k in ks]

    issue(each(relay, (gates, 1)), [])
    issue(each(relay, (gates, 0), (ups, 0)), each(relay, (gates, 0), (ups, 0), (gates, 1)))
    for copy in firsthand:
        copy.wait_send()
    meet(0)
    issue(
        each(ship, (ups, 1)),
        each(ship, (gates, 1), (ups, 1), (gates, 2), (ups, 2), (downs, 0)),
    )
    spread(order[0])
    gathered(0)
    issue([], each(relay, (ups, 1)))
    gathered(1)
    spread(order[1])
    gathered(2)
    issue(each(relay, (gates, 2)) + each(ship, (downs, 0)), [])
    spread(order[2])
    spread(order[3])
    issue(each(relay, (ups, 2)), each(relay, (gates, 2)))
    for b in order:
        collected(b)

    def product(b):
        lhs = x[:, :, :, aligned(b, depth)].reshape(rows, depth)
        return jnp.dot(lhs, wgu[aligned(b, depth), :], preferred_element_type=F32)

    def loaded(which):
        def act(width):
            loads = own_loads(width)
            for n in which:
                loads[n].wait()

        sized(me_s, act)

    def landed(i):
        for k in range(4):
            arrived(k, i)

    loaded((0, 1))
    acc[...] = product(me_s)
    landed(0)
    acc[...] += product(near[0])
    issue(each(relay, (ups, 1)), each(relay, (ups, 2)))

    def release():
        for k in ups:
            gone(k, 1)
        issue([], each(gone, (gates, 1), (gates, 2), (ups, 2)))
        meet(1)
        issue(
            [
                (lambda: pl.semaphore_signal(
                    met.at[2], inc=1, device_id={"sp": near[0]}, device_id_type=MESH
                ),)
            ],
            [(lambda: pl.semaphore_wait(met.at[2], 1),)],
        )
        for i in (2, 1):
            for k in downs:
                ship(k, i)

    pl.when(inner)(release)

    def add(i):
        landed(i)
        acc[...] += product(near[i])

    pl.when(inner)(lambda: add(2))
    pl.when(edge)(lambda: add(1))
    for k in downs:
        relay(k, 0)
    pl.when(edge)(release)
    last = jnp.where(inner, near[1], near[2])
    pl.when(inner)(lambda: landed(1))
    pl.when(edge)(lambda: landed(2))
    total = acc[...] + product(last)
    h[...] = (jax.nn.silu(total[:, :wide]) * total[:, wide:]).astype(BF16)

    blocks = [(i, q) for i in (0, 1, 3, 2) for q in range(2)]
    held = len(blocks) // 2
    steps = [(n, None) for n in range(6)] + [(n, g) for g in (me_g, 1 - me_g) for n in (6, 7)]

    def place_of(n):
        i, q = blocks[n]
        return 2 * order[i] + q

    def lanes_of(m):
        part = steps[m][1]
        return (half_col, pl.ds(0, half_col)) if part is None else (
            part_col, aligned(part, part_col)
        )

    def columns(m):
        n, part = steps[m]
        if part is None:
            return aligned(place_of(n), half_col)
        return aligned(2 * place_of(n) + part, part_col)

    firsts, turns = {}, {}

    def down(m):
        n, part = steps[m]
        i, q = blocks[n]
        if i and m not in (6, 7):
            arrived(downs[2 * q], i - 1)
            arrived(downs[2 * q + 1], i - 1)
        width = lanes_of(m)[0]
        y = jnp.dot(h[...], wd[:, columns(m)], preferred_element_type=F32)
        y = y.reshape(n_sp, n_tp, own, width)
        y1_out[m, 0, :, :, :width] = y[:, 1].astype(BF16)
        y1_out[m, 1, :, :, :width] = y[:, 3].astype(BF16)
        piece = (m, slice(None), slice(None), slice(None), pl.ds(0, width))
        firsts[m] = send(y1_out.at[piece], y1_in.at[piece], s1.at[m], r1.at[m], tp=mate)
        keep[m, 0, :, :, :width] = y[:, 0]
        keep[m, 1, :, :, :width] = y[:, 2]

    def stage_two(m):
        width = lanes_of(m)[0]
        firsts[m].wait_recv()
        y2_out[m, :, :, :width] = (
            keep[m, 1, :, :, :width] + y1_in[m, 1, :, :, :width].astype(F32)
        ).astype(BF16)
        piece = (m, slice(None), slice(None), pl.ds(0, width))
        turns[m] = send(y2_out.at[piece], y2_in.at[piece], s2.at[m], r2.at[m], tp=across)
        keep[m, 0, :, :, :width] += y1_in[m, 0, :, :, :width].astype(F32)

    def paired(n):
        c = place_of(n)
        piece = y3_in.at[c] if n < held else y3_in.at[c, 0]
        return pltpu.make_async_remote_copy(
            src_ref=piece, dst_ref=piece, send_sem=s3.at[c], recv_sem=r3.at[c],
            device_id={"sp": partner}, device_id_type=MESH,
        )

    def crossed(n):
        c = place_of(n)
        return pltpu.make_async_remote_copy(
            src_ref=y4_out.at[c], dst_ref=y4_in.at[c], send_sem=s4.at[c], recv_sem=r4.at[c],
            device_id={"sp": opposite}, device_id_type=MESH,
        )

    def straight(n, j):
        return pltpu.make_async_remote_copy(
            src_ref=y5_out.at[n - held, j], dst_ref=y5_in.at[0, 0],
            send_sem=s5.at[n - held, j], recv_sem=r5.at[0, 0],
            device_id={"sp": 2 - 2 * side + j}, device_id_type=MESH,
        )

    def stage_three(m):
        n, part = steps[m]
        c = place_of(n)
        width, lanes = lanes_of(m)
        turns[m].wait_recv()
        keep[m, 0, :, :, :width] += y2_in[m, :, :, :width].astype(F32)
        if n < held:
            for k, row in enumerate((partner, lax.rem(partner + 2, n_sp))):
                y3_out[c, k] = keep[m, 0, row].astype(BF16)
            send(y3_out.at[c], y3_in.at[c], s3.at[c], r3.at[c], sp=partner)
            return
        y3_out[c, 0, :, lanes] = keep[m, 0, partner, :, :width].astype(BF16)
        piece = (c, 0, slice(None), lanes)
        send(y3_out.at[piece], y3_in.at[piece], s3.at[c], r3.at[c], sp=partner)
        for j in range(2):
            far = 2 - 2 * side + j
            y5_out[n - held, j, :, lanes] = keep[m, 0, far, :, :width].astype(BF16)
            send(y5_out.at[n - held, j, :, lanes], y5_in.at[c % held, me_s % 2, :, lanes],
                 s5.at[n - held, j], r5.at[c % held, me_s % 2], sp=far)

    def stage_four(n):
        c = place_of(n)
        paired(n).wait_recv()
        y4_out[c] = (keep[n, 0, opposite] + y3_in[c, 1].astype(F32)).astype(BF16)
        crossed(n).start()
        at = aligned(c, half_col)
        stream[:, at] += keep[n, 0, me_s] + y3_in[c, 0].astype(F32)

    def finish(n):
        c = place_of(n)
        if n < held:
            at = aligned(c, half_col)
            total = stream[:, at]
            for j in range(2):
                piece = y5_in.at[c % held, j]
                pltpu.make_async_remote_copy(
                    src_ref=piece, dst_ref=piece, send_sem=s5.at[0, j],
                    recv_sem=r5.at[c % held, j], device_id={"sp": opposite}, device_id_type=MESH,
                ).wait_recv()
                total += y5_in[c % held, j].astype(F32)
            out_ref[:, at] = total.astype(BF16)
            return
        paired(n).wait_recv()
        crossed(n).wait_recv()
        for m, (half, part) in enumerate(steps):
            if half == n:
                width, lanes = lanes_of(m)
                at = columns(m)
                out_ref[:, at] = (
                    stream[:, at] + keep[m, 0, me_s, :, :width]
                    + y3_in[c, 0, :, lanes].astype(F32) + y4_in[c, :, lanes].astype(F32)
                ).astype(BF16)

    loaded((2,))
    for m in range(6):
        if m in (1, 2):
            relay(downs[2 * m - 2], 2)
            relay(downs[2 * m - 1], 2)
        if m == 4:
            relay(downs[0], 1)
            relay(downs[1], 1)
        if m == 5:
            relay(downs[2], 1)
            relay(downs[3], 1)
        if m > held:
            stage_two(m - 1)
        down(m)
        if 1 <= m <= held:
            stage_two(m - 1)
        if m >= 3:
            stage_three(m - 3)
    down(6)
    down(7)
    for m in (5, 6, 7):
        stage_two(m)
    stage_three(3)
    issue([(stage_four, 0), (stage_four, 1)], [])
    down(8)
    stage_three(4)
    issue([(stage_four, 2), (stage_four, 3)], [])
    down(9)
    stage_two(8)
    stage_three(5)
    stage_three(6)
    stage_two(9)
    stage_three(7)
    issue([], [(stage_four, 0), (stage_four, 1)])
    stage_three(8)
    issue([], [(stage_four, 2), (stage_four, 3)])
    stage_three(9)
    for copy in sent + [d[n] for d in (firsts, turns) for n in d]:
        copy.wait_send()

    @pl.when(inner)
    def _():
        for n in (2, 3):
            along(me_s, n, near[0]).wait_send()

    issue(each(gone, (gates, 1), (gates, 2), (ups, 2)), [])
    for k in range(8):
        for i in range(3):
            if i == 0 or k > 3:
                gone(k, i)
            sized(me_s, lambda width: passed(k, i, width).wait_send())
    for n in (4, 5, 0, 1, 2, 3, 6, 7):
        finish(n)
    for n in range(len(blocks)):
        paired(n).wait_send()
        if n < held:
            crossed(n).wait_send()
        else:
            for j in range(2):
                straight(n, j).wait_send()


def moved_weights(
    ssm_input, residual_in, log_step, decay_real, freq, in_real, in_imag, out_real, out_imag,
    skip, w_glu, b_glu, w_branch, norm_gain, w_gate, w_up, w_down,
):
    sizes = {axis: lax.axis_size(axis) for axis in ("grp", "sp", "tp")}
    n_sp, n_tp = sizes["sp"], sizes["tp"]
    tok, width = ssm_input.shape
    groups, states = decay_real.shape
    group = in_real.shape[2]
    lanes = groups * states
    own = tok // n_tp
    chan, d_model = w_branch.shape
    depth, hid = w_gate.shape
    cols = w_down.shape[1]
    wide = -(-hid // (TILE * n_sp)) * TILE
    rows = n_sp * tok
    operands = (
        ssm_input, residual_in, log_step[None], decay_real, freq,
        in_real.swapaxes(1, 2).reshape(width, states),
        in_imag.swapaxes(1, 2).reshape(width, states),
        out_real.reshape(width, states), out_imag.reshape(width, states),
        skip[None], w_glu, b_glu[None], w_branch, norm_gain[None], w_gate, w_up, w_down,
    )
    blocks, steps = 2 * n_sp, 2 * n_sp + 2
    vm = pl.BlockSpec(memory_space=pltpu.VMEM)
    hbm = pl.BlockSpec(memory_space=pl.ANY)
    dma = pltpu.SemaphoreType.DMA
    vmem = pltpu.VMEM
    return pl.pallas_call(
        functools.partial(layer_kernel, sizes),
        out_shape=pltpu.VMEM((own, d_model), BF16),
        in_specs=[hbm] * len(operands),
        out_specs=vm,
        scratch_shapes=[
            vmem((n_sp, n_tp, own, d_model), BF16),
            vmem((own, d_model), F32),
            vmem((d_model, 2 * wide), BF16),
            vmem((wide, d_model), BF16),
            vmem((rows, 2 * wide), F32),
            vmem((rows, wide), BF16),
            vmem((steps, 2, n_sp, own, cols // 2), F32),
            vmem((steps, 2, n_sp, own, cols // 2), BF16),
            vmem((steps, 2, n_sp, own, cols // 2), BF16),
            vmem((steps, n_sp, own, cols // 2), BF16),
            vmem((steps, n_sp, own, cols // 2), BF16),
            vmem((blocks, 2, own, cols // 2), BF16),
            vmem((blocks, 2, own, cols // 2), BF16),
            vmem((blocks, own, cols // 2), BF16),
            vmem((blocks, own, cols // 2), BF16),
            vmem((blocks // 2, 2, own, cols // 2), BF16),
            vmem((blocks // 2, 2, own, cols // 2), BF16),
            dma((3,)),
            dma((8, 3)), dma((8, n_sp)), dma((8, 3)), dma((8, 3)),
            dma((4,)), dma((n_sp,)),
            dma((n_sp,)), dma((n_sp,)),
            dma((n_sp, 2)), dma((n_sp, 2)),
            dma((steps,)), dma((steps,)), dma((steps,)), dma((steps,)),
            dma((blocks,)), dma((blocks,)), dma((blocks,)), dma((blocks,)),
            dma((blocks // 2, 2)), dma((blocks // 2, 2)),
            pltpu.SemaphoreType.REGULAR((3,)),
            dma((len(SMALL),)),
            *[vmem(operands[at].shape, operands[at].dtype) for at in SMALL],
            vmem((chan, chan), BF16),
            vmem((chan, d_model), BF16),
            vmem((own, d_model), BF16),
            vmem((8, lanes), F32),
            vmem((tok, lanes), F32),
            vmem((tok, lanes), F32),
            vmem((tok, lanes), F32),
            vmem((tok, lanes), F32),
            vmem((2, lanes), F32),
            vmem((n_sp - 1, 2, lanes), F32),
            vmem((n_tp, own, width), BF16),
            vmem((n_tp - 1, own, width), BF16),
            vmem((own, chan), F32),
            dma((3,)),
            dma((n_sp - 1,)), dma((n_sp - 1,)),
            dma((n_tp - 1,)), dma((n_tp - 1,)),
        ],
        compiler_params=pltpu.CompilerParams(collective_id=0, has_side_effects=True),
        name="layer",
    )(*operands)


def per_device(*arguments):
    sizes = tuple(lax.axis_size(axis) for axis in ("grp", "sp", "tp"))
    tiles = arguments[14].shape[1] // TILE
    fits = sizes == (2, 4, 4) and tiles % 4 == 3
    return (moved_weights if fits else gathered_weights)(*arguments)


def solution(mesh):
    placed = (
        P(("grp", "sp"), "tp"),
        P(("grp", "sp"), None),
        P("tp"),
        P("tp", None),
        P("tp", None),
        P("tp", None, None),
        P("tp", None, None),
        P("tp", None, None),
        P("tp", None, None),
        P("tp"),
        P(),
        P(),
        P(),
        P(),
        P("sp", "tp"),
        P("sp", "tp"),
        P("tp", "sp"),
    )
    return jax.shard_map(
        per_device,
        mesh=mesh,
        in_specs=placed,
        out_specs=P(("grp", "sp", "tp"), None),
        check_vma=False,
    )
```

```python
import functools
import math

import jax
import jax.numpy as jnp
from jax import lax
from jax.experimental import pallas as pl
from jax.experimental.pallas import tpu as pltpu
from jax.sharding import PartitionSpec as P

EPS = 1e-06


def prefix(shard, axis, combine, identity):
    count, place = (lax.axis_size(axis), lax.axis_index(axis))
    everything = jax.tree.map(lambda part: lax.all_gather(part, axis), shard)
    start = jax.tree.map(
        lambda part, zero: jnp.broadcast_to(jnp.asarray(zero, part.dtype), part.shape),
        shard,
        identity,
    )

    def lap(k, before):
        reached = k < place
        new = combine(before, jax.tree.map(lambda part: part[k], everything))
        return jax.tree.map(lambda a, b: jnp.where(reached, a, b), new, before)

    return lax.fori_loop(0, count, lap, start)


def discretize(log_step, decay_real, freq, in_real, in_imag):
    step_size = jnp.exp(log_step)[:, None]
    magnitude = jnp.exp(decay_real * step_size)
    abar_re = magnitude * jnp.cos(freq * step_size)
    abar_im = magnitude * jnp.sin(freq * step_size)
    denominator = decay_real * decay_real + freq * freq
    less_re = abar_re - 1.0
    hold_re = ((less_re * decay_real + abar_im * freq) / denominator)[..., None]
    hold_im = ((abar_im * decay_real - less_re * freq) / denominator)[..., None]
    bbar_re = hold_re * in_real - hold_im * in_imag
    bbar_im = hold_re * in_imag + hold_im * in_real
    return (step_size, abar_re, abar_im, bbar_re, bbar_im)


def powers(decay_real, freq, step_size, length):
    steps_up = (jnp.arange(length, dtype=jnp.int32) + 1).astype(jnp.float32)[:, None, None]
    magnitude = jnp.exp((decay_real * step_size)[None] * steps_up)
    phase = (freq * step_size)[None] * steps_up
    return (magnitude * jnp.cos(phase), magnitude * jnp.sin(phase))


def compose(earlier, later):
    a1r, a1i, b1r, b1i = earlier
    a2r, a2i, b2r, b2i = later
    return (
        a2r * a1r - a2i * a1i,
        a2r * a1i + a2i * a1r,
        a2r * b1r - a2i * b1i + b2r,
        a2r * b1i + a2i * b1r + b2i,
    )


def local_states(inputs, decay_real, freq, step_size, bbar_re, bbar_im):
    highest = lax.Precision.HIGHEST
    tok_rows, group_count, unused = inputs.shape
    lanes = group_count * decay_real.shape[1]
    drive_re = jnp.einsum("lgm,gpm->lgp", inputs, bbar_re, precision=highest).reshape(
        tok_rows, lanes
    )
    drive_im = jnp.einsum("lgm,gpm->lgp", inputs, bbar_im, precision=highest).reshape(
        tok_rows, lanes
    )
    span = math.gcd(tok_rows, 16)
    spans = tok_rows // span
    rate = (decay_real * step_size).reshape(lanes)
    turn = (freq * step_size).reshape(lanes)
    later = jnp.arange(span, dtype=jnp.int32)[:, None]
    earlier = jnp.arange(span, dtype=jnp.int32)[None, :]
    lag = (later - earlier).astype(jnp.float32)
    causal = (later >= earlier)[..., None]
    lag_pos = jnp.maximum(lag, 0.0)[..., None]
    table_mag = jnp.exp(rate[None, None] * lag_pos)
    table_re = jnp.where(causal, table_mag * jnp.cos(turn[None, None] * lag_pos), 0.0)
    table_im = jnp.where(causal, table_mag * jnp.sin(turn[None, None] * lag_pos), 0.0)
    block_re = drive_re.reshape(spans, 1, span, lanes)
    block_im = drive_im.reshape(spans, 1, span, lanes)
    inner_re = jnp.sum(table_re[None] * block_re - table_im[None] * block_im, axis=2)
    inner_im = jnp.sum(table_re[None] * block_im + table_im[None] * block_re, axis=2)
    steps_up = (jnp.arange(span, dtype=jnp.int32) + 1).astype(jnp.float32)[:, None]
    pow_mag = jnp.exp(rate[None] * steps_up)
    pow_re = pow_mag * jnp.cos(turn[None] * steps_up)
    pow_im = pow_mag * jnp.sin(turn[None] * steps_up)
    span_re = pow_re[-1]
    span_im = pow_im[-1]

    def carry_step(entering, ends):
        next_re = span_re * entering[0] - span_im * entering[1] + ends[0]
        next_im = span_re * entering[1] + span_im * entering[0] + ends[1]
        return ((next_re, next_im), entering)

    zeros = jnp.zeros((lanes,), jnp.float32)
    unused_carry, entering = lax.scan(
        carry_step, (zeros, zeros), (inner_re[:, -1], inner_im[:, -1])
    )
    state_re = inner_re + pow_re[None] * entering[0][:, None] - pow_im[None] * entering[1][:, None]
    state_im = inner_im + pow_re[None] * entering[1][:, None] + pow_im[None] * entering[0][:, None]
    shape = (tok_rows, group_count, decay_real.shape[1])
    return (state_re.reshape(shape), state_im.reshape(shape))


def readout(state_re, state_im, out_real, out_imag, skip_mat, inputs):
    highest = lax.Precision.HIGHEST
    values = (
        jnp.einsum("lgp,gmp->lgm", state_re, out_real, precision=highest)
        - jnp.einsum("lgp,gmp->lgm", state_im, out_imag, precision=highest)
        + skip_mat[None] * inputs
    )
    values = jax.nn.gelu(values)
    return values.reshape(values.shape[0], -1).astype(jnp.bfloat16)


def row_norm(stream, norm_gain):
    scale_rows = lax.rsqrt(jnp.mean(stream * stream, axis=-1, keepdims=True) + EPS)
    return (stream * scale_rows * norm_gain).astype(jnp.bfloat16)


def gathered_weights(
    ssm_input,
    residual_in,
    log_step,
    decay_real,
    freq,
    in_real,
    in_imag,
    out_real,
    out_imag,
    skip,
    w_glu,
    b_glu,
    w_branch,
    norm_gain,
    w_gate,
    w_up,
    w_down,
):
    tok_rows, width_local = ssm_input.shape
    group_count = log_step.shape[0]
    group_size = in_real.shape[2]
    tp_count = lax.axis_size("tp")
    tp_index = lax.axis_index("tp")
    own_rows = tok_rows // tp_count
    step_size, abar_re, abar_im, bbar_re, bbar_im = discretize(
        log_step, decay_real, freq, in_real, in_imag
    )
    pow_re, pow_im = powers(decay_real, freq, step_size, tok_rows)
    inputs = ssm_input.astype(jnp.float32).reshape(tok_rows, group_count, group_size)
    local_re, local_im = local_states(inputs, decay_real, freq, step_size, bbar_re, bbar_im)
    identity = (
        jnp.ones_like(abar_re),
        jnp.zeros_like(abar_re),
        jnp.zeros_like(abar_re),
        jnp.zeros_like(abar_re),
    )
    carried = prefix((pow_re[-1], pow_im[-1], local_re[-1], local_im[-1]), "sp", compose, identity)
    state_re = local_re + pow_re * carried[2][None] - pow_im * carried[3][None]
    state_im = local_im + pow_re * carried[3][None] + pow_im * carried[2][None]
    mixer_out = readout(
        state_re, state_im, out_real, out_imag, skip.reshape(group_count, group_size), inputs
    )
    mixer_rows = lax.all_to_all(mixer_out, "tp", split_axis=0, concat_axis=1, tiled=True)
    glu_pre = jnp.dot(mixer_rows, w_glu, preferred_element_type=jnp.float32) + b_glu
    gated = (mixer_rows.astype(jnp.float32) * jax.nn.sigmoid(glu_pre)).astype(jnp.bfloat16)
    residual_own = lax.dynamic_slice_in_dim(residual_in, tp_index * own_rows, own_rows, 0)
    stream = residual_own.astype(jnp.float32) + jnp.dot(
        gated, w_branch, preferred_element_type=jnp.float32
    )
    normed = row_norm(stream, norm_gain)
    normed_all = lax.all_gather(normed, "tp", axis=0, tiled=True)
    gate_sum = jnp.dot(
        normed_all,
        lax.all_gather(w_gate, "sp", axis=0, tiled=True),
        preferred_element_type=jnp.float32,
    )
    up_sum = jnp.dot(
        normed_all,
        lax.all_gather(w_up, "sp", axis=0, tiled=True),
        preferred_element_type=jnp.float32,
    )
    hidden = (jax.nn.silu(gate_sum) * up_sum).astype(jnp.bfloat16)
    down_whole = lax.all_gather(w_down, "sp", axis=1, tiled=True)
    summed = lax.psum_scatter(
        jnp.dot(hidden, down_whole, preferred_element_type=jnp.float32).astype(jnp.bfloat16),
        "tp",
        scatter_dimension=0,
        tiled=True,
    ).astype(jnp.float32)
    return (stream + summed).astype(jnp.bfloat16)


MESH = pl.DeviceIdType.MESH
F32 = jnp.float32
BF16 = jnp.bfloat16
NT = (((1,), (1,)), ((), ()))


def greet(sizes, place):
    barrier = pltpu.get_barrier_semaphore()
    for axis in sizes:
        for d in range(1, sizes[axis]):
            pl.semaphore_signal(
                barrier, inc=1, device_id={axis: lax.rem(place[axis] + d, sizes[axis])},
                device_id_type=MESH,
            )
    pl.semaphore_wait(barrier, sum(sizes.values()) - len(sizes))


def send(src, dst, ss, rs, **to):
    copy = pltpu.make_async_remote_copy(
        src_ref=src, dst_ref=dst, send_sem=ss, recv_sem=rs, device_id=to, device_id_type=MESH
    )
    copy.start()
    return copy


def aligned(index, size):
    return pl.ds(pl.multiple_of(index * size, size), size)


def mixer(
    n_sp, n_tp, after_ends,
    u_ref, res_ref, ls_ref, dec_ref, frq_ref, inr_ref, ini_ref, outr_ref, outi_ref,
    skip_ref, wglu_ref, bglu_ref, wbr_ref, gain_ref,
    normed_ref, stream_ref,
    wglu, wbr, res, coef, xr, xi, pr_all, pi_all, fin, fin_in, mo, rows_in, glu,
    load_sem, fs, fr, rs, rr,
):
    me_s, me_t = lax.axis_index("sp"), lax.axis_index("tp")
    tok, width = u_ref.shape
    groups, states = dec_ref.shape
    group = width // groups
    lanes = groups * states
    own = tok // n_tp
    loads = [
        pltpu.make_async_copy(
            res_ref.at[pl.ds(pl.multiple_of(me_t * own, own), own)], res, load_sem.at[0]
        ),
        pltpu.make_async_copy(wglu_ref, wglu, load_sem.at[1]),
        pltpu.make_async_copy(wbr_ref, wbr, load_sem.at[2]),
    ]
    for load in loads:
        load.start()

    same = lax.broadcasted_iota(jnp.int32, (groups, groups), 0) == lax.broadcasted_iota(
        jnp.int32, (groups, groups), 1
    )
    step = jnp.exp(jnp.sum(jnp.where(same, ls_ref[...], 0.0), axis=1, keepdims=True))
    dec, frq = dec_ref[...], frq_ref[...]
    mag = jnp.exp(dec * step)
    ar = mag * jnp.cos(frq * step)
    ai = mag * jnp.sin(frq * step)
    den = dec * dec + frq * frq
    less = ar - 1.0
    hr = (less * dec + ai * frq) / den
    hi = (ai * dec - less * frq) / den
    for g in range(groups):
        at = slice(g * states, (g + 1) * states)
        coef[0:1, at] = ar[g : g + 1, :]
        coef[1:2, at] = ai[g : g + 1, :]
        coef[2:3, at] = hr[g : g + 1, :]
        coef[3:4, at] = hi[g : g + 1, :]

    u = u_ref[...]
    part = 128
    spread = (
        lax.broadcasted_iota(jnp.int32, (states, part), 1) % states
        == lax.broadcasted_iota(jnp.int32, (states, part), 0)
    ).astype(BF16)
    rows_group = lax.broadcasted_iota(jnp.int32, (width, part), 0) // group
    lane_group = lax.broadcasted_iota(jnp.int32, (width, part), 1) // states

    def spread_out(ref):
        return jnp.dot(ref[...].astype(BF16), spread, preferred_element_type=F32)

    def only(wide, c):
        return jnp.where(rows_group == lane_group + c * (part // states), wide, 0.0).astype(BF16)

    in_r, in_i = spread_out(inr_ref), spread_out(ini_ref)
    row = lax.broadcasted_iota(jnp.int32, (tok, part), 0)
    row8 = lax.broadcasted_iota(jnp.int32, (8, part), 0)
    for c in range(lanes // part):
        at = slice(c * part, (c + 1) * part)
        vr = jnp.dot(u, only(in_r, c), preferred_element_type=F32)
        vi = jnp.dot(u, only(in_i, c), preferred_element_type=F32)
        cr, ci = coef[2:3, at], coef[3:4, at]
        sr, si = cr * vr - ci * vi, cr * vi + ci * vr
        pr, pi = coef[0:1, at], coef[1:2, at]
        tr, ti = jnp.ones((8, part), F32), jnp.zeros((8, part), F32)
        s = 1
        while s <= tok:
            if s <= 8:
                bit = ((row8 + 1) & s) != 0
                br, bi = jnp.where(bit, pr, 1.0), jnp.where(bit, pi, 0.0)
                tr, ti = tr * br - ti * bi, tr * bi + ti * br
            if s >= 8 and s < tok:
                tr, ti = (
                    jnp.concatenate([tr, tr * pr - ti * pi], 0),
                    jnp.concatenate([ti, tr * pi + ti * pr], 0),
                )
            if s < tok:
                if s < 8:
                    yr = jnp.where(row >= s, pltpu.roll(sr, s, 0), 0.0)
                    yi = jnp.where(row >= s, pltpu.roll(si, s, 0), 0.0)
                else:
                    gap = jnp.zeros((s, part), F32)
                    yr = jnp.concatenate([gap, sr[: tok - s]], 0)
                    yi = jnp.concatenate([gap, si[: tok - s]], 0)
                sr, si = sr + (pr * yr - pi * yi), si + (pr * yi + pi * yr)
            pr, pi = pr * pr - pi * pi, 2.0 * pr * pi
            s *= 2
        xr[:, at], xi[:, at] = sr, si
        pr_all[:, at], pi_all[:, at] = tr, ti
        fin[0:1, at] = sr[tok - 1 : tok]
        fin[1:2, at] = si[tok - 1 : tok]

    def end_to(d):
        return pltpu.make_async_remote_copy(
            src_ref=fin, dst_ref=fin_in.at[d - 1], send_sem=fs.at[d - 1], recv_sem=fr.at[d - 1],
            device_id={"sp": lax.rem(me_s + d, n_sp)}, device_id_type=MESH,
        )

    for d in range(1, n_sp):
        @pl.when(me_s + d < n_sp)
        def _():
            end_to(d).start()
    after_ends()

    out_r, out_i = spread_out(outr_ref), spread_out(outi_ref)
    outr = jnp.concatenate([only(out_r, c) for c in range(lanes // part)], axis=1)
    outi = jnp.concatenate([only(out_i, c) for c in range(lanes // part)], axis=1)
    for d in range(1, n_sp):
        @pl.when(me_s >= d)
        def _():
            end_to(d).wait_recv()
    er, ei = pr_all[tok - 1 : tok, :], pi_all[tok - 1 : tok, :]
    pr, pi = jnp.ones((1, lanes), F32), jnp.zeros((1, lanes), F32)
    cr, ci = jnp.zeros((1, lanes), F32), jnp.zeros((1, lanes), F32)
    for d in range(1, n_sp):
        fr_, fi_ = fin_in[d - 1, 0:1, :], fin_in[d - 1, 1:2, :]
        reached = me_s >= d
        cr = cr + jnp.where(reached, pr * fr_ - pi * fi_, 0.0)
        ci = ci + jnp.where(reached, pr * fi_ + pi * fr_, 0.0)
        pr, pi = pr * er - pi * ei, pr * ei + pi * er
    tr, ti = pr_all[...], pi_all[...]
    sr = (xr[...] + (tr * cr - ti * ci)).astype(BF16)
    si = (xi[...] + (tr * ci + ti * cr)).astype(BF16)
    y = lax.dot_general(sr, outr, NT, preferred_element_type=F32) - lax.dot_general(
        si, outi, NT, preferred_element_type=F32
    )
    for d in range(1, n_sp):
        @pl.when(me_s + d < n_sp)
        def _():
            end_to(d).wait_send()
    y = jax.nn.gelu(y + skip_ref[...] * u.astype(F32))
    mo[...] = y.astype(BF16).reshape(n_tp, own, width)
    turns = []
    for d in range(1, n_tp):
        to = lax.rem(me_t + d, n_tp)
        copy = pltpu.make_async_remote_copy(
            src_ref=mo.at[to], dst_ref=rows_in.at[d - 1], send_sem=rs.at[d - 1],
            recv_sem=rr.at[d - 1], device_id={"tp": to}, device_id_type=MESH,
        )
        copy.start()
        turns.append(copy)
    for load in loads:
        load.wait()

    def source(d):
        return pl.ds(pl.multiple_of(lax.rem(me_t + n_tp - d, n_tp) * width, width), width)

    blocks = [mo[me_t]]
    pre = bglu_ref[...] + jnp.dot(blocks[0], wglu[source(0), :], preferred_element_type=F32)
    for d in range(1, n_tp):
        turns[d - 1].wait()
        blocks.append(rows_in[d - 1])
        pre = pre + jnp.dot(blocks[d], wglu[source(d), :], preferred_element_type=F32)
    glu[...] = pre
    stream = res[...].astype(F32)
    for d in range(n_tp):
        gate = jax.nn.sigmoid(glu[:, source(d)])
        gated = (blocks[d].astype(F32) * gate).astype(BF16)
        stream = stream + jnp.dot(gated, wbr[source(d), :], preferred_element_type=F32)
    stream_ref[...] = stream
    scale = lax.rsqrt(jnp.mean(stream * stream, axis=-1, keepdims=True) + EPS)
    normed_ref[...] = (stream * scale * gain_ref[...]).astype(BF16)


TILE = 128
SMALL = (0, 2, 3, 4, 5, 6, 7, 8, 9, 11, 13)


def layer_kernel(sizes, *refs):
    n_sp, n_tp = sizes["sp"], sizes["tp"]
    place = {axis: lax.axis_index(axis) for axis in sizes}
    me_g, me_s, me_t = place["grp"], place["sp"], place["tp"]
    wg_ref, wu_ref, wd_ref, out_ref = refs[14:18]
    x, stream, wgu, wd, acc, h = refs[18:24]
    keep, y1_out, y1_in, y2_out, y2_in, y3_out, y3_in, y4_out, y4_in, y5_out, y5_in = refs[24:35]
    (load_sem, ws, wr, fs, fr, az_s, az_r, ax_s, ax_r, am_s, am_r,
     s1, r1, s2, r2, s3, r3, s4, r4, s5, r5, met, small_sem) = refs[35:58]
    small = refs[58 : 58 + len(SMALL)]
    mixer_scratch = refs[58 + len(SMALL) :]
    inputs = list(refs[:14])
    fetches = []
    for n, at in enumerate(SMALL):
        fetches.append(pltpu.make_async_copy(inputs[at], small[n], small_sem.at[n]))
        inputs[at] = small[n]
    for fetch in fetches:
        fetch.start()
    own, d_model = stream.shape
    depth, hid = wg_ref.shape
    cols = wd_ref.shape[1]
    wide = wgu.shape[1] // 2
    rows = n_sp * n_tp * own
    parity = me_t % 2
    short = (n_sp - 1) * (1 - parity)
    part_row, part_col = depth // 4, cols // 4
    half_col = 2 * part_col

    side = me_s // 2
    inner = me_s % 2 != side
    partner = me_s + 1 - 2 * (me_s % 2)
    opposite = lax.rem(me_s + 2, n_sp)
    near = [partner, 2 - side, 3 * (1 - side)]
    order = [me_s] + near
    far_slot = 2 - (me_s % 2 + side) % 2
    slots = [0, far_slot, far_slot]
    mate = me_t + 1 - 2 * (me_t % 2)
    across = lax.rem(me_t + 2, n_tp)

    def sized(to, act):
        @pl.when(to == short)
        def _():
            act(wide - TILE)

        @pl.when(to != short)
        def _():
            act(wide)

    def first(to):
        return (3 * to - parity * ((to + 3) // 4)) * TILE

    def shipped(k, i, width):
        start = pl.ds(pl.multiple_of(first(near[i]), TILE), width)
        if k < 4:
            at = 2 * me_g + k % 2
            src = (wg_ref, wu_ref)[k // 2].at[aligned(at, part_row), start]
            dst = wgu.at[aligned(4 * me_s + at, part_row), pl.ds(k // 2 * wide, width)]
        else:
            at = 2 * ((k - 4) // 2) + me_g
            skipped, count = k % 2 * (width // 2), width // 2
            start = pl.ds(pl.multiple_of(first(near[i]) + skipped, TILE // 2), count)
            src = wd_ref.at[start, aligned(at, part_col)]
            dst = wd.at[pl.ds(skipped, count), aligned(4 * me_s + at, part_col)]
        return pltpu.make_async_remote_copy(
            src_ref=src, dst_ref=dst, send_sem=ws.at[k // 4, i],
            recv_sem=wr.at[max(k - 1, 0), slots[i]],
            device_id={"sp": near[i]}, device_id_type=MESH,
        )

    def ship(k, i):
        sized(near[i], lambda width: shipped(k, i, width).start())

    def handed(k, i, width):
        at = 4 * near[i] + 2 * me_g + k % 2
        if k == 0:
            return wgu.at[aligned(2 * near[i] + me_g, 2 * part_row), pl.ds(0, width)]
        if k < 4:
            return wgu.at[aligned(at, part_row), pl.ds(k // 2 * wide, width)]
        at = 4 * near[i] + 2 * ((k - 4) // 2) + me_g
        return wd.at[pl.ds(k % 2 * (width // 2), width // 2), aligned(at, part_col)]

    def whole(k, width, half=False):
        if k < 4:
            return wgu.at[pl.ds(0, 4 * part_row), pl.ds(0, width)]
        return wd.at[pl.ds(0, width), pl.ds(0, part_col if half else half_col)]

    def passed(k, i, piece):
        return pltpu.make_async_remote_copy(
            src_ref=piece, dst_ref=piece, send_sem=fs.at[k // 4, i],
            recv_sem=fr.at[k // 4 * (k // 2 - 1), i],
            device_id={"grp": 1 - me_g}, device_id_type=MESH,
        )

    def relay(k, i):
        def act(width):
            piece = handed(k, i, width)
            pltpu.make_async_remote_copy(
                src_ref=piece, dst_ref=piece, send_sem=ws.at[k // 4, i],
                recv_sem=wr.at[max(k - 1, 0), i],
                device_id={"sp": near[i]}, device_id_type=MESH,
            ).wait_recv()
            passed(k, i, piece).start()

        sized(me_s, act)

    def arrived(k, i):
        sized(me_s, lambda width: passed(k, i, whole(k, width, True)).wait_recv())

    def gone(k, i):
        def act(width):
            piece = whole(k, width)
            pltpu.make_async_remote_copy(
                src_ref=piece, dst_ref=piece, send_sem=ws.at[k // 4, i], recv_sem=wr.at[0, i],
                device_id={"sp": near[i]}, device_id_type=MESH,
            ).wait_send()

        sized(near[i], act)

    def own_loads(width):
        start = pl.ds(pl.multiple_of(first(me_s), TILE), width)
        return [
            pltpu.make_async_copy(
                ref.at[:, start], wgu.at[aligned(me_s, depth), pl.ds(k * wide, width)],
                load_sem.at[k],
            )
            for k, ref in enumerate((wg_ref, wu_ref))
        ] + [
            pltpu.make_async_copy(
                wd_ref.at[start, :], wd.at[pl.ds(0, width), aligned(me_s, cols)], load_sem.at[2]
            )
        ]

    def start_loads(width):
        for load in own_loads(width):
            load.start()

    edge = jnp.logical_not(inner)

    def issue(at_inner, at_edge):
        for where, jobs in ((inner, at_inner), (edge, at_edge)):
            @pl.when(where)
            def _():
                for act, *where_to in jobs:
                    act(*where_to)

    ends_in = mixer_scratch[9]
    ends_in[...] = jnp.zeros_like(ends_in)
    greet(sizes, place)
    issue([(ship, 0, 1), (ship, 0, 0)], [(ship, 0, 0)])
    sized(me_s, start_loads)

    @pl.when(me_s == short)
    def _():
        for k in range(2):
            wgu[:, (k + 1) * wide - TILE : (k + 1) * wide] = jnp.zeros((n_sp * depth, TILE), BF16)
        wd[wide - TILE :, :] = jnp.zeros((TILE, d_model), BF16)

    for fetch in fetches:
        fetch.wait()

    def after_ends():
        issue([(ship, 1, 1)] + [(ship, k, 2) for k in range(4)], [])
        for k in (1, 2, 3):
            ship(k, 0)

    mixer(
        n_sp, n_tp, after_ends, *inputs, x.at[me_s, 0], stream, *mixer_scratch
    )

    def along(b, n, to):
        return pltpu.make_async_remote_copy(
            src_ref=x.at[b, 0], dst_ref=x.at[b, 0], send_sem=az_s.at[n], recv_sem=az_r.at[b],
            device_id={"sp": to}, device_id_type=MESH,
        )

    def share(b):
        send(x.at[b, 0], x.at[b, 2], ax_s.at[0], ax_r.at[b], tp=across)
        send(x.at[b, 0], x.at[b, 1], am_s.at[0], am_r.at[0], tp=mate)

    def spread(b):
        pltpu.make_async_remote_copy(
            src_ref=x.at[b, 2], dst_ref=x.at[b, 2], send_sem=ax_s.at[0], recv_sem=ax_r.at[b],
            device_id={"tp": across}, device_id_type=MESH,
        ).wait_recv()
        send(x.at[b, 2], x.at[b, 3], am_s.at[0], am_r.at[0], tp=mate)

    def rows_to(to, piece, ss, rs):
        return pltpu.make_async_remote_copy(
            src_ref=piece, dst_ref=piece, send_sem=ss.at[0], recv_sem=rs.at[0],
            device_id={"tp": to}, device_id_type=MESH,
        )

    def meet(n):
        pl.semaphore_signal(met.at[n], inc=1, device_id={"tp": mate}, device_id_type=MESH)
        pl.semaphore_wait(met.at[n], 1)

    firsthand = [along(me_s, i, near[i]) for i in range(2)]
    for copy in firsthand:
        copy.start()
    share(me_s)

    def gathered(i):
        b = near[i]
        along(b, 0, near[0]).wait_recv()
        if i:
            @pl.when(inner)
            def _():
                along(b, 1 + i, near[0]).start()
        share(b)

    gates, ups, downs = (0, 1), (2, 3), (4, 5, 6, 7)

    def each(act, *groups):
        return [
            (act, k, i) for ks, i in groups for k in ks if act is ship or k != 1
        ]

    issue(each(relay, (gates, 1)), [])
    issue(each(relay, (gates, 0), (ups, 0)), each(relay, (gates, 0), (ups, 0), (gates, 1)))
    for copy in firsthand:
        copy.wait_send()
    meet(0)
    issue(
        each(ship, (ups, 1), (downs[:2], 2)),
        each(ship, (gates, 1), (ups, 1), (gates, 2), (downs, 0), (ups, 2)),
    )
    spread(order[0])
    gathered(0)
    issue([], each(relay, (ups, 1)))
    gathered(1)
    spread(order[1])
    gathered(2)
    issue(each(relay, (gates, 2)) + each(ship, (downs, 0)), [])
    spread(order[2])
    spread(order[3])
    issue(each(relay, (ups, 2)), each(relay, (gates, 2)))
    rows_to(mate, x.at[:, pl.ds(0, 2)], am_s, am_r).wait_recv()

    def product(b):
        lhs = x[:, :, :, aligned(b, depth)].reshape(rows, depth)
        return jnp.dot(lhs, wgu[aligned(b, depth), :], preferred_element_type=F32)

    def loaded(which):
        def act(width):
            loads = own_loads(width)
            for n in which:
                loads[n].wait()

        sized(me_s, act)

    def landed(i):
        arrived(0, i)

    loaded((0, 1))
    acc[...] = product(me_s)
    landed(0)
    acc[...] += product(near[0])
    issue(each(relay, (ups, 1)), each(relay, (ups, 2)))

    def release():
        gone(0, 1)
        issue([], [(gone, 0, 2)])
        meet(1)
        issue(
            [
                (lambda: pl.semaphore_signal(
                    met.at[2], inc=1, device_id={"sp": near[0]}, device_id_type=MESH
                ),)
            ],
            [(lambda: pl.semaphore_wait(met.at[2], 1),)],
        )
        issue([], each(ship, (downs[:2], 2)))
        for i in (2, 1):
            for k in (downs[2:] if i == 2 else downs):
                ship(k, i)

    pl.when(inner)(release)

    def add(i):
        landed(i)
        acc[...] += product(near[i])

    pl.when(inner)(lambda: add(2))
    pl.when(edge)(lambda: add(1))
    for k in downs:
        relay(k, 0)
    pl.when(edge)(release)
    last = jnp.where(inner, near[1], near[2])
    pl.when(inner)(lambda: landed(1))
    pl.when(edge)(lambda: landed(2))
    total = acc[...] + product(last)
    h[...] = (jax.nn.silu(total[:, :wide]) * total[:, wide:]).astype(BF16)

    blocks = [(i, q) for i in (0, 1, 3, 2) for q in range(2)]
    held = len(blocks) // 2
    steps = [(n, None) for n in range(6)] + [(n, g) for g in (me_g, 1 - me_g) for n in (6, 7)]

    def place_of(n):
        i, q = blocks[n]
        return 2 * order[i] + q

    def lanes_of(m):
        part = steps[m][1]
        return (half_col, pl.ds(0, half_col)) if part is None else (
            part_col, aligned(part, part_col)
        )

    def columns(m):
        n, part = steps[m]
        if part is None:
            return aligned(place_of(n), half_col)
        return aligned(2 * place_of(n) + part, part_col)

    firsts, turns = {}, {}

    def down(m):
        n, part = steps[m]
        i, q = blocks[n]
        if i and m not in (6, 7):
            arrived(downs[2 * q], i - 1)
        width = lanes_of(m)[0]
        y = jnp.dot(h[...], wd[:, columns(m)], preferred_element_type=F32)
        y = y.reshape(n_sp, n_tp, own, width)
        y1_out[m, 0, :, :, :width] = y[:, 1].astype(BF16)
        y1_out[m, 1, :, :, :width] = y[:, 3].astype(BF16)
        piece = (m, slice(None), slice(None), slice(None), pl.ds(0, width))
        firsts[m] = send(y1_out.at[piece], y1_in.at[piece], s1.at[0], r1.at[m], tp=mate)
        keep[m, 0, :, :, :width] = y[:, 0]
        keep[m, 1, :, :, :width] = y[:, 2]

    def stage_two(m):
        width = lanes_of(m)[0]
        firsts[m].wait_recv()
        y2_out[m, :, :, :width] = (
            keep[m, 1, :, :, :width] + y1_in[m, 1, :, :, :width].astype(F32)
        ).astype(BF16)
        piece = (m, slice(None), slice(None), pl.ds(0, width))
        turns[m] = send(y2_out.at[piece], y2_in.at[piece], s2.at[0], r2.at[m], tp=across)
        keep[m, 0, :, :, :width] += y1_in[m, 0, :, :, :width].astype(F32)

    def paired(n):
        c = place_of(n)
        piece = y3_in.at[c] if n < held else y3_in.at[c, 0]
        return pltpu.make_async_remote_copy(
            src_ref=piece, dst_ref=piece, send_sem=s3.at[0], recv_sem=r3.at[c],
            device_id={"sp": partner}, device_id_type=MESH,
        )

    def crossed(n):
        c = place_of(n)
        return pltpu.make_async_remote_copy(
            src_ref=y4_out.at[c], dst_ref=y4_in.at[c], send_sem=s4.at[0], recv_sem=r4.at[c % held],
            device_id={"sp": opposite}, device_id_type=MESH,
        )

    def stage_three(m):
        n, part = steps[m]
        c = place_of(n)
        width, lanes = lanes_of(m)
        turns[m].wait_recv()
        keep[m, 0, :, :, :width] += y2_in[m, :, :, :width].astype(F32)
        if n < held:
            for k, row in enumerate((partner, lax.rem(partner + 2, n_sp))):
                y3_out[c, k] = keep[m, 0, row].astype(BF16)
            send(y3_out.at[c], y3_in.at[c], s3.at[0], r3.at[c], sp=partner)
            return
        y3_out[c, 0, :, lanes] = keep[m, 0, partner, :, :width].astype(BF16)
        piece = (c, 0, slice(None), lanes)
        send(y3_out.at[piece], y3_in.at[piece], s3.at[0], r3.at[c], sp=partner)
        for j in range(2):
            far = 2 - 2 * side + j
            y5_out[n - held, j, :, lanes] = keep[m, 0, far, :, :width].astype(BF16)
            send(y5_out.at[n - held, j, :, lanes], y5_in.at[c % held, me_s % 2, :, lanes],
                 s5.at[0], r5.at[c % held], sp=far)

    def stage_four(n):
        c = place_of(n)
        paired(n).wait_recv()
        y4_out[c] = (keep[n, 0, opposite] + y3_in[c, 1].astype(F32)).astype(BF16)
        crossed(n).start()
        at = aligned(c, half_col)
        stream[:, at] += keep[n, 0, me_s] + y3_in[c, 0].astype(F32)

    def finish(n):
        c = place_of(n)
        if n < held:
            at = aligned(c, half_col)
            total = stream[:, at]
            piece = y5_in.at[c % held]
            pltpu.make_async_remote_copy(
                src_ref=piece, dst_ref=piece, send_sem=s5.at[0], recv_sem=r5.at[c % held],
                device_id={"sp": opposite}, device_id_type=MESH,
            ).wait_recv()
            for j in range(2):
                total += y5_in[c % held, j].astype(F32)
            out_ref[:, at] = total.astype(BF16)
            return
        paired(n).wait_recv()
        crossed(n).wait_recv()
        for m, (half, part) in enumerate(steps):
            if half == n:
                width, lanes = lanes_of(m)
                at = columns(m)
                out_ref[:, at] = (
                    stream[:, at] + keep[m, 0, me_s, :, :width]
                    + y3_in[c, 0, :, lanes].astype(F32) + y4_in[c, :, lanes].astype(F32)
                ).astype(BF16)

    loaded((2,))
    for m in range(6):
        if m in (1, 2):
            relay(downs[2 * m - 2], 2)
            relay(downs[2 * m - 1], 2)
        if m == 4:
            relay(downs[0], 1)
            relay(downs[1], 1)
        if m == 5:
            relay(downs[2], 1)
            relay(downs[3], 1)
        if m > held:
            stage_two(m - 1)
        down(m)
        if 1 <= m <= held:
            stage_two(m - 1)
        if m >= 3:
            stage_three(m - 3)
    down(6)
    down(7)
    for m in (5, 6, 7):
        stage_two(m)
    stage_three(3)
    issue([(stage_four, 0), (stage_four, 1)], [])
    down(8)
    stage_three(4)
    issue([(stage_four, 2), (stage_four, 3)], [])
    down(9)
    stage_two(8)
    stage_three(5)
    stage_three(6)
    stage_two(9)
    stage_three(7)
    issue([], [(stage_four, 0), (stage_four, 1)])
    stage_three(8)
    issue([], [(stage_four, 2), (stage_four, 3)])
    stage_three(9)
    rows_to(across, x.at[:, 0], ax_s, ax_r).wait_send()
    rows_to(mate, x.at[:, pl.ds(0, 2)], am_s, am_r).wait_send()
    rows_to(mate, y1_out.at[pl.ds(0, len(blocks))], s1, r1).wait_send()
    rows_to(across, y2_out.at[pl.ds(0, len(blocks))], s2, r2).wait_send()

    @pl.when(inner)
    def _():
        for n in (2, 3):
            along(me_s, n, near[0]).wait_send()

    gone(0, 0)
    issue([(gone, 0, 2)], [])
    for i in range(3):
        gone(4, i)
        for k in (0, 4):
            sized(me_s, lambda width: passed(k, i, whole(k, width)).wait_send())
    for n in (4, 5, 0, 1, 2, 3, 6, 7):
        finish(n)
    for to, piece, ss, rs in (
        (partner, y3_out.at[pl.ds(0, 6)], s3, r3),
        (opposite, y4_out.at[pl.ds(0, held)], s4, r4),
        (opposite, y5_out, s5, r5),
    ):
        pltpu.make_async_remote_copy(
            src_ref=piece, dst_ref=piece, send_sem=ss.at[0], recv_sem=rs.at[0],
            device_id={"sp": to}, device_id_type=MESH,
        ).wait_send()


def moved_weights(
    ssm_input, residual_in, log_step, decay_real, freq, in_real, in_imag, out_real, out_imag,
    skip, w_glu, b_glu, w_branch, norm_gain, w_gate, w_up, w_down,
):
    sizes = {axis: lax.axis_size(axis) for axis in ("grp", "sp", "tp")}
    n_sp, n_tp = sizes["sp"], sizes["tp"]
    tok, width = ssm_input.shape
    groups, states = decay_real.shape
    group = in_real.shape[2]
    lanes = groups * states
    own = tok // n_tp
    chan, d_model = w_branch.shape
    depth, hid = w_gate.shape
    cols = w_down.shape[1]
    wide = -(-hid // (TILE * n_sp)) * TILE
    rows = n_sp * tok
    operands = (
        ssm_input, residual_in, log_step[None], decay_real, freq,
        in_real.swapaxes(1, 2).reshape(width, states),
        in_imag.swapaxes(1, 2).reshape(width, states),
        out_real.reshape(width, states), out_imag.reshape(width, states),
        skip[None], w_glu, b_glu[None], w_branch, norm_gain[None], w_gate, w_up, w_down,
    )
    blocks, steps = 2 * n_sp, 2 * n_sp + 2
    vm = pl.BlockSpec(memory_space=pltpu.VMEM)
    hbm = pl.BlockSpec(memory_space=pl.ANY)
    dma = pltpu.SemaphoreType.DMA
    vmem = pltpu.VMEM
    return pl.pallas_call(
        functools.partial(layer_kernel, sizes),
        out_shape=pltpu.VMEM((own, d_model), BF16),
        in_specs=[hbm] * len(operands),
        out_specs=vm,
        scratch_shapes=[
            vmem((n_sp, n_tp, own, d_model), BF16),
            vmem((own, d_model), F32),
            vmem((d_model, 2 * wide), BF16),
            vmem((wide, d_model), BF16),
            vmem((rows, 2 * wide), F32),
            vmem((rows, wide), BF16),
            vmem((steps, 2, n_sp, own, cols // 2), F32),
            vmem((steps, 2, n_sp, own, cols // 2), BF16),
            vmem((steps, 2, n_sp, own, cols // 2), BF16),
            vmem((steps, n_sp, own, cols // 2), BF16),
            vmem((steps, n_sp, own, cols // 2), BF16),
            vmem((blocks, 2, own, cols // 2), BF16),
            vmem((blocks, 2, own, cols // 2), BF16),
            vmem((blocks, own, cols // 2), BF16),
            vmem((blocks, own, cols // 2), BF16),
            vmem((blocks // 2, 2, own, cols // 2), BF16),
            vmem((blocks // 2, 2, own, cols // 2), BF16),
            dma((3,)),
            dma((2, 3)), dma((7, 3)), dma((2, 3)), dma((3, 3)),
            dma((4,)), dma((n_sp,)),
            dma((1,)), dma((n_sp,)),
            dma((1,)), dma((1,)),
            dma((1,)), dma((steps,)), dma((1,)), dma((steps,)),
            dma((1,)), dma((blocks,)), dma((1,)), dma((blocks // 2,)),
            dma((1,)), dma((blocks // 2,)),
            pltpu.SemaphoreType.REGULAR((3,)),
            dma((len(SMALL),)),
            *[vmem(operands[at].shape, operands[at].dtype) for at in SMALL],
            vmem((chan, chan), BF16),
            vmem((chan, d_model), BF16),
            vmem((own, d_model), BF16),
            vmem((8, lanes), F32),
            vmem((tok, lanes), F32),
            vmem((tok, lanes), F32),
            vmem((tok, lanes), F32),
            vmem((tok, lanes), F32),
            vmem((2, lanes), F32),
            vmem((n_sp - 1, 2, lanes), F32),
            vmem((n_tp, own, width), BF16),
            vmem((n_tp - 1, own, width), BF16),
            vmem((own, chan), F32),
            dma((3,)),
            dma((n_sp - 1,)), dma((n_sp - 1,)),
            dma((n_tp - 1,)), dma((n_tp - 1,)),
        ],
        compiler_params=pltpu.CompilerParams(collective_id=0, has_side_effects=True),
        name="layer",
    )(*operands)


def per_device(*arguments):
    sizes = tuple(lax.axis_size(axis) for axis in ("grp", "sp", "tp"))
    tiles = arguments[14].shape[1] // TILE
    fits = sizes == (2, 4, 4) and tiles % 4 == 3
    return (moved_weights if fits else gathered_weights)(*arguments)


def solution(mesh):
    placed = (
        P(("grp", "sp"), "tp"),
        P(("grp", "sp"), None),
        P("tp"),
        P("tp", None),
        P("tp", None),
        P("tp", None, None),
        P("tp", None, None),
        P("tp", None, None),
        P("tp", None, None),
        P("tp"),
        P(),
        P(),
        P(),
        P(),
        P("sp", "tp"),
        P("sp", "tp"),
        P("tp", "sp"),
    )
    return jax.shard_map(
        per_device,
        mesh=mesh,
        in_specs=placed,
        out_specs=P(("grp", "sp", "tp"), None),
        check_vma=False,
    )
```

```python
import functools
import math

import jax
import jax.numpy as jnp
from jax import lax
from jax.experimental import pallas as pl
from jax.experimental.pallas import tpu as pltpu
from jax.sharding import PartitionSpec as P

EPS = 1e-06


def prefix(shard, axis, combine, identity):
    count, place = (lax.axis_size(axis), lax.axis_index(axis))
    everything = jax.tree.map(lambda part: lax.all_gather(part, axis), shard)
    start = jax.tree.map(
        lambda part, zero: jnp.broadcast_to(jnp.asarray(zero, part.dtype), part.shape),
        shard,
        identity,
    )

    def lap(k, before):
        reached = k < place
        new = combine(before, jax.tree.map(lambda part: part[k], everything))
        return jax.tree.map(lambda a, b: jnp.where(reached, a, b), new, before)

    return lax.fori_loop(0, count, lap, start)


def discretize(log_step, decay_real, freq, in_real, in_imag):
    step_size = jnp.exp(log_step)[:, None]
    magnitude = jnp.exp(decay_real * step_size)
    abar_re = magnitude * jnp.cos(freq * step_size)
    abar_im = magnitude * jnp.sin(freq * step_size)
    denominator = decay_real * decay_real + freq * freq
    less_re = abar_re - 1.0
    hold_re = ((less_re * decay_real + abar_im * freq) / denominator)[..., None]
    hold_im = ((abar_im * decay_real - less_re * freq) / denominator)[..., None]
    bbar_re = hold_re * in_real - hold_im * in_imag
    bbar_im = hold_re * in_imag + hold_im * in_real
    return (step_size, abar_re, abar_im, bbar_re, bbar_im)


def powers(decay_real, freq, step_size, length):
    steps_up = (jnp.arange(length, dtype=jnp.int32) + 1).astype(jnp.float32)[:, None, None]
    magnitude = jnp.exp((decay_real * step_size)[None] * steps_up)
    phase = (freq * step_size)[None] * steps_up
    return (magnitude * jnp.cos(phase), magnitude * jnp.sin(phase))


def compose(earlier, later):
    a1r, a1i, b1r, b1i = earlier
    a2r, a2i, b2r, b2i = later
    return (
        a2r * a1r - a2i * a1i,
        a2r * a1i + a2i * a1r,
        a2r * b1r - a2i * b1i + b2r,
        a2r * b1i + a2i * b1r + b2i,
    )


def local_states(inputs, decay_real, freq, step_size, bbar_re, bbar_im):
    highest = lax.Precision.HIGHEST
    tok_rows, group_count, unused = inputs.shape
    lanes = group_count * decay_real.shape[1]
    drive_re = jnp.einsum("lgm,gpm->lgp", inputs, bbar_re, precision=highest).reshape(
        tok_rows, lanes
    )
    drive_im = jnp.einsum("lgm,gpm->lgp", inputs, bbar_im, precision=highest).reshape(
        tok_rows, lanes
    )
    span = math.gcd(tok_rows, 16)
    spans = tok_rows // span
    rate = (decay_real * step_size).reshape(lanes)
    turn = (freq * step_size).reshape(lanes)
    later = jnp.arange(span, dtype=jnp.int32)[:, None]
    earlier = jnp.arange(span, dtype=jnp.int32)[None, :]
    lag = (later - earlier).astype(jnp.float32)
    causal = (later >= earlier)[..., None]
    lag_pos = jnp.maximum(lag, 0.0)[..., None]
    table_mag = jnp.exp(rate[None, None] * lag_pos)
    table_re = jnp.where(causal, table_mag * jnp.cos(turn[None, None] * lag_pos), 0.0)
    table_im = jnp.where(causal, table_mag * jnp.sin(turn[None, None] * lag_pos), 0.0)
    block_re = drive_re.reshape(spans, 1, span, lanes)
    block_im = drive_im.reshape(spans, 1, span, lanes)
    inner_re = jnp.sum(table_re[None] * block_re - table_im[None] * block_im, axis=2)
    inner_im = jnp.sum(table_re[None] * block_im + table_im[None] * block_re, axis=2)
    steps_up = (jnp.arange(span, dtype=jnp.int32) + 1).astype(jnp.float32)[:, None]
    pow_mag = jnp.exp(rate[None] * steps_up)
    pow_re = pow_mag * jnp.cos(turn[None] * steps_up)
    pow_im = pow_mag * jnp.sin(turn[None] * steps_up)
    span_re = pow_re[-1]
    span_im = pow_im[-1]

    def carry_step(entering, ends):
        next_re = span_re * entering[0] - span_im * entering[1] + ends[0]
        next_im = span_re * entering[1] + span_im * entering[0] + ends[1]
        return ((next_re, next_im), entering)

    zeros = jnp.zeros((lanes,), jnp.float32)
    unused_carry, entering = lax.scan(
        carry_step, (zeros, zeros), (inner_re[:, -1], inner_im[:, -1])
    )
    state_re = inner_re + pow_re[None] * entering[0][:, None] - pow_im[None] * entering[1][:, None]
    state_im = inner_im + pow_re[None] * entering[1][:, None] + pow_im[None] * entering[0][:, None]
    shape = (tok_rows, group_count, decay_real.shape[1])
    return (state_re.reshape(shape), state_im.reshape(shape))


def readout(state_re, state_im, out_real, out_imag, skip_mat, inputs):
    highest = lax.Precision.HIGHEST
    values = (
        jnp.einsum("lgp,gmp->lgm", state_re, out_real, precision=highest)
        - jnp.einsum("lgp,gmp->lgm", state_im, out_imag, precision=highest)
        + skip_mat[None] * inputs
    )
    values = jax.nn.gelu(values)
    return values.reshape(values.shape[0], -1).astype(jnp.bfloat16)


def row_norm(stream, norm_gain):
    scale_rows = lax.rsqrt(jnp.mean(stream * stream, axis=-1, keepdims=True) + EPS)
    return (stream * scale_rows * norm_gain).astype(jnp.bfloat16)


def gathered_weights(
    ssm_input,
    residual_in,
    log_step,
    decay_real,
    freq,
    in_real,
    in_imag,
    out_real,
    out_imag,
    skip,
    w_glu,
    b_glu,
    w_branch,
    norm_gain,
    w_gate,
    w_up,
    w_down,
):
    tok_rows, width_local = ssm_input.shape
    group_count = log_step.shape[0]
    group_size = in_real.shape[2]
    tp_count = lax.axis_size("tp")
    tp_index = lax.axis_index("tp")
    own_rows = tok_rows // tp_count
    step_size, abar_re, abar_im, bbar_re, bbar_im = discretize(
        log_step, decay_real, freq, in_real, in_imag
    )
    pow_re, pow_im = powers(decay_real, freq, step_size, tok_rows)
    inputs = ssm_input.astype(jnp.float32).reshape(tok_rows, group_count, group_size)
    local_re, local_im = local_states(inputs, decay_real, freq, step_size, bbar_re, bbar_im)
    identity = (
        jnp.ones_like(abar_re),
        jnp.zeros_like(abar_re),
        jnp.zeros_like(abar_re),
        jnp.zeros_like(abar_re),
    )
    carried = prefix((pow_re[-1], pow_im[-1], local_re[-1], local_im[-1]), "sp", compose, identity)
    state_re = local_re + pow_re * carried[2][None] - pow_im * carried[3][None]
    state_im = local_im + pow_re * carried[3][None] + pow_im * carried[2][None]
    mixer_out = readout(
        state_re, state_im, out_real, out_imag, skip.reshape(group_count, group_size), inputs
    )
    mixer_rows = lax.all_to_all(mixer_out, "tp", split_axis=0, concat_axis=1, tiled=True)
    glu_pre = jnp.dot(mixer_rows, w_glu, preferred_element_type=jnp.float32) + b_glu
    gated = (mixer_rows.astype(jnp.float32) * jax.nn.sigmoid(glu_pre)).astype(jnp.bfloat16)
    residual_own = lax.dynamic_slice_in_dim(residual_in, tp_index * own_rows, own_rows, 0)
    stream = residual_own.astype(jnp.float32) + jnp.dot(
        gated, w_branch, preferred_element_type=jnp.float32
    )
    normed = row_norm(stream, norm_gain)
    normed_all = lax.all_gather(normed, "tp", axis=0, tiled=True)
    gate_sum = jnp.dot(
        normed_all,
        lax.all_gather(w_gate, "sp", axis=0, tiled=True),
        preferred_element_type=jnp.float32,
    )
    up_sum = jnp.dot(
        normed_all,
        lax.all_gather(w_up, "sp", axis=0, tiled=True),
        preferred_element_type=jnp.float32,
    )
    hidden = (jax.nn.silu(gate_sum) * up_sum).astype(jnp.bfloat16)
    down_whole = lax.all_gather(w_down, "sp", axis=1, tiled=True)
    summed = lax.psum_scatter(
        jnp.dot(hidden, down_whole, preferred_element_type=jnp.float32).astype(jnp.bfloat16),
        "tp",
        scatter_dimension=0,
        tiled=True,
    ).astype(jnp.float32)
    return (stream + summed).astype(jnp.bfloat16)


MESH = pl.DeviceIdType.MESH
F32 = jnp.float32
BF16 = jnp.bfloat16
NT = (((1,), (1,)), ((), ()))


def greet(sizes, place):
    barrier = pltpu.get_barrier_semaphore()
    for axis in sizes:
        for d in range(1, sizes[axis]):
            pl.semaphore_signal(
                barrier, inc=1, device_id={axis: lax.rem(place[axis] + d, sizes[axis])},
                device_id_type=MESH,
            )
    pl.semaphore_wait(barrier, sum(sizes.values()) - len(sizes))


def send(src, dst, ss, rs, **to):
    copy = pltpu.make_async_remote_copy(
        src_ref=src, dst_ref=dst, send_sem=ss, recv_sem=rs, device_id=to, device_id_type=MESH
    )
    copy.start()
    return copy


def aligned(index, size):
    return pl.ds(pl.multiple_of(index * size, size), size)


def mixer(
    n_sp, n_tp, after_ends,
    u_ref, res_ref, ls_ref, dec_ref, frq_ref, inr_ref, ini_ref, outr_ref, outi_ref,
    skip_ref, wglu_ref, bglu_ref, wbr_ref, gain_ref,
    normed_ref, stream_ref,
    wglu, wbr, res, coef, xr, xi, pr_all, pi_all, fin, fin_in, mo, rows_in, glu,
    load_sem, fs, fr, rs, rr,
):
    me_s, me_t = lax.axis_index("sp"), lax.axis_index("tp")
    tok, width = u_ref.shape
    groups, states = dec_ref.shape
    group = width // groups
    lanes = groups * states
    own = tok // n_tp
    loads = [
        pltpu.make_async_copy(
            res_ref.at[pl.ds(pl.multiple_of(me_t * own, own), own)], res, load_sem.at[0]
        ),
        pltpu.make_async_copy(wglu_ref, wglu, load_sem.at[1]),
        pltpu.make_async_copy(wbr_ref, wbr, load_sem.at[2]),
    ]
    for load in loads:
        load.start()

    same = lax.broadcasted_iota(jnp.int32, (groups, groups), 0) == lax.broadcasted_iota(
        jnp.int32, (groups, groups), 1
    )
    step = jnp.exp(jnp.sum(jnp.where(same, ls_ref[...], 0.0), axis=1, keepdims=True))
    dec, frq = dec_ref[...], frq_ref[...]
    mag = jnp.exp(dec * step)
    ar = mag * jnp.cos(frq * step)
    ai = mag * jnp.sin(frq * step)
    den = dec * dec + frq * frq
    less = ar - 1.0
    hr = (less * dec + ai * frq) / den
    hi = (ai * dec - less * frq) / den
    for g in range(groups):
        at = slice(g * states, (g + 1) * states)
        coef[0:1, at] = ar[g : g + 1, :]
        coef[1:2, at] = ai[g : g + 1, :]
        coef[2:3, at] = hr[g : g + 1, :]
        coef[3:4, at] = hi[g : g + 1, :]

    u = u_ref[...]
    part = 128
    spread = (
        lax.broadcasted_iota(jnp.int32, (states, part), 1) % states
        == lax.broadcasted_iota(jnp.int32, (states, part), 0)
    ).astype(BF16)
    rows_group = lax.broadcasted_iota(jnp.int32, (width, part), 0) // group
    lane_group = lax.broadcasted_iota(jnp.int32, (width, part), 1) // states

    def spread_out(ref):
        return jnp.dot(ref[...].astype(BF16), spread, preferred_element_type=F32)

    def only(wide, c):
        return jnp.where(rows_group == lane_group + c * (part // states), wide, 0.0).astype(BF16)

    in_r, in_i = spread_out(inr_ref), spread_out(ini_ref)
    row = lax.broadcasted_iota(jnp.int32, (tok, part), 0)
    row8 = lax.broadcasted_iota(jnp.int32, (8, part), 0)
    for c in range(lanes // part):
        at = slice(c * part, (c + 1) * part)
        vr = jnp.dot(u, only(in_r, c), preferred_element_type=F32)
        vi = jnp.dot(u, only(in_i, c), preferred_element_type=F32)
        cr, ci = coef[2:3, at], coef[3:4, at]
        sr, si = cr * vr - ci * vi, cr * vi + ci * vr
        pr, pi = coef[0:1, at], coef[1:2, at]
        tr, ti = jnp.ones((8, part), F32), jnp.zeros((8, part), F32)
        s = 1
        while s <= tok:
            if s <= 8:
                bit = ((row8 + 1) & s) != 0
                br, bi = jnp.where(bit, pr, 1.0), jnp.where(bit, pi, 0.0)
                tr, ti = tr * br - ti * bi, tr * bi + ti * br
            if s >= 8 and s < tok:
                tr, ti = (
                    jnp.concatenate([tr, tr * pr - ti * pi], 0),
                    jnp.concatenate([ti, tr * pi + ti * pr], 0),
                )
            if s < tok:
                if s < 8:
                    yr = jnp.where(row >= s, pltpu.roll(sr, s, 0), 0.0)
                    yi = jnp.where(row >= s, pltpu.roll(si, s, 0), 0.0)
                else:
                    gap = jnp.zeros((s, part), F32)
                    yr = jnp.concatenate([gap, sr[: tok - s]], 0)
                    yi = jnp.concatenate([gap, si[: tok - s]], 0)
                sr, si = sr + (pr * yr - pi * yi), si + (pr * yi + pi * yr)
            pr, pi = pr * pr - pi * pi, 2.0 * pr * pi
            s *= 2
        xr[:, at], xi[:, at] = sr, si
        pr_all[:, at], pi_all[:, at] = tr, ti
        fin[0:1, at] = sr[tok - 1 : tok]
        fin[1:2, at] = si[tok - 1 : tok]

    def end_to(d):
        return pltpu.make_async_remote_copy(
            src_ref=fin, dst_ref=fin_in.at[d - 1], send_sem=fs.at[d - 1], recv_sem=fr.at[d - 1],
            device_id={"sp": lax.rem(me_s + d, n_sp)}, device_id_type=MESH,
        )

    for d in range(1, n_sp):
        @pl.when(me_s + d < n_sp)
        def _():
            end_to(d).start()
    after_ends()

    out_r, out_i = spread_out(outr_ref), spread_out(outi_ref)
    outr = jnp.concatenate([only(out_r, c) for c in range(lanes // part)], axis=1)
    outi = jnp.concatenate([only(out_i, c) for c in range(lanes // part)], axis=1)
    for d in range(1, n_sp):
        @pl.when(me_s >= d)
        def _():
            end_to(d).wait_recv()
    er, ei = pr_all[tok - 1 : tok, :], pi_all[tok - 1 : tok, :]
    pr, pi = jnp.ones((1, lanes), F32), jnp.zeros((1, lanes), F32)
    cr, ci = jnp.zeros((1, lanes), F32), jnp.zeros((1, lanes), F32)
    for d in range(1, n_sp):
        fr_, fi_ = fin_in[d - 1, 0:1, :], fin_in[d - 1, 1:2, :]
        reached = me_s >= d
        cr = cr + jnp.where(reached, pr * fr_ - pi * fi_, 0.0)
        ci = ci + jnp.where(reached, pr * fi_ + pi * fr_, 0.0)
        pr, pi = pr * er - pi * ei, pr * ei + pi * er
    tr, ti = pr_all[...], pi_all[...]
    sr = (xr[...] + (tr * cr - ti * ci)).astype(BF16)
    si = (xi[...] + (tr * ci + ti * cr)).astype(BF16)
    y = lax.dot_general(sr, outr, NT, preferred_element_type=F32) - lax.dot_general(
        si, outi, NT, preferred_element_type=F32
    )
    for d in range(1, n_sp):
        @pl.when(me_s + d < n_sp)
        def _():
            end_to(d).wait_send()
    y = jax.nn.gelu(y + skip_ref[...] * u.astype(F32))
    mo[...] = y.astype(BF16).reshape(n_tp, own, width)
    turns = []
    for d in range(1, n_tp):
        to = lax.rem(me_t + d, n_tp)
        copy = pltpu.make_async_remote_copy(
            src_ref=mo.at[to], dst_ref=rows_in.at[d - 1], send_sem=rs.at[d - 1],
            recv_sem=rr.at[d - 1], device_id={"tp": to}, device_id_type=MESH,
        )
        copy.start()
        turns.append(copy)
    for load in loads:
        load.wait()

    def source(d):
        return pl.ds(pl.multiple_of(lax.rem(me_t + n_tp - d, n_tp) * width, width), width)

    blocks = [mo[me_t]]
    pre = bglu_ref[...] + jnp.dot(blocks[0], wglu[source(0), :], preferred_element_type=F32)
    for d in range(1, n_tp):
        turns[d - 1].wait()
        blocks.append(rows_in[d - 1])
        pre = pre + jnp.dot(blocks[d], wglu[source(d), :], preferred_element_type=F32)
    glu[...] = pre
    stream = res[...].astype(F32)
    for d in range(n_tp):
        gate = jax.nn.sigmoid(glu[:, source(d)])
        gated = (blocks[d].astype(F32) * gate).astype(BF16)
        stream = stream + jnp.dot(gated, wbr[source(d), :], preferred_element_type=F32)
    stream_ref[...] = stream
    scale = lax.rsqrt(jnp.mean(stream * stream, axis=-1, keepdims=True) + EPS)
    normed_ref[...] = (stream * scale * gain_ref[...]).astype(BF16)


TILE = 128
SMALL = (0, 2, 3, 4, 5, 6, 7, 8, 9, 11, 13)


def layer_kernel(sizes, *refs):
    n_sp, n_tp = sizes["sp"], sizes["tp"]
    place = {axis: lax.axis_index(axis) for axis in sizes}
    me_g, me_s, me_t = place["grp"], place["sp"], place["tp"]
    wg_ref, wu_ref, wd_ref, out_ref = refs[14:18]
    x, stream, wgu, wd, acc, h = refs[18:24]
    keep, y1_out, y1_in, y2_out, y2_in, y3_out, y3_in, y4_out, y4_in, y5_out, y5_in = refs[24:35]
    (load_sem, ws, wr, fs, fr, az_s, az_r, ax_s, ax_r, am_s, am_r,
     s1, r1, s2, r2, s3, r3, s4, r4, s5, r5, met, small_sem) = refs[35:58]
    small = refs[58 : 58 + len(SMALL)]
    mixer_scratch = refs[58 + len(SMALL) :]
    inputs = list(refs[:14])
    fetches = []
    for n, at in enumerate(SMALL):
        fetches.append(pltpu.make_async_copy(inputs[at], small[n], small_sem.at[n]))
        inputs[at] = small[n]
    for fetch in fetches:
        fetch.start()
    own, d_model = stream.shape
    depth, hid = wg_ref.shape
    cols = wd_ref.shape[1]
    wide = wgu.shape[1] // 2
    rows = n_sp * n_tp * own
    parity = me_t % 2
    short = (n_sp - 1) * (1 - parity)
    part_row, part_col = depth // 4, cols // 4
    half_col = 2 * part_col

    side = me_s // 2
    inner = me_s % 2 != side
    partner = me_s + 1 - 2 * (me_s % 2)
    opposite = lax.rem(me_s + 2, n_sp)
    near = [partner, 2 - side, 3 * (1 - side)]
    order = [me_s] + near
    far_slot = 2 - (me_s % 2 + side) % 2
    slots = [0, far_slot, far_slot]
    mate = me_t + 1 - 2 * (me_t % 2)
    across = lax.rem(me_t + 2, n_tp)

    def sized(to, act):
        @pl.when(to == short)
        def _():
            act(wide - TILE)

        @pl.when(to != short)
        def _():
            act(wide)

    def first(to):
        return (3 * to - parity * ((to + 3) // 4)) * TILE

    def shipped(k, i, width):
        start = pl.ds(pl.multiple_of(first(near[i]), TILE), width)
        if k < 4:
            at = 2 * me_g + k % 2
            src = (wg_ref, wu_ref)[k // 2].at[aligned(at, part_row), start]
            dst = wgu.at[aligned(4 * me_s + at, part_row), pl.ds(k // 2 * wide, width)]
        else:
            at = 2 * ((k - 4) // 2) + me_g
            skipped, count = k % 2 * (width // 2), width // 2
            start = pl.ds(pl.multiple_of(first(near[i]) + skipped, TILE // 2), count)
            src = wd_ref.at[start, aligned(at, part_col)]
            dst = wd.at[pl.ds(skipped, count), aligned(4 * me_s + at, part_col)]
        return pltpu.make_async_remote_copy(
            src_ref=src, dst_ref=dst, send_sem=ws.at[k // 4, i],
            recv_sem=wr.at[max(k - 1, 0), slots[i]],
            device_id={"sp": near[i]}, device_id_type=MESH,
        )

    def ship(k, i):
        sized(near[i], lambda width: shipped(k, i, width).start())

    def handed(k, i, width):
        at = 4 * near[i] + 2 * me_g + k % 2
        if k == 0:
            return wgu.at[aligned(2 * near[i] + me_g, 2 * part_row), pl.ds(0, width)]
        if k < 4:
            return wgu.at[aligned(at, part_row), pl.ds(k // 2 * wide, width)]
        at = 4 * near[i] + 2 * ((k - 4) // 2) + me_g
        return wd.at[pl.ds(k % 2 * (width // 2), width // 2), aligned(at, part_col)]

    def whole(k, width, half=False):
        if k < 4:
            return wgu.at[pl.ds(0, 4 * part_row), pl.ds(0, width)]
        return wd.at[pl.ds(0, width), pl.ds(0, part_col if half else half_col)]

    def passed(k, i, piece):
        return pltpu.make_async_remote_copy(
            src_ref=piece, dst_ref=piece, send_sem=fs.at[k // 4, i],
            recv_sem=fr.at[k // 4 * (k // 2 - 1), i],
            device_id={"grp": 1 - me_g}, device_id_type=MESH,
        )

    def relay(k, i):
        def act(width):
            piece = handed(k, i, width)
            pltpu.make_async_remote_copy(
                src_ref=piece, dst_ref=piece, send_sem=ws.at[k // 4, i],
                recv_sem=wr.at[max(k - 1, 0), i],
                device_id={"sp": near[i]}, device_id_type=MESH,
            ).wait_recv()
            passed(k, i, piece).start()

        sized(me_s, act)

    def arrived(k, i):
        sized(me_s, lambda width: passed(k, i, whole(k, width, True)).wait_recv())

    def gone(k, i):
        def act(width):
            piece = whole(k, width)
            pltpu.make_async_remote_copy(
                src_ref=piece, dst_ref=piece, send_sem=ws.at[k // 4, i], recv_sem=wr.at[0, i],
                device_id={"sp": near[i]}, device_id_type=MESH,
            ).wait_send()

        sized(near[i], act)

    def own_loads(width):
        start = pl.ds(pl.multiple_of(first(me_s), TILE), width)
        return [
            pltpu.make_async_copy(
                ref.at[:, start], wgu.at[aligned(me_s, depth), pl.ds(k * wide, width)],
                load_sem.at[k],
            )
            for k, ref in enumerate((wg_ref, wu_ref))
        ] + [
            pltpu.make_async_copy(
                wd_ref.at[start, :], wd.at[pl.ds(0, width), aligned(me_s, cols)], load_sem.at[2]
            )
        ]

    def start_loads(width):
        for load in own_loads(width):
            load.start()

    edge = jnp.logical_not(inner)

    def issue(at_inner, at_edge):
        for where, jobs in ((inner, at_inner), (edge, at_edge)):
            @pl.when(where)
            def _():
                for act, *where_to in jobs:
                    act(*where_to)

    ends_in = mixer_scratch[9]
    ends_in[...] = jnp.zeros_like(ends_in)
    greet(sizes, place)
    issue([(ship, 0, 1), (ship, 0, 0)], [(ship, 0, 0)])
    sized(me_s, start_loads)

    @pl.when(me_s == short)
    def _():
        for k in range(2):
            wgu[:, (k + 1) * wide - TILE : (k + 1) * wide] = jnp.zeros((n_sp * depth, TILE), BF16)
        wd[wide - TILE :, :] = jnp.zeros((TILE, d_model), BF16)

    for fetch in fetches:
        fetch.wait()

    def after_ends():
        issue([(ship, 1, 1)] + [(ship, k, 2) for k in range(4)], [])
        for k in (1, 2, 3):
            ship(k, 0)

    mixer(
        n_sp, n_tp, after_ends, *inputs, x.at[me_s, 0], stream, *mixer_scratch
    )

    def along(b, n, to):
        return pltpu.make_async_remote_copy(
            src_ref=x.at[b, 0], dst_ref=x.at[b, 0], send_sem=az_s.at[n], recv_sem=az_r.at[b],
            device_id={"sp": to}, device_id_type=MESH,
        )

    def share(b):
        send(x.at[b, 0], x.at[b, 2], ax_s.at[0], ax_r.at[b], tp=across)
        send(x.at[b, 0], x.at[b, 1], am_s.at[0], am_r.at[0], tp=mate)

    def spread(b):
        pltpu.make_async_remote_copy(
            src_ref=x.at[b, 2], dst_ref=x.at[b, 2], send_sem=ax_s.at[0], recv_sem=ax_r.at[b],
            device_id={"tp": across}, device_id_type=MESH,
        ).wait_recv()
        send(x.at[b, 2], x.at[b, 3], am_s.at[0], am_r.at[0], tp=mate)

    def rows_to(to, piece, ss, rs):
        return pltpu.make_async_remote_copy(
            src_ref=piece, dst_ref=piece, send_sem=ss.at[0], recv_sem=rs.at[0],
            device_id={"tp": to}, device_id_type=MESH,
        )

    def meet(n):
        pl.semaphore_signal(met.at[n], inc=1, device_id={"tp": mate}, device_id_type=MESH)
        pl.semaphore_wait(met.at[n], 1)

    firsthand = [along(me_s, i, near[i]) for i in range(2)]
    for copy in firsthand:
        copy.start()
    share(me_s)

    def gathered(i):
        b = near[i]
        along(b, 0, near[0]).wait_recv()
        if i:
            @pl.when(inner)
            def _():
                along(b, 1 + i, near[0]).start()
        share(b)

    gates, ups, downs = (0, 1), (2, 3), (4, 5, 6, 7)

    def each(act, *groups):
        return [
            (act, k, i) for ks, i in groups for k in ks if act is ship or k != 1
        ]

    issue(each(relay, (gates, 1)), [])
    issue(each(relay, (gates, 0), (ups, 0)), each(relay, (gates, 0), (ups, 0), (gates, 1)))
    for copy in firsthand:
        copy.wait_send()
    meet(0)
    issue(
        each(ship, (ups, 1), (downs[:2], 2)),
        each(ship, (gates, 1), (ups, 1), (gates, 2), (downs, 0), (ups, 2)),
    )
    spread(order[0])
    gathered(0)
    issue([], each(relay, (ups, 1)))
    gathered(1)
    spread(order[1])
    gathered(2)
    issue(each(relay, (gates, 2)) + each(ship, (downs, 0)), [])
    spread(order[2])
    spread(order[3])
    issue(each(relay, (ups, 2)), each(relay, (gates, 2)))
    rows_to(mate, x.at[:, pl.ds(0, 2)], am_s, am_r).wait_recv()

    def product(b):
        lhs = x[:, :, :, aligned(b, depth)].reshape(rows, depth)
        return jnp.dot(lhs, wgu[aligned(b, depth), :], preferred_element_type=F32)

    def loaded(which):
        def act(width):
            loads = own_loads(width)
            for n in which:
                loads[n].wait()

        sized(me_s, act)

    def landed(i):
        arrived(0, i)

    loaded((0, 1))
    acc[...] = product(me_s)
    landed(0)
    acc[...] += product(near[0])
    issue(each(relay, (ups, 1)), each(relay, (ups, 2)))

    def release():
        gone(0, 1)
        issue([], [(gone, 0, 2)])
        meet(1)
        issue(
            [
                (lambda: pl.semaphore_signal(
                    met.at[2], inc=1, device_id={"sp": near[0]}, device_id_type=MESH
                ),)
            ],
            [(lambda: pl.semaphore_wait(met.at[2], 1),)],
        )
        issue([], each(ship, (downs[:2], 2)))
        for i in (2, 1):
            for k in (downs[2:] if i == 2 else downs):
                ship(k, i)

    pl.when(inner)(release)

    def add(i):
        landed(i)
        acc[...] += product(near[i])

    pl.when(inner)(lambda: add(2))
    pl.when(edge)(lambda: add(1))
    for k in downs:
        relay(k, 0)
    pl.when(edge)(release)
    last = jnp.where(inner, near[1], near[2])
    pl.when(inner)(lambda: landed(1))
    pl.when(edge)(lambda: landed(2))
    total = acc[...] + product(last)
    h[...] = (jax.nn.silu(total[:, :wide]) * total[:, wide:]).astype(BF16)

    blocks = [(i, q) for i in (0, 1, 3, 2) for q in range(2)]
    held = len(blocks) // 2
    steps = [(n, None) for n in range(6)] + [(n, g) for g in (me_g, 1 - me_g) for n in (6, 7)]

    def place_of(n):
        i, q = blocks[n]
        return 2 * order[i] + q

    def lanes_of(m):
        part = steps[m][1]
        return (half_col, pl.ds(0, half_col)) if part is None else (
            part_col, aligned(part, part_col)
        )

    def columns(m):
        n, part = steps[m]
        if part is None:
            return aligned(place_of(n), half_col)
        return aligned(2 * place_of(n) + part, part_col)

    firsts, turns = {}, {}

    def down(m):
        n, part = steps[m]
        i, q = blocks[n]
        if i and m not in (6, 7):
            arrived(downs[2 * q], i - 1)
        width = lanes_of(m)[0]
        y = jnp.dot(h[...], wd[:, columns(m)], preferred_element_type=F32)
        y = y.reshape(n_sp, n_tp, own, width)
        y1_out[m, 0, :, :, :width] = y[:, 1].astype(BF16)
        y1_out[m, 1, :, :, :width] = y[:, 3].astype(BF16)
        piece = (m, slice(None), slice(None), slice(None), pl.ds(0, width))
        firsts[m] = send(y1_out.at[piece], y1_in.at[piece], s1.at[0], r1.at[m], tp=mate)
        keep[m, 0, :, :, :width] = y[:, 0]
        keep[m, 1, :, :, :width] = y[:, 2]

    def stage_two(m):
        width = lanes_of(m)[0]
        firsts[m].wait_recv()
        y2_out[m, :, :, :width] = (
            keep[m, 1, :, :, :width] + y1_in[m, 1, :, :, :width].astype(F32)
        ).astype(BF16)
        piece = (m, slice(None), slice(None), pl.ds(0, width))
        turns[m] = send(y2_out.at[piece], y2_in.at[piece], s2.at[0], r2.at[m], tp=across)
        keep[m, 0, :, :, :width] += y1_in[m, 0, :, :, :width].astype(F32)

    def paired(n):
        c = place_of(n)
        piece = y3_in.at[c] if n < held else y3_in.at[c, 0]
        return pltpu.make_async_remote_copy(
            src_ref=piece, dst_ref=piece, send_sem=s3.at[0], recv_sem=r3.at[c],
            device_id={"sp": partner}, device_id_type=MESH,
        )

    def crossed(n):
        c = place_of(n)
        return pltpu.make_async_remote_copy(
            src_ref=y4_out.at[c], dst_ref=y4_in.at[c], send_sem=s4.at[0], recv_sem=r4.at[c % held],
            device_id={"sp": opposite}, device_id_type=MESH,
        )

    def stage_three(m):
        n, part = steps[m]
        c = place_of(n)
        width, lanes = lanes_of(m)
        turns[m].wait_recv()
        keep[m, 0, :, :, :width] += y2_in[m, :, :, :width].astype(F32)
        if n < held:
            for k, row in enumerate((partner, lax.rem(partner + 2, n_sp))):
                y3_out[c, k] = keep[m, 0, row].astype(BF16)
            send(y3_out.at[c], y3_in.at[c], s3.at[0], r3.at[c], sp=partner)
            return
        y3_out[c, 0, :, lanes] = keep[m, 0, partner, :, :width].astype(BF16)
        piece = (c, 0, slice(None), lanes)
        send(y3_out.at[piece], y3_in.at[piece], s3.at[0], r3.at[c], sp=partner)
        for j in range(2):
            far = 2 - 2 * side + j
            y5_out[n - held, j, :, lanes] = keep[m, 0, far, :, :width].astype(BF16)
            send(y5_out.at[n - held, j, :, lanes], y5_in.at[c % held, me_s % 2, :, lanes],
                 s5.at[0], r5.at[c % held], sp=far)

    def stage_four(n):
        c = place_of(n)
        paired(n).wait_recv()
        y4_out[c] = (keep[n, 0, opposite] + y3_in[c, 1].astype(F32)).astype(BF16)
        crossed(n).start()
        at = aligned(c, half_col)
        stream[:, at] += keep[n, 0, me_s] + y3_in[c, 0].astype(F32)

    def finish(n):
        c = place_of(n)
        if n < held:
            at = aligned(c, half_col)
            total = stream[:, at]
            piece = y5_in.at[c % held]
            pltpu.make_async_remote_copy(
                src_ref=piece, dst_ref=piece, send_sem=s5.at[0], recv_sem=r5.at[c % held],
                device_id={"sp": opposite}, device_id_type=MESH,
            ).wait_recv()
            for j in range(2):
                total += y5_in[c % held, j].astype(F32)
            out_ref[:, at] = total.astype(BF16)
            return
        paired(n).wait_recv()
        crossed(n).wait_recv()
        for m, (half, part) in enumerate(steps):
            if half == n:
                width, lanes = lanes_of(m)
                at = columns(m)
                out_ref[:, at] = (
                    stream[:, at] + keep[m, 0, me_s, :, :width]
                    + y3_in[c, 0, :, lanes].astype(F32) + y4_in[c, :, lanes].astype(F32)
                ).astype(BF16)

    loaded((2,))
    for m in range(6):
        if m in (2, 3):
            relay(downs[2 * m - 4], 2)
            relay(downs[2 * m - 3], 2)
        if m == 4:
            relay(downs[0], 1)
            relay(downs[1], 1)
        if m == 5:
            relay(downs[2], 1)
            relay(downs[3], 1)
        if m > held:
            stage_two(m - 1)
        down(m)
        if 1 <= m <= held:
            stage_two(m - 1)
        if m >= 3:
            stage_three(m - 3)
    down(6)
    down(7)
    for m in (5, 6, 7):
        stage_two(m)
    stage_three(3)
    issue([(stage_four, 0), (stage_four, 1)], [])
    down(8)
    stage_three(4)
    issue([(stage_four, 2), (stage_four, 3)], [])
    down(9)
    stage_two(8)
    stage_three(5)
    stage_three(6)
    stage_two(9)
    stage_three(7)
    issue([], [(stage_four, 0), (stage_four, 1)])
    stage_three(8)
    issue([], [(stage_four, 2), (stage_four, 3)])
    stage_three(9)
    rows_to(across, x.at[:, 0], ax_s, ax_r).wait_send()
    rows_to(mate, x.at[:, pl.ds(0, 2)], am_s, am_r).wait_send()
    rows_to(mate, y1_out.at[pl.ds(0, len(blocks))], s1, r1).wait_send()
    rows_to(across, y2_out.at[pl.ds(0, len(blocks))], s2, r2).wait_send()

    @pl.when(inner)
    def _():
        for n in (2, 3):
            along(me_s, n, near[0]).wait_send()

    gone(0, 0)
    issue([(gone, 0, 2)], [])
    for i in range(3):
        gone(4, i)
        for k in (0, 4):
            sized(me_s, lambda width: passed(k, i, whole(k, width)).wait_send())
    for n in (4, 5, 0, 1, 2, 3, 6, 7):
        finish(n)
    for to, piece, ss, rs in (
        (partner, y3_out.at[pl.ds(0, 6)], s3, r3),
        (opposite, y4_out.at[pl.ds(0, held)], s4, r4),
        (opposite, y5_out, s5, r5),
    ):
        pltpu.make_async_remote_copy(
            src_ref=piece, dst_ref=piece, send_sem=ss.at[0], recv_sem=rs.at[0],
            device_id={"sp": to}, device_id_type=MESH,
        ).wait_send()


def moved_weights(
    ssm_input, residual_in, log_step, decay_real, freq, in_real, in_imag, out_real, out_imag,
    skip, w_glu, b_glu, w_branch, norm_gain, w_gate, w_up, w_down,
):
    sizes = {axis: lax.axis_size(axis) for axis in ("grp", "sp", "tp")}
    n_sp, n_tp = sizes["sp"], sizes["tp"]
    tok, width = ssm_input.shape
    groups, states = decay_real.shape
    group = in_real.shape[2]
    lanes = groups * states
    own = tok // n_tp
    chan, d_model = w_branch.shape
    depth, hid = w_gate.shape
    cols = w_down.shape[1]
    wide = -(-hid // (TILE * n_sp)) * TILE
    rows = n_sp * tok
    operands = (
        ssm_input, residual_in, log_step[None], decay_real, freq,
        in_real.swapaxes(1, 2).reshape(width, states),
        in_imag.swapaxes(1, 2).reshape(width, states),
        out_real.reshape(width, states), out_imag.reshape(width, states),
        skip[None], w_glu, b_glu[None], w_branch, norm_gain[None], w_gate, w_up, w_down,
    )
    blocks, steps = 2 * n_sp, 2 * n_sp + 2
    vm = pl.BlockSpec(memory_space=pltpu.VMEM)
    hbm = pl.BlockSpec(memory_space=pl.ANY)
    dma = pltpu.SemaphoreType.DMA
    vmem = pltpu.VMEM
    return pl.pallas_call(
        functools.partial(layer_kernel, sizes),
        out_shape=pltpu.VMEM((own, d_model), BF16),
        in_specs=[hbm] * len(operands),
        out_specs=vm,
        scratch_shapes=[
            vmem((n_sp, n_tp, own, d_model), BF16),
            vmem((own, d_model), F32),
            vmem((d_model, 2 * wide), BF16),
            vmem((wide, d_model), BF16),
            vmem((rows, 2 * wide), F32),
            vmem((rows, wide), BF16),
            vmem((steps, 2, n_sp, own, cols // 2), F32),
            vmem((steps, 2, n_sp, own, cols // 2), BF16),
            vmem((steps, 2, n_sp, own, cols // 2), BF16),
            vmem((steps, n_sp, own, cols // 2), BF16),
            vmem((steps, n_sp, own, cols // 2), BF16),
            vmem((blocks, 2, own, cols // 2), BF16),
            vmem((blocks, 2, own, cols // 2), BF16),
            vmem((blocks, own, cols // 2), BF16),
            vmem((blocks, own, cols // 2), BF16),
            vmem((blocks // 2, 2, own, cols // 2), BF16),
            vmem((blocks // 2, 2, own, cols // 2), BF16),
            dma((3,)),
            dma((2, 3)), dma((7, 3)), dma((2, 3)), dma((3, 3)),
            dma((4,)), dma((n_sp,)),
            dma((1,)), dma((n_sp,)),
            dma((1,)), dma((1,)),
            dma((1,)), dma((steps,)), dma((1,)), dma((steps,)),
            dma((1,)), dma((blocks,)), dma((1,)), dma((blocks // 2,)),
            dma((1,)), dma((blocks // 2,)),
            pltpu.SemaphoreType.REGULAR((3,)),
            dma((len(SMALL),)),
            *[vmem(operands[at].shape, operands[at].dtype) for at in SMALL],
            vmem((chan, chan), BF16),
            vmem((chan, d_model), BF16),
            vmem((own, d_model), BF16),
            vmem((8, lanes), F32),
            vmem((tok, lanes), F32),
            vmem((tok, lanes), F32),
            vmem((tok, lanes), F32),
            vmem((tok, lanes), F32),
            vmem((2, lanes), F32),
            vmem((n_sp - 1, 2, lanes), F32),
            vmem((n_tp, own, width), BF16),
            vmem((n_tp - 1, own, width), BF16),
            vmem((own, chan), F32),
            dma((3,)),
            dma((n_sp - 1,)), dma((n_sp - 1,)),
            dma((n_tp - 1,)), dma((n_tp - 1,)),
        ],
        compiler_params=pltpu.CompilerParams(collective_id=0, has_side_effects=True),
        name="layer",
    )(*operands)


def per_device(*arguments):
    sizes = tuple(lax.axis_size(axis) for axis in ("grp", "sp", "tp"))
    tiles = arguments[14].shape[1] // TILE
    fits = sizes == (2, 4, 4) and tiles % 4 == 3
    return (moved_weights if fits else gathered_weights)(*arguments)


def solution(mesh):
    placed = (
        P(("grp", "sp"), "tp"),
        P(("grp", "sp"), None),
        P("tp"),
        P("tp", None),
        P("tp", None),
        P("tp", None, None),
        P("tp", None, None),
        P("tp", None, None),
        P("tp", None, None),
        P("tp"),
        P(),
        P(),
        P(),
        P(),
        P("sp", "tp"),
        P("sp", "tp"),
        P("tp", "sp"),
    )
    return jax.shard_map(
        per_device,
        mesh=mesh,
        in_specs=placed,
        out_specs=P(("grp", "sp", "tp"), None),
        check_vma=False,
    )
```
